32 devices in a mesh: sp: 16 (over z, y, x), tp: 2 (over core).
Axes of the slice: x: 2, y: 2, z: 4, core: 2. Of those that a mesh axis runs over, the one named last changes fastest.
Arguments:
- tokens: bfloat16 [4096, 4096], P('sp', 'tp'), may hold values from -480 to 480
- gain: float32 [4096], P('tp'), may hold values from 0.1 to 1.9
- q_att: bfloat16 [4096, 2048], P('sp', 'tp'), may hold values from -2.90625 to 2.90625
- k_att: bfloat16 [4096, 1024], P('sp', 'tp'), may hold values from -0.09375 to 0.09375
- v_att: bfloat16 [4096, 1024], P('sp', 'tp'), may hold values from -0.75 to 0.75
- q_ret: bfloat16 [4096, 1024], P('sp', 'tp'), may hold values from -0.09375 to 0.09375
- k_ret: bfloat16 [4096, 1024], P('sp', 'tp'), may hold values from -0.09375 to 0.09375
- v_ret: bfloat16 [4096, 1024], P('sp', 'tp'), may hold values from -0.09375 to 0.09375
- out_att: bfloat16 [2048, 4096], P('tp', 'sp'), may hold values from -0.109375 to 0.109375
- out_ret: bfloat16 [1024, 4096], P('tp', 'sp'), may hold values from -0.109375 to 0.109375
- sink: float32 [16], P('tp'), may hold values from 3 to 7
- decay_log: float32 [8, 4096], P('tp', 'sp'), may hold values from -2.125 to 0
Outputs:
- mixed: bfloat16 [4096, 4096], P(('sp', 'tp'))
- log_weight: float32 [16, 4096], P('tp', 'sp')
The draws below stay inside these ranges and needn't reach their ends.
All inputs are finite; a program needn't handle non-finite values.
Results may differ from the reference program's by a relative error of at most 0.017.
Values may be sent and summed in bfloat16 or wider, within the bound.
A program may use at most 128 MiB of HBM per device.

```python
import jax
import jax.numpy as jnp
from jax import lax

D = 4096
ATT_HEADS = 16
KV_HEADS = 8
RET_HEADS = 8
HEAD_DIM = 128
SPAN_RADIUS = 128
TOK_DEV = 256
TOKENS = 4096
N_TP = 2


def drawn_pair(key):
    base = jax.random.fold_in(key, 31)
    lookup_fraction = jnp.clip(jax.random.normal(jax.random.fold_in(base, 1), (D, KV_HEADS * HEAD_DIM), jnp.float32), -6.0, 6.0) * D ** (-0.5)
    query_part = jnp.clip(jax.random.normal(jax.random.fold_in(base, 2), (D, ATT_HEADS * HEAD_DIM), jnp.float32), -6.0, 6.0) * D ** (-0.5)
    return (query_part, lookup_fraction)


def draw_q_att(key, part):
    return drawn_pair(key)[0].astype(jnp.bfloat16)


def draw_k_att(key, part):
    return drawn_pair(key)[1].astype(jnp.bfloat16)


def draw_tokens(key, part):
    normal_part = jnp.clip(jax.random.normal(jax.random.fold_in(key, 41), (TOKENS, D), jnp.float32), -6.0, 6.0)
    column = jnp.arange(D).astype(jnp.float32) / D
    course = 2.0 * (jnp.arange(TOKENS).astype(jnp.float32) + 0.5) / TOKENS - 1.0
    direction = jax.random.uniform(jax.random.fold_in(key, 43), (1, D), jnp.float32, -1.0, 1.0)
    drift = jnp.exp(1.2 * direction * course[:, None])
    scale = drift * (4.0 ** column)[None, :]
    return (normal_part * scale).astype(jnp.bfloat16)


def draw_decay_log(key, part):
    blocks = TOKENS // TOK_DEV
    share = 0.5
    fast = jax.random.uniform(jax.random.fold_in(key, 51), (RET_HEADS, 1), jnp.float32) < share
    fast_rate = jax.random.uniform(jax.random.fold_in(key, 52), (RET_HEADS, 1), jnp.float32, 10.0, 16.0) / TOK_DEV
    slow_rate = jax.random.uniform(jax.random.fold_in(key, 53), (RET_HEADS, 1), jnp.float32, 0.1, 0.3) / TOKENS
    fading_pace = jnp.where(fast, fast_rate, slow_rate)
    scaling_factor = jnp.exp(jax.random.uniform(jax.random.fold_in(key, 54), (RET_HEADS, blocks), jnp.float32, jnp.log(0.5), jnp.log(2.0)))
    scaling_factor = jnp.repeat(scaling_factor, TOK_DEV, axis=1)
    spots = jax.random.randint(jax.random.fold_in(key, 55), (2,), 0, TOKENS)
    agreement_tally = (jnp.arange(TOKENS)[None, :] == spots[:, None]).astype(jnp.float32)
    discarded_entries = jnp.log(jax.random.uniform(jax.random.fold_in(key, 56), (2, RET_HEADS), jnp.float32, 0.5, 0.8))
    clustered_lists = jnp.dot(discarded_entries.T, agreement_tally)
    return -fading_pace * scaling_factor + clustered_lists


def steps_of(key, dims, cuts, least, largest):
    loudness, own = 1.0, jax.random.fold_in(key, 6)
    for axis_at, shards_of in cuts:
        heights = jnp.exp(jax.random.uniform(jax.random.fold_in(own, axis_at), (shards_of,), jnp.float32, least / len(cuts), largest / len(cuts)))
        loudness = loudness * jnp.repeat(heights, dims[axis_at] // shards_of).reshape([-1 if axis == axis_at else 1 for axis in range(len(dims))])
    return loudness


def scatter_about(key, extent, spread, reach, split=(), kind=jnp.bfloat16):
    values = jax.random.normal(key, extent, jnp.float32) * spread
    if len(split) > 0:
        values = steps_of(key, extent, split, -0.22, 0.18) * values
    return jnp.clip(values, min=-reach, max=reach).astype(kind)


def setup_inputs(seed: int = 0) -> dict:
    streams_of = jax.random.split(jax.random.key(seed), 13)
    return {
        "tokens": draw_tokens(jax.random.fold_in(streams_of[12], 71), 0),
        "gain": jnp.clip(1.0 + 0.18 * jax.random.normal(streams_of[1], (D,), jnp.float32), 0.1, 1.9),
        "q_att": draw_q_att(jax.random.fold_in(streams_of[12], 71), 0),
        "k_att": draw_k_att(jax.random.fold_in(streams_of[12], 71), 0),
        "v_att": scatter_about(streams_of[4], (D, KV_HEADS * HEAD_DIM), (max(D // 64, 1)) ** -0.5, 0.75, ((0, 16), (1, 2))),
        "q_ret": scatter_about(streams_of[5], (D, RET_HEADS * HEAD_DIM), D ** -0.5, 0.09375, ((0, 16), (1, 2))),
        "k_ret": scatter_about(streams_of[6], (D, RET_HEADS * HEAD_DIM), D ** -0.5, 0.09375, ((0, 16), (1, 2))),
        "v_ret": scatter_about(streams_of[7], (D, RET_HEADS * HEAD_DIM), D ** -0.5, 0.09375, ((0, 16), (1, 2))),
        "out_att": scatter_about(streams_of[8], (ATT_HEADS * HEAD_DIM, D), ((ATT_HEADS + RET_HEADS) * HEAD_DIM) ** -0.5, 0.109375, ((0, 2), (1, 16))),
        "out_ret": scatter_about(streams_of[9], (RET_HEADS * HEAD_DIM, D), ((ATT_HEADS + RET_HEADS) * HEAD_DIM) ** -0.5, 0.109375, ((0, 2), (1, 16))),
        "sink": jnp.clip(3.0 + 4.0 * jax.random.uniform(streams_of[10], (ATT_HEADS,), jnp.float32) ** steps_of(streams_of[10], (ATT_HEADS,), ((0, 2),), -0.2, 0.2), 3.0, 7.0),
        "decay_log": draw_decay_log(jax.random.fold_in(streams_of[12], 71), 0),
    }


def rotate(values, angles):
    half = values.shape[-1] // 2
    first = values[..., :half]
    second = values[..., half:]
    cosine = jnp.cos(angles)[:, None, :]
    sine = jnp.sin(angles)[:, None, :]
    return jnp.concatenate([first * cosine - second * sine, second * cosine + first * sine], axis=-1)

def angle_table(positions):
    freqs = 10000.0 ** (-jnp.arange(0, HEAD_DIM, 2).astype(jnp.float32) / HEAD_DIM)
    return positions[:, None] * freqs[None, :]

def window_attention(queries, padded_keys, padded_values, sink_logit, offset, total_rows, block_rows):
    count = queries.shape[0] // block_rows
    nearby_memory = queries.shape[1]
    group = queries.shape[2]

    def single_block(index):
        begin = index * block_rows
        block_query = lax.dynamic_slice_in_dim(queries, begin, block_rows, 0).astype(jnp.float32)
        block_keys = lax.dynamic_slice_in_dim(padded_keys, begin, block_rows + 2 * SPAN_RADIUS, 0).astype(jnp.float32)
        block_values = lax.dynamic_slice_in_dim(padded_values, begin, block_rows + 2 * SPAN_RADIUS, 0).astype(jnp.float32)
        scores = jnp.einsum('qhgd,khd->hgqk', block_query, block_keys) * HEAD_DIM ** (-0.5)
        query_pos = offset + begin + jnp.arange(block_rows, dtype=jnp.int32)
        key_pos = offset + begin - SPAN_RADIUS + jnp.arange(block_rows + 2 * SPAN_RADIUS, dtype=jnp.int32)
        spacing = key_pos[None, :] - query_pos[:, None]
        valid = (jnp.abs(spacing) <= SPAN_RADIUS) & (key_pos >= 0)[None, :] & (key_pos < total_rows)[None, :]
        masked = jnp.where(valid, scores, -jnp.inf)
        top = jnp.maximum(lax.optimization_barrier(jnp.max(masked, axis=-1)), sink_logit[:, :, None])
        expo = jnp.exp(masked - top[..., None])
        total = lax.optimization_barrier(jnp.sum(expo, axis=-1)) + jnp.exp(sink_logit[:, :, None] - top)
        logs = top + jnp.log(total)
        probs = (expo / total[..., None]).astype(jnp.bfloat16)
        result = jnp.einsum('hgqk,khd->qhgd', probs.astype(jnp.float32), block_values).astype(jnp.bfloat16)
        return (result.reshape(block_rows, nearby_memory * group * HEAD_DIM), logs.reshape(nearby_memory * group, block_rows))
    outs, logs = lax.map(single_block, jnp.arange(count, dtype=jnp.int32))
    return (outs.reshape(queries.shape[0], -1), jnp.moveaxis(logs, 0, 1).reshape(logs.shape[1], -1))

def retention(queries, keys, values, decay):
    blocks = queries.shape[0] // TOK_DEV
    heads = queries.shape[1]
    highest = lax.Precision.HIGHEST
    query_b = queries.reshape(blocks, TOK_DEV, heads, HEAD_DIM)
    key_b = keys.reshape(blocks, TOK_DEV, heads, HEAD_DIM)
    value_b = values.reshape(blocks, TOK_DEV, heads, HEAD_DIM)
    decay_b = jnp.moveaxis(decay.reshape(heads, blocks, TOK_DEV), 1, 0)

    def local(items):
        query_f = items[0].astype(jnp.float32)
        key_f = items[1].astype(jnp.float32)
        value_f = items[2].astype(jnp.float32)
        cumul = jnp.cumsum(items[3], axis=1)
        last = cumul[:, -1]
        scores = jnp.einsum('qhd,khd->hqk', query_f, key_f)
        weights = jnp.exp(-jnp.abs(cumul[:, :, None] - cumul[:, None, :]))
        inner = jnp.einsum('hqk,khd->qhd', scores * weights, value_f, precision=highest)
        forward = jnp.einsum('hk,khd,khe->hde', jnp.exp(last[:, None] - cumul), key_f, value_f, precision=highest)
        backward = jnp.einsum('hk,khd,khe->hde', jnp.exp(cumul), key_f, value_f, precision=highest)
        return (inner, forward, backward, jnp.exp(last), cumul)
    inner, forward, backward, totals, cumuls = lax.map(local, (query_b, key_b, value_b, decay_b))

    def step(carry, item):
        return (item[0][:, None, None] * carry + item[1], carry)
    zero = jnp.zeros(forward.shape[1:], jnp.float32)
    _, before = lax.scan(step, zero, (totals, forward))
    _, after = lax.scan(step, zero, (totals, backward), reverse=True)
    query_f = query_b.astype(jnp.float32)
    lead = jnp.moveaxis(jnp.exp(cumuls), 1, 2)[..., None]
    trail = jnp.moveaxis(jnp.exp(cumuls[:, :, -1:] - cumuls), 1, 2)[..., None]
    carried = lead * jnp.einsum('bqhd,bhde->bqhe', query_f, before, precision=highest)
    carried = carried + trail * jnp.einsum('bqhd,bhde->bqhe', query_f, after, precision=highest)
    blended_output = inner + carried
    middle_point = blended_output - lax.optimization_barrier(jnp.mean(blended_output, axis=-1, keepdims=True))
    normed = middle_point * lax.rsqrt(lax.optimization_barrier(jnp.mean(middle_point * middle_point, axis=-1, keepdims=True)) + 1e-06)
    return normed.astype(jnp.bfloat16).reshape(queries.shape[0], heads * HEAD_DIM)

def reference(tokens, gain, q_att, k_att, v_att, q_ret, k_ret, v_ret, out_att, out_ret, sink, decay_log):
    widened = tokens.astype(jnp.float32)
    inverse = lax.rsqrt(lax.optimization_barrier(jnp.sum(widened * widened, axis=1)) / D + 1e-06)[:, None]
    scaled = (widened * gain).astype(jnp.bfloat16)

    def project(weight):
        return jnp.dot(scaled, weight, preferred_element_type=jnp.float32) * inverse
    angles = angle_table(jnp.arange(TOKENS).astype(jnp.float32))
    group = ATT_HEADS // KV_HEADS
    att_query = rotate(project(q_att).reshape(TOKENS, ATT_HEADS, HEAD_DIM), angles).astype(jnp.bfloat16)
    att_key = rotate(project(k_att).reshape(TOKENS, KV_HEADS, HEAD_DIM), angles).astype(jnp.bfloat16)
    att_value = project(v_att).astype(jnp.bfloat16).reshape(TOKENS, KV_HEADS, HEAD_DIM)
    padding = ((SPAN_RADIUS, SPAN_RADIUS), (0, 0), (0, 0))
    att_out, log_weight = window_attention(att_query.reshape(TOKENS, KV_HEADS, group, HEAD_DIM), jnp.pad(att_key, padding), jnp.pad(att_value, padding), sink.reshape(KV_HEADS, group), 0, TOKENS, min(TOK_DEV, 512))
    ret_query = project(q_ret).astype(jnp.bfloat16).reshape(TOKENS, RET_HEADS, HEAD_DIM)
    ret_key = (jnp.dot(scaled, k_ret, preferred_element_type=jnp.float32) * (inverse * HEAD_DIM ** (-0.5))).astype(jnp.bfloat16).reshape(TOKENS, RET_HEADS, HEAD_DIM)
    ret_value = project(v_ret).astype(jnp.bfloat16).reshape(TOKENS, RET_HEADS, HEAD_DIM)
    ret_out = retention(ret_query, ret_key, ret_value, decay_log)
    att_width = ATT_HEADS * HEAD_DIM // N_TP
    ret_width = RET_HEADS * HEAD_DIM // N_TP
    summed = jnp.zeros((TOKENS, D), jnp.float32)
    for member in range(N_TP):
        term = jnp.dot(att_out[:, member * att_width:(member + 1) * att_width], out_att[member * att_width:(member + 1) * att_width], preferred_element_type=jnp.float32)
        term = term + jnp.dot(ret_out[:, member * ret_width:(member + 1) * ret_width], out_ret[member * ret_width:(member + 1) * ret_width], preferred_element_type=jnp.float32)
        summed = summed + lax.optimization_barrier(term.astype(jnp.bfloat16)).astype(jnp.float32)
    return (summed.astype(jnp.bfloat16), log_weight)
```

```python
import math

import jax
import jax.numpy as jnp
import numpy as np
from jax import lax
from jax.experimental import pallas as pl
from jax.experimental.pallas import tpu as pltpu
from jax.sharding import Mesh
from jax.sharding import PartitionSpec as P

HEAD_DIM = 128
SPAN_RADIUS = 128
BLOCK = 256
HIGHEST = lax.Precision.HIGHEST
MESH = pl.DeviceIdType.MESH


def gather(x, axis, dim):
    if lax.axis_size(axis) == 1:
        return x
    return lax.all_gather(x, axis, axis=dim, tiled=True)


def exchange(x, axis, split, concat):
    if lax.axis_size(axis) == 1:
        return x
    return lax.all_to_all(x, axis, split, concat, tiled=True)


def halo(shard, axis, width):
    peers, length = lax.axis_size(axis), shard.shape[1]
    up = [(i, i + 1) for i in range(peers - 1)]
    down = [(j, i) for i, j in up]
    before = lax.ppermute(shard[:, length - width :], axis, up)
    after = lax.ppermute(shard[:, :width], axis, down)
    return jnp.concatenate([before, shard, after], axis=1)


def rotate(values, cosine, sine):
    half = values.shape[-1] // 2
    first, second = values[..., :half], values[..., half:]
    return jnp.concatenate(
        [first * cosine - second * sine, second * cosine + first * sine], axis=-1
    ).astype(jnp.bfloat16)


class Stream:
    def __init__(self, where, remote, refs, pack):
        self.where, self.remote, self.pack = where, remote, pack
        (
            self.wide, self.away, self.out,
            self.load, self.x_send, self.z_send, self.h_send, self.y_send,
            self.p_recv, self.w_recv,
        ) = refs

    def fetch(self):
        w = self.where
        targets = (
            (self.out.at[0], 1 - w.g, 1 - w.x),
            (self.out.at[1], w.g, 1 - w.x),
            (self.wide.at[w.own], w.g, w.x),
            (self.away.at[w.x], 1 - w.g, w.x),
        )
        for i, (target, g, x) in enumerate(targets):
            self.pack(2 * g + x, target, self.load.at[i])

    def fetched(self):
        w = self.where
        for i, target in enumerate(
            (self.out.at[0], self.out.at[1], self.wide.at[w.own], self.away.at[w.x])
        ):
            pltpu.make_async_copy(target, target, self.load.at[i]).wait()

    def along_x(self, k):
        w = self.where
        if k == 0:
            return self.remote(
                self.out.at[0], self.away.at[w.x], self.x_send.at[0], self.p_recv.at[0], w.to_x
            )
        return self.remote(
            self.out.at[1], self.wide.at[w.own], self.x_send.at[1], self.w_recv.at[w.own], w.to_x
        )

    def along_z(self, k):
        w = self.where
        x = w.x if k == 0 else 1 - w.x
        s = w.at(w.zh, w.zl, w.y, x)
        return self.remote(
            self.away.at[x], self.wide.at[s], self.z_send.at[k], self.w_recv.at[s], w.to_z
        )

    def near(self, k):
        w = self.where
        return w.at(w.zh, (w.zl, 1 - w.zl)[k // 2], w.y, (w.x, 1 - w.x)[k % 2])

    def far(self, k):
        w = self.where
        return w.at(1 - w.zh, (w.zl, 1 - w.zl)[1 - k // 2], w.y, (w.x, 1 - w.x)[k % 2])

    def along_h(self, k):
        s = self.near(k)
        return self.remote(
            self.wide.at[s], self.wide.at[s], self.h_send.at[k], self.w_recv.at[s], self.where.to_h
        )

    def along_y(self, k):
        s = self.near(k) if k < 4 else self.far(k - 4)
        return self.remote(
            self.wide.at[s], self.wide.at[s], self.y_send.at[k], self.w_recv.at[s], self.where.to_y
        )

    def arrive(self, s):
        self.remote(
            self.wide.at[s], self.wide.at[s], self.x_send.at[0], self.w_recv.at[s], self.where.to_x
        ).wait_recv()

    def arrive_away(self):
        w = self.where
        slot = self.away.at[1 - w.x]
        self.remote(slot, slot, self.x_send.at[0], self.p_recv.at[0], w.to_x).wait_recv()

    def arrive_across(self):
        w = self.where
        for zh in (w.zh, 1 - w.zh):
            for zl in range(2):
                for x in range(2):
                    self.arrive(w.at(zh, zl, 1 - w.y, x))

    def drain(self):
        for k in range(2):
            self.along_x(k).wait_send()
            self.along_z(k).wait_send()
        for k in range(4):
            self.along_h(k).wait_send()
        for k in range(8):
            self.along_y(k).wait_send()


class Place:
    def __init__(self):
        self.zh, self.zl, self.y, self.x, self.c = (
            lax.axis_index(a) for a in ("zh", "zl", "y", "x", "tp")
        )
        self.g = lax.rem(self.zh + self.zl, 2)
        self.h = 2 * self.g + self.x
        self.own = self.at(self.zh, self.zl, self.y, self.x)
        self.b = 2 * self.zl + self.x
        self.to_x = {"x": 1 - self.x}
        self.to_z = {"zl": 1 - self.zl}
        self.to_y = {"y": 1 - self.y}
        self.to_h = {"zh": 1 - self.zh, "zl": 1 - self.zl}
        self.to_hy = {"zh": 1 - self.zh, "zl": 1 - self.zl, "y": 1 - self.y}
        self.to_zx = {"zl": 1 - self.zl, "x": 1 - self.x}
        self.to_c = {"tp": 1 - self.c}

    @staticmethod
    def at(zh, zl, y, x):
        return ((zh * 2 + zl) * 2 + y) * 2 + x


def fused_kernel(
    tokens, gain, q_att, k_att, v_att, q_ret, k_ret, v_ret, out_att, out_ret, sink, decay,
    cos_t, sin_t, base,
    mixed, logs_out,
    raw, scl, ssq, gains, proj, kvext, qrot, rets, dec, cumr, cumc, coef, states, stall,
    mix, logm, lsend, lrecv, mine, give, take, s1, r1, s2, r2,
    t_load, t_x, t_z, t_c, t_recv, g_sem, d_sem, halo_sem, st_sem, l_sem,
    give_s, take_r, s1_s, r1_r, s2_s, r2_r,
    *streams,
):
    w = Place()
    f32, bf16 = jnp.float32, jnp.bfloat16
    own, half_d = tokens.shape
    rows = 4 * own
    run_rows = 2 * own
    total_rows = 16 * own
    H = HEAD_DIM
    edge = SPAN_RADIUS

    def remote(src, dst, send, recv, to):
        return pltpu.make_async_remote_copy(
            src_ref=src, dst_ref=dst, send_sem=send, recv_sem=recv,
            device_id=to, device_id_type=MESH,
        )

    def lanes(h, n):
        return pl.ds(pl.multiple_of(h * n, n), n)

    def pack_cols(parts):
        def pack(h, target, sem):
            start = 0
            for ref in parts:
                n = ref.shape[1] // 4
                pltpu.make_async_copy(
                    ref.at[:, lanes(h, n)], target.at[:, pl.ds(start, n)], sem
                ).start()
                start += n
        return pack

    def pack_rows(parts):
        def pack(h, target, sem):
            start = 0
            for ref in parts:
                n = ref.shape[0] // 4
                pltpu.make_async_copy(
                    ref.at[lanes(h, n), :], target.at[pl.ds(start, n), :], sem
                ).start()
                start += n
        return pack

    n = len(streams) // 3
    A = Stream(w, remote, streams[:n], pack_cols((q_att, k_att, v_att)))
    R = Stream(w, remote, streams[n : 2 * n], pack_cols((q_ret, k_ret, v_ret)))
    O = Stream(w, remote, streams[2 * n :], pack_rows((out_att, out_ret)))

    token_load = pltpu.make_async_copy(tokens, raw.at[w.c, w.b], t_load.at[0])
    gain_load = pltpu.make_async_copy(gain, gains.at[w.c], t_load.at[1])
    decay_load = pltpu.make_async_copy(decay, dec.at[w.zh, w.y, w.zl, w.x], t_load.at[2])

    def block(zl, x):
        return 2 * zl + x

    def token(b, send, to):
        here = raw.at[w.c, b]
        return remote(here, here, send, t_recv.at[w.c, b], to)

    tokens_x = (
        token(w.b, t_x.at[0], w.to_x),
        token(block(1 - w.zl, w.x), t_x.at[1], w.to_x),
    )
    tokens_z = token(w.b, t_z.at[0], w.to_z)

    def tokens_c(k):
        b = block((w.zl, 1 - w.zl)[k // 2], (w.x, 1 - w.x)[k % 2])
        return token(b, t_c.at[k], w.to_c)

    def token_arrive(k, e=None):
        b = block((w.zl, 1 - w.zl)[k // 2], (w.x, 1 - w.x)[k % 2])
        e = w.c if e is None else e
        here = raw.at[e, b]
        remote(here, here, t_x.at[0], t_recv.at[e, b], w.to_x).wait_recv()

    gain_c = remote(gains.at[w.c], gains.at[w.c], g_sem.at[0], g_sem.at[1], w.to_c)

    d_parts = (
        (dec.at[w.zh, w.y, w.zl, w.x], dec.at[w.zh, w.y, w.zl, 1 - w.x], w.to_x),
        (dec.at[w.zh, w.y, w.zl], dec.at[w.zh, w.y, 1 - w.zl], w.to_z),
        (dec.at[w.zh, w.y], dec.at[w.zh, 1 - w.y], w.to_y),
        (dec.at[w.zh], dec.at[1 - w.zh], w.to_h),
    )

    def decay_send(k):
        src, _, to = d_parts[k]
        return remote(src, src, d_sem.at[0, k], d_sem.at[1, k], to)

    def decay_arrive(k):
        _, dst, to = d_parts[k]
        remote(dst, dst, d_sem.at[0, k], d_sem.at[1, k], to).wait_recv()

    A.fetch()
    token_load.start()
    gain_load.start()
    decay_load.start()
    R.fetch()
    O.fetch()

    barrier = pltpu.get_barrier_semaphore()
    friends = (w.to_x, w.to_z, w.to_y, w.to_h, w.to_hy, w.to_zx, w.to_c)
    for to in friends:
        pl.semaphore_signal(barrier, inc=1, device_id=to, device_id_type=MESH)
    pl.semaphore_wait(barrier, len(friends))

    middle = w.g == 1

    A.fetched()
    A.along_x(0).start()
    A.along_z(0).start()
    A.along_y(0).start()
    R.fetched()
    R.along_x(0).start()
    R.along_z(0).start()
    R.along_y(0).start()
    A.along_x(1).start()
    R.along_x(1).start()

    @pl.when(middle)
    def _():
        A.along_h(0).start()
        R.along_h(0).start()

    decay_load.wait()
    gain_load.wait()
    gain_c.start()
    decay_send(0).start()
    token_load.wait()
    tokens_x[0].start()
    tokens_c(0).start()

    def scale(e, b):
        @pl.loop(0, own // 16)
        def _(i):
            value = raw[e, b, pl.ds(pl.multiple_of(i * 16, 16), 16), :].astype(f32)
            at = pl.ds(pl.multiple_of(b * own + i * 16, 16), 16)
            scl[e, at, :] = (value * gains[e]).astype(bf16)
            square = value * value
            total = square[:, :H]
            for k in range(1, half_d // H):
                total = total + square[:, k * H : (k + 1) * H]
            ssq[e, at, :] = total

    @pl.when((w.zh == 0) & (w.y == 0))
    def _():
        kvext[0, :, 0:edge, :] = jnp.zeros((2, edge, H), bf16)

    @pl.when((w.zh == 1) & (w.y == 1))
    def _():
        kvext[1, :, edge + run_rows :, :] = jnp.zeros((2, edge, H), bf16)

    scale(w.c, w.b)
    A.arrive_away()
    A.along_z(1).start()
    decay_arrive(0)
    decay_send(1).start()
    R.arrive_away()
    R.along_z(1).start()
    tokens_z.start()
    decay_arrive(1)
    decay_send(2).start()
    remote(gains.at[1 - w.c], gains.at[1 - w.c], g_sem.at[0], g_sem.at[1], w.to_c).wait_recv()
    token_arrive(0, 1 - w.c)
    scale(1 - w.c, w.b)
    for k in (2, 1, 3):
        for stream in (A, R):
            stream.arrive(stream.near(k))
            stream.along_y(k).start()

            @pl.when(middle)
            def _():
                stream.along_h(k).start()

    @pl.when(w.g == 0)
    def _():
        for k in range(4):
            A.along_h(k).start()
        for k in range(4):
            R.along_h(k).start()

    decay_arrive(2)
    decay_send(3).start()
    decay_arrive(3)

    lane = lax.broadcasted_iota(jnp.int32, (8, run_rows), 1)
    for slot in range(2):
        row = jnp.concatenate(
            [dec[w.zh, w.y, slot, x, pl.ds(w.h, 1), :] for x in range(2)], axis=1
        )
        row = jnp.broadcast_to(row, (8, run_rows))
        step = 1
        while step < run_rows:
            row = row + jnp.where(lane >= step, pltpu.roll(row, step, axis=1), 0.0)
            step *= 2
        cumr[slot] = row
        cumc[slot] = jnp.transpose(jnp.broadcast_to(row[0:1], (H, run_rows)))
    lane = lax.broadcasted_iota(jnp.int32, (8, H), 1)
    run = lax.broadcasted_iota(jnp.int32, (8, H), 0)
    totals = jnp.zeros((8, H), f32)
    for zh in range(2):
        for slot in range(2):
            for y in range(2):
                pair = sum(dec[zh, y, slot, x, pl.ds(w.h, 1), :] for x in range(2))
                value = jnp.sum(pair, axis=1, keepdims=True)
                totals = jnp.where(lane == 4 * zh + 2 * slot + y, value, totals)
    for slot in range(2):
        me = 4 * w.zh + 2 * slot + w.y
        between = (lane > jnp.minimum(run, me)) & (lane < jnp.maximum(run, me))
        factor = jnp.exp(jnp.sum(jnp.where(between, totals, 0.0), axis=1, keepdims=True))
        factor = jnp.broadcast_to(factor, (8, H))
        coef[slot, 0] = jnp.where(run < me, factor, 0.0)
        coef[slot, 1] = jnp.where(run > me, factor, 0.0)

    token_arrive(2)
    tokens_x[1].start()
    tokens_c(2).start()
    token_arrive(1)
    tokens_c(1).start()
    O.fetched()
    O.along_x(0).start()
    O.along_x(1).start()
    for k in (2, 1):
        b = block((w.zl, 1 - w.zl)[k // 2], (w.x, 1 - w.x)[k % 2])
        scale(w.c, b)
    for k in (2, 1):
        b = block((w.zl, 1 - w.zl)[k // 2], (w.x, 1 - w.x)[k % 2])
        token_arrive(k, 1 - w.c)
        scale(1 - w.c, b)
    for k in range(4):
        A.arrive(A.far(k))
        A.along_y(4 + k).start()

    def pass_far(stream, k):
        stream.arrive(stream.far(k))
        stream.along_y(4 + k).start()

    @pl.when(middle)
    def _():
        for k in range(4):
            pass_far(R, k)

    token_arrive(3)
    tokens_c(3).start()
    b3 = block(1 - w.zl, 1 - w.x)
    scale(w.c, b3)
    token_arrive(3, 1 - w.c)
    scale(1 - w.c, b3)
    O.along_z(0).start()
    A.arrive_across()

    def project(stream, b, start, width):
        at = pl.ds(pl.multiple_of(b * own, own), own)
        depth = half_d // own
        first = stream.wide[0:depth, :, start : start + width].reshape(half_d, width)
        second = stream.wide[depth : 2 * depth, :, start : start + width].reshape(half_d, width)
        value = jnp.dot(scl[0, at, :], first, preferred_element_type=f32)
        return value + jnp.dot(scl[1, at, :], second, preferred_element_type=f32)

    def inverse(b):
        at = pl.ds(pl.multiple_of(b * own, own), own)
        squares = jnp.sum(ssq[0, at, :] + ssq[1, at, :], axis=1, keepdims=True)
        return lax.rsqrt(squares / (2 * half_d) + 1e-06)

    def angles(b):
        s = w.at(w.zh, b // 2, w.y, b % 2)
        c0, s0, s0n, c0n = (base[i, pl.ds(s, 1), :] for i in range(4))
        cosine = cos_t[...] * c0 - sin_t[...] * s0
        sine = cos_t[...] * s0n + sin_t[...] * c0n
        return cosine, sine

    def turn(value, cosine, sine):
        return (value * cosine + pltpu.roll(value, H // 2, axis=1) * sine).astype(bf16)

    def attention_inputs(b):
        at = pl.ds(pl.multiple_of(b * own, own), own)
        scale_b = inverse(b)
        cosine, sine = angles(b)
        query = project(A, b, 0, 2 * H) * scale_b
        qrot[at, :H] = turn(query[:, :H], cosine, sine)
        qrot[at, H:] = turn(query[:, H:], cosine, sine)
        other = project(A, b, 2 * H, 2 * H) * scale_b
        inner = pl.ds(pl.multiple_of(edge + (b % 2) * own, edge), own)
        kvext[b // 2, 0, inner, :] = turn(other[:, :H], cosine, sine)
        kvext[b // 2, 1, inner, :] = other[:, H:].astype(bf16)

    @pl.loop(0, 4)
    def _(b):
        attention_inputs(b)

    y = w.y
    head, tail, before_at, after_at = edge, run_rows, 0, edge + run_rows

    def pick(a, b):
        return a + (b - a) * y

    def piece(slot, start):
        return kvext.at[slot, :, pl.ds(pl.multiple_of(start, edge), edge), :]

    halo_y = [
        remote(
            piece(pick(s0, s1), pick(f0, f1)), piece(pick(d0, d1), pick(o0, o1)),
            halo_sem.at[0, i], halo_sem.at[1, i], w.to_y,
        )
        for i, (s0, f0, d0, o0, s1, f1, d1, o1) in enumerate(
            (
                (0, tail, 0, before_at, 0, head, 0, after_at),
                (1, head, 0, after_at, 0, tail, 1, before_at),
                (1, tail, 1, before_at, 1, head, 1, after_at),
            )
        )
    ]
    halo_far = remote(
        piece(pick(0, 1), pick(head, tail)), piece(pick(1, 0), pick(after_at, before_at)),
        halo_sem.at[0, 3], halo_sem.at[1, 3], w.to_hy,
    )
    has_far = ((y == 0) & (w.zh == 1)) | ((y == 1) & (w.zh == 0))
    for copy in halo_y:
        copy.start()

    @pl.when(has_far)
    def _():
        halo_far.start()

    @pl.when(w.g == 0)
    def _():
        for k in range(4):
            pass_far(R, k)

    O.along_y(0).start()
    O.along_h(0).start()
    O.arrive_away()
    O.along_z(1).start()

    def halo_arrive(slot, start, i, to):
        here = piece(slot, start)
        remote(here, here, halo_sem.at[0, i], halo_sem.at[1, i], to).wait_recv()

    halo_arrive(pick(0, 0), pick(after_at, before_at), 0, w.to_y)
    halo_arrive(pick(1, 0), pick(before_at, after_at), 1, w.to_y)
    halo_arrive(pick(1, 1), pick(after_at, before_at), 2, w.to_y)

    @pl.when(has_far)
    def _():
        halo_arrive(pick(0, 1), pick(before_at, after_at), 3, w.to_hy)

    def attend_tile(i):
        slot, j = i // 4, i % 4
        query = qrot[pl.ds(pl.multiple_of(i * edge, edge), edge), :]
        query = jnp.concatenate([query[:, :H], query[:, H:]], axis=0)
        span = pl.ds(pl.multiple_of(j * edge, edge), 3 * edge)
        key, value = kvext[slot, 0, span, :], kvext[slot, 1, span, :]
        score = lax.dot_general(
            query, key, (((1,), (1,)), ((), ())), preferred_element_type=f32
        ) * H ** (-0.5)
        row = lax.broadcasted_iota(jnp.int32, score.shape, 0)
        col = lax.broadcasted_iota(jnp.int32, score.shape, 1)
        shift = col - jnp.where(row < edge, row, row - edge)
        start = w.at(w.zh, slot, y, 0) * own + j * edge - edge
        valid = (
            (shift >= 0) & (shift <= 2 * edge) & (col >= -start) & (col < total_rows - start)
        )
        masked = jnp.where(valid, score, -jnp.inf)
        first = lax.broadcasted_iota(jnp.int32, (2 * edge, 1), 0) < edge
        limit = jnp.where(first, sink[2 * w.h], sink[2 * w.h + 1])
        top = jnp.maximum(jnp.max(masked, axis=1, keepdims=True), limit)
        expo = jnp.exp(masked - top)
        total = jnp.sum(expo, axis=1, keepdims=True) + jnp.exp(limit - top)
        logs = top + jnp.log(total)
        probs = (expo * (1.0 / total)).astype(bf16)
        result = jnp.dot(probs, value, preferred_element_type=f32).astype(bf16)
        at = pl.ds(pl.multiple_of((i // 2) * edge, edge), edge)
        mix[i % 2, at, 0:H] = result[:edge]
        mix[i % 2, at, H : 2 * H] = result[edge:]
        column = lax.broadcasted_iota(jnp.int32, (2 * edge, H), 1)
        logm[...] = jnp.where(column == i, logs, logm[...])

    logm[...] = jnp.zeros_like(logm)

    @pl.loop(0, 4)
    def _(i):
        attend_tile(i)

    for k in (2, 1, 3):
        O.arrive(O.near(k))
        O.along_y(k).start()

        @pl.when(middle)
        def _():
            O.along_h(k).start()

    @pl.loop(4, 8)
    def _(i):
        attend_tile(i)

    turned = jnp.transpose(logm[...])
    for b in range(4):
        lsend[b] = turned[2 * b : 2 * b + 2]
        lrecv[w.h] = jnp.where(w.b == b, turned[2 * b : 2 * b + 2], lrecv[w.h] if b else 0.0)
    h_of = lambda zl, x: 2 * lax.rem(w.zh + zl, 2) + x
    log_to = (
        (1 - w.x, w.zl, w.to_x), (w.x, 1 - w.zl, w.to_z), (1 - w.x, 1 - w.zl, w.to_zx),
    )
    log_sends = [
        remote(lsend.at[block(zl, x)], lrecv.at[w.h], l_sem.at[0, i], l_sem.at[1, i], to)
        for i, (x, zl, to) in enumerate(log_to)
    ]

    R.arrive_across()

    def retention_inputs(b):
        at = pl.ds(pl.multiple_of(b * own, own), own)
        scale_b = inverse(b)
        both = project(R, b, 0, 2 * H)
        rets[0, at, :] = (both[:, :H] * scale_b).astype(bf16)
        rets[1, at, :] = (both[:, H:] * (scale_b * H ** (-0.5))).astype(bf16)
        rets[2, at, :] = (project(R, b, 2 * H, H) * scale_b).astype(bf16)

    @pl.loop(0, 4)
    def _(b):
        retention_inputs(b)

    for slot in range(2):
        at = pl.ds(slot * run_rows, run_rows)
        last = cumr[slot, 0:1, run_rows - 1 : run_rows]
        key, value = rets[1, at, :].astype(f32), rets[2, at, :]
        for i, weight in enumerate((jnp.exp(last - cumc[slot]), jnp.exp(cumc[slot]))):
            lhs = (key * weight).astype(bf16)
            state = lax.dot_general(
                lhs, value, (((0,), (0,)), ((), ())), preferred_element_type=f32
            ).astype(bf16)
            stall[w.zh, w.y, slot, i] = state
    state_sends = [
        remote(
            stall.at[w.zh, w.y], stall.at[w.zh, w.y], st_sem.at[0, i], st_sem.at[1, i], to
        )
        for i, to in enumerate((w.to_y, w.to_h, w.to_hy))
    ]
    for copy in state_sends:
        copy.start()
    for copy in log_sends:
        copy.start()

    @pl.when(w.g == 0)
    def _():
        for k in range(1, 4):
            O.along_h(k).start()

    def inner_tile(i):
        slot = i // 2
        at = pl.ds(pl.multiple_of(i * own, own), own)
        keys = pl.ds(pl.multiple_of(slot * run_rows, run_rows), run_rows)
        score = lax.dot_general(
            rets[0, at, :], rets[1, keys, :], (((1,), (1,)), ((), ())),
            preferred_element_type=f32,
        )
        column = cumc[slot, pl.ds(pl.multiple_of((i % 2) * own, own), own), :]
        column = jnp.concatenate([column] * (run_rows // H), axis=1)
        weight = jnp.exp(-jnp.abs(column - cumr[slot, 0:1, :]))
        proj[at, :] = jnp.dot(
            (score * weight).astype(bf16), rets[2, keys, :], preferred_element_type=f32
        )

    @pl.loop(0, 4)
    def _(i):
        inner_tile(i)

    for i, (zh, yy) in enumerate(((w.zh, 1 - y), (1 - w.zh, y), (1 - w.zh, 1 - y))):
        here = stall.at[zh, yy]
        remote(here, here, st_sem.at[0, i], st_sem.at[1, i], w.to_y).wait_recv()
    for slot in range(2):
        for i in range(2):
            total = jnp.zeros((H, H), f32)
            for zh in range(2):
                for s in range(2):
                    for yy in range(2):
                        r = 4 * zh + 2 * s + yy
                        total = total + coef[slot, i, r : r + 1, :] * stall[
                            zh, yy, s, i
                        ].astype(f32)
            states[slot, :, i * H : (i + 1) * H] = total.astype(bf16)

    def finish_tile(i):
        slot = i // 2
        at = pl.ds(pl.multiple_of(i * own, own), own)
        column = cumc[slot, pl.ds(pl.multiple_of((i % 2) * own, own), own), :]
        last = cumr[slot, 0:1, run_rows - 1 : run_rows]
        carried = jnp.dot(rets[0, at, :], states[slot], preferred_element_type=f32)
        value = (
            proj[at, :] + jnp.exp(column) * carried[:, :H]
            + jnp.exp(last - column) * carried[:, H:]
        )
        value = value - jnp.mean(value, axis=1, keepdims=True)
        value = value * lax.rsqrt(jnp.mean(value * value, axis=1, keepdims=True) + 1e-06)
        value = value.astype(bf16)
        out = pl.ds(pl.multiple_of(i * edge, edge), edge)
        mix[0, out, 2 * H :] = value[:edge]
        mix[1, out, 2 * H :] = value[edge:]

    @pl.loop(0, 4)
    def _(i):
        finish_tile(i)

    for k in range(4):
        pass_far(O, k)

    chunks = 8

    def columns_of(i, x):
        a, far, zl = i // 4, (i // 2) % 2, i % 2
        yy = a + y - 2 * a * y
        zh = far + w.zh - 2 * far * w.zh
        return w.at(zh, zl, yy, x)

    def swap(i):
        return remote(give.at[i], take.at[i], give_s.at[i], take_r.at[i], w.to_c)

    def first_hop(i):
        return (
            remote(s1.at[i, 0], r1.at[i, 0], s1_s.at[i, 0], r1_r.at[i, 0], w.to_x),
            remote(s1.at[i, 1], r1.at[i, 1], s1_s.at[i, 1], r1_r.at[i, 1], w.to_z),
        )

    def second_hop(i):
        return (
            remote(s2.at[i, 0], r2.at[i, 0], s2_s.at[i, 0], r2_r.at[i, 0], w.to_z),
            remote(s2.at[i, 1], r2.at[i, 1], s2_s.at[i, 1], r2_r.at[i, 1], w.to_x),
        )

    def part(b):
        return pl.ds(pl.multiple_of(b * edge, edge), edge)

    @pl.loop(0, chunks + 3)
    def _(step):
        @pl.when(step < chunks)
        def _():
            i = step

            @pl.when(i >= chunks // 2)
            def _():
                for x in range(2):
                    O.arrive(columns_of(i, x))

            for k in range(2):
                give[i, k] = jnp.dot(
                    mix[1 - w.c], O.wide[columns_of(i, k)], preferred_element_type=f32
                ).astype(bf16)
            swap(i).start()
            for k in range(2):
                mine[i, k] = jnp.dot(
                    mix[w.c], O.wide[columns_of(i, k)], preferred_element_type=f32
                )

        @pl.when((step >= 1) & (step < chunks + 1))
        def _():
            i = step - 1
            swap(i).wait_recv()
            for k in range(2):
                for j in range(2):
                    b = block(j, 1 - w.x) if k == 0 else block(1 - w.zl, j)
                    total = mine[i, k, part(b), :] + take[i, k, part(b), :].astype(f32)
                    s1[i, k, j] = total.astype(bf16)
            for copy in first_hop(i):
                copy.start()
            for k in range(2):
                for j in range(2):
                    b = block(j, w.x) if k == 0 else block(w.zl, j)
                    mine[i, k, part(b), :] += take[i, k, part(b), :].astype(f32)

        @pl.when((step >= 2) & (step < chunks + 2))
        def _():
            i = step - 2
            for k, copy in enumerate(first_hop(i)):
                copy.wait_recv()
                b = block(1 - w.zl, w.x) if k == 0 else block(w.zl, 1 - w.x)
                j = 1 - w.zl if k == 0 else 1 - w.x
                s2[i, k] = (mine[i, k, part(b), :] + r1[i, k, j].astype(f32)).astype(bf16)
                second_hop(i)[k].start()
            for k in range(2):
                j = w.zl if k == 0 else w.x
                mine[i, k, part(w.b), :] += r1[i, k, j].astype(f32)

        @pl.when(step >= 3)
        def _():
            i = step - 3
            for k, copy in enumerate(second_hop(i)):
                copy.wait_recv()
                at = pl.ds(pl.multiple_of(columns_of(i, k) * own, own), own)
                total = mine[i, k, part(w.b), :] + r2[i, k].astype(f32)
                mixed[:, at] = total.astype(mixed.dtype)

    for i, (x, zl, to) in enumerate(log_to):
        here = lrecv.at[h_of(zl, x)]
        remote(here, here, l_sem.at[0, i], l_sem.at[1, i], to).wait_recv()
    for h in range(4):
        for head_i in range(2):
            for t in range(2):
                logs_out[2 * h + head_i : 2 * h + head_i + 1, t * edge : (t + 1) * edge] = (
                    lrecv[h, t : t + 1, head_i * edge : (head_i + 1) * edge]
                )

    for stream in (A, R, O):
        stream.drain()
    for k in range(4):
        tokens_c(k).wait_send()
        decay_send(k).wait_send()
    for copy in tokens_x + (tokens_z, gain_c):
        copy.wait_send()
    for copy in halo_y + state_sends + log_sends:
        copy.wait_send()

    @pl.when(has_far)
    def _():
        halo_far.wait_send()

    @pl.loop(0, chunks)
    def _(i):
        swap(i).wait_send()
        for copy in first_hop(i) + second_hop(i):
            copy.wait_send()


def fused(*args):
    tokens, gain, q_att = args[:3]
    out_att, out_ret, sink, decay_log = args[8:]
    own, half_d = tokens.shape
    rows, run_rows = 4 * own, 2 * own
    H, edge = HEAD_DIM, SPAN_RADIUS
    bf16, f32 = jnp.bfloat16, jnp.float32
    dma, vmem = pltpu.SemaphoreType.DMA, pltpu.VMEM
    depth = q_att.shape[0]
    width = out_att.shape[1] * 16

    freqs = 10000.0 ** (-np.arange(0, H, 2, dtype=np.float64) / H)
    freqs = np.concatenate([freqs, freqs])[None, :]
    sign = np.where(np.arange(H) < H // 2, -1.0, 1.0)[None, :]
    inner = np.arange(own)[:, None] * freqs
    outer = (np.arange(16) * own)[:, None] * freqs
    cos_t, sin_t = jnp.asarray(np.cos(inner), f32), jnp.asarray(np.sin(inner), f32)
    base = jnp.asarray(
        np.stack([np.cos(outer), np.sin(outer), sign * np.sin(outer), sign * np.cos(outer)]), f32
    )

    def stream(block):
        return [
            vmem((16,) + block, bf16), vmem((2,) + block, bf16), vmem((2,) + block, bf16),
            dma((4,)), dma((2,)), dma((2,)), dma((4,)), dma((8,)), dma((1,)), dma((16,)),
        ]

    out_rows = (out_att.shape[0] + out_ret.shape[0]) // 4
    tile = (8, 2, 4 * edge, own)
    hbm, inside = pl.BlockSpec(memory_space=pl.ANY), pl.BlockSpec(memory_space=pltpu.VMEM)
    return pl.pallas_call(
        fused_kernel,
        out_shape=(
            jax.ShapeDtypeStruct((own // 2, width), bf16),
            jax.ShapeDtypeStruct((sink.shape[0], own), f32),
        ),
        in_specs=[hbm] * 10 + [pl.BlockSpec(memory_space=pltpu.SMEM), hbm] + [inside] * 3,
        out_specs=[inside] * 2,
        scratch_shapes=[
            vmem((2, 4, own, half_d), bf16),
            vmem((2, rows, half_d), bf16),
            vmem((2, rows, H), f32),
            vmem((2, 1, half_d), f32),
            vmem((rows, H), f32),
            vmem((2, 2, run_rows + 2 * edge, H), bf16),
            vmem((rows, 2 * H), bf16),
            vmem((3, rows, H), bf16),
            vmem((2, 2, 2, 2) + decay_log.shape, f32),
            vmem((2, 8, run_rows), f32),
            vmem((2, run_rows, H), f32),
            vmem((2, 2, 8, H), f32),
            vmem((2, H, 2 * H), bf16),
            vmem((2, 2, 2, 2, H, H), bf16),
            vmem((2, 4 * edge, 3 * H), bf16),
            vmem((2 * edge, H), f32),
            vmem((4, 2, 2 * edge), f32),
            vmem((4, 2, 2 * edge), f32),
            vmem(tile, f32), vmem(tile, bf16), vmem(tile, bf16),
            vmem((8, 2, 2, edge, own), bf16), vmem((8, 2, 2, edge, own), bf16),
            vmem((8, 2, edge, own), bf16), vmem((8, 2, edge, own), bf16),
            dma((3,)), dma((2,)), dma((1,)), dma((4,)), dma((2, 4)), dma((2,)), dma((2, 4)),
            dma((2, 4)), dma((2, 3)), dma((2, 3)),
            dma((8,)), dma((8,)), dma((8, 2)), dma((8, 2)), dma((8, 2)), dma((8, 2)),
        ]
        + stream((depth, 4 * H))
        + stream((depth, 3 * H))
        + stream((out_rows, own)),
        compiler_params=pltpu.CompilerParams(
            collective_id=0, has_side_effects=True, vmem_limit_bytes=67043328
        ),
        cost_estimate=pl.CostEstimate(
            flops=10**11, bytes_accessed=2 * 10**7, transcendentals=0
        ),
    )(
        tokens, gain.reshape(1, half_d), *args[2:10], sink, decay_log, cos_t, sin_t, base
    )


def attend(query, key, value, sink, offset, total_rows):
    rows, kv, group, _ = query.shape
    ext = halo(jnp.stack([key, value]), "t", SPAN_RADIUS)
    size = min(rows, BLOCK)
    count = rows // size
    span = size + 2 * SPAN_RADIUS
    pieces = jnp.stack([ext[:, b * size : b * size + span] for b in range(count)])
    blocks = query.reshape(count, size, kv, group, HEAD_DIM)
    scores = jnp.einsum(
        "bqhgd,bkhd->bhgqk", blocks, pieces[:, 0], preferred_element_type=jnp.float32
    ) * HEAD_DIM ** (-0.5)
    base = offset + jnp.arange(count, dtype=jnp.int32) * size
    query_pos = base[:, None] + jnp.arange(size, dtype=jnp.int32)
    key_pos = base[:, None] - SPAN_RADIUS + jnp.arange(span, dtype=jnp.int32)
    spacing = key_pos[:, None, :] - query_pos[:, :, None]
    inside = (key_pos >= 0) & (key_pos < total_rows)
    valid = (jnp.abs(spacing) <= SPAN_RADIUS) & inside[:, None, :]
    masked = jnp.where(valid[:, None, None], scores, -jnp.inf)
    limit = sink[None, :, :, None]
    top = jnp.maximum(jnp.max(masked, axis=-1), limit)
    expo = jnp.exp(masked - top[..., None])
    total = jnp.sum(expo, axis=-1) + jnp.exp(limit - top)
    logs = top + jnp.log(total)
    probs = (expo / total[..., None]).astype(jnp.bfloat16)
    result = jnp.einsum(
        "bhgqk,bkhd->bqhgd", probs, pieces[:, 1], preferred_element_type=jnp.float32
    ).astype(jnp.bfloat16)
    logs = jnp.transpose(logs, (1, 2, 0, 3)).reshape(kv * group, rows)
    return result.reshape(rows, kv * group * HEAD_DIM), logs


def retain(query, key, value, decay):
    rows, heads, _ = query.shape
    peers, index = lax.axis_size("t"), lax.axis_index("t")
    cumul = jnp.cumsum(decay, axis=1)
    last = cumul[:, -1]
    query_f, key_f, value_f = (v.astype(jnp.float32) for v in (query, key, value))
    trailing = jnp.exp(last[:, None] - cumul)
    leading = jnp.exp(cumul)
    forward = jnp.einsum("hk,khd,khe->hde", trailing, key_f, value_f, precision=HIGHEST)
    backward = jnp.einsum("hk,khd,khe->hde", leading, key_f, value_f, precision=HIGHEST)
    tail = jnp.broadcast_to(last[:, None, None], (heads, 8, HEAD_DIM))
    sent = jnp.concatenate([forward, backward, tail], axis=1)
    seen = lax.all_gather(sent, "t", axis=0)
    lasts = seen[:, :, 2 * HEAD_DIM, 0]
    at = jnp.arange(peers)
    low = jnp.minimum(at, index)[:, None]
    high = jnp.maximum(at, index)[:, None]
    between = (at[None, :] > low) & (at[None, :] < high)
    spans = jnp.exp(jnp.sum(jnp.where(between[:, :, None], lasts[None], 0.0), axis=1))
    before = jnp.sum(
        jnp.where(at < index, 1.0, 0.0)[:, None, None, None]
        * spans[:, :, None, None]
        * seen[:, :, :HEAD_DIM],
        axis=0,
    )
    after = jnp.sum(
        jnp.where(at > index, 1.0, 0.0)[:, None, None, None]
        * spans[:, :, None, None]
        * seen[:, :, HEAD_DIM : 2 * HEAD_DIM],
        axis=0,
    )
    scores = jnp.einsum("qhd,khd->hqk", query, key, preferred_element_type=jnp.float32)
    weights = jnp.exp(-jnp.abs(cumul[:, :, None] - cumul[:, None, :]))
    mix = jnp.einsum("hqk,khd->qhd", scores * weights, value_f, precision=HIGHEST)
    mix = mix + leading.T[:, :, None] * jnp.einsum(
        "qhd,hde->qhe", query_f, before, precision=HIGHEST
    )
    mix = mix + trailing.T[:, :, None] * jnp.einsum(
        "qhd,hde->qhe", query_f, after, precision=HIGHEST
    )
    middle = mix - jnp.mean(mix, axis=-1, keepdims=True)
    normed = middle * lax.rsqrt(jnp.mean(middle * middle, axis=-1, keepdims=True) + 1e-06)
    return normed.astype(jnp.bfloat16).reshape(rows, heads * HEAD_DIM)


def shards(
    tokens, gain, q_att, k_att, v_att, q_ret, k_ret, v_ret, out_att, out_ret, sink, decay_log
):
    parts = lax.axis_size("h")
    own = tokens.shape[0]
    rows = own * parts
    width = tokens.shape[1] * lax.axis_size("tp")
    kv = k_att.shape[1] // HEAD_DIM // parts
    group = q_att.shape[1] // k_att.shape[1]
    att = kv * group
    ret = q_ret.shape[1] // HEAD_DIM // parts
    offset = lax.axis_index("t") * rows
    total_rows = rows * lax.axis_size("t")

    packed = jnp.concatenate(
        [
            w.reshape(w.shape[0], parts, w.shape[1] // parts)
            for w in (q_att, k_att, v_att, q_ret, k_ret, v_ret)
        ],
        axis=2,
    )
    packed = jnp.moveaxis(packed, 1, 0)
    out_pack = jnp.concatenate(
        [w.reshape(parts, w.shape[0] // parts, w.shape[1]) for w in (out_att, out_ret)], axis=1
    )
    widened = tokens.astype(jnp.float32)
    sums = jnp.sum(widened * widened, axis=1)
    scaled = (widened * gain).astype(jnp.bfloat16)
    cores = lax.axis_size("tp")
    flat = packed.reshape(parts * packed.shape[1], packed.shape[2])
    weight = gather(exchange(flat, "h", 0, 0), "t", 0)
    whole = gather(gather(scaled, "h", 0), "tp", 1)
    proj = jnp.dot(whole, weight, preferred_element_type=jnp.float32)
    out_own = exchange(out_pack, "h", 0, 0)
    sums = lax.all_gather(sums, ("h", "tp"))
    decay = exchange(decay_log, "h", 0, 1)
    squares = jnp.sum(sums.reshape(parts, cores, own), axis=1).reshape(rows)
    inverse = lax.rsqrt(squares / width + 1e-06)[:, None]

    edges = [att, kv, kv, ret, ret, ret]
    starts = [sum(edges[:i]) * HEAD_DIM for i in range(6)]
    qa, ka, va, qr, kr, vr = (
        proj[:, s : s + n * HEAD_DIM].reshape(rows, n, HEAD_DIM) for s, n in zip(starts, edges)
    )
    scale = inverse[:, :, None]
    positions = (offset + jnp.arange(rows, dtype=jnp.int32)).astype(jnp.float32)
    freqs = 10000.0 ** (-jnp.arange(0, HEAD_DIM, 2).astype(jnp.float32) / HEAD_DIM)
    angles = positions[:, None] * freqs[None, :]
    cosine, sine = jnp.cos(angles)[:, None, :], jnp.sin(angles)[:, None, :]
    att_query = rotate(qa * scale, cosine, sine)
    att_key = rotate(ka * scale, cosine, sine)
    att_value = (va * scale).astype(jnp.bfloat16)
    ret_query = (qr * scale).astype(jnp.bfloat16)
    ret_key = (kr * (scale * HEAD_DIM ** (-0.5))).astype(jnp.bfloat16)
    ret_value = (vr * scale).astype(jnp.bfloat16)

    logits = lax.dynamic_slice_in_dim(sink, lax.axis_index("h") * att, att).reshape(kv, group)
    att_out, logs = attend(
        att_query.reshape(rows, kv, group, HEAD_DIM), att_key, att_value, logits, offset, total_rows
    )
    ret_out = retain(ret_query, ret_key, ret_value, decay)

    out_wide = gather(out_own, "t", 0)
    mixers = jnp.concatenate([att_out, ret_out], axis=1)
    depth = out_wide.shape[1]
    out_wide = jnp.moveaxis(out_wide, 0, 1).reshape(depth, -1)
    mixed = jnp.dot(mixers, out_wide, preferred_element_type=jnp.float32).astype(jnp.bfloat16)
    mixed = lax.psum_scatter(mixed, ("h", "tp"), scatter_dimension=0, tiled=True)
    return mixed, exchange(logs, "h", 1, 0)


def fits(args, sp, tp):
    tokens, _, q_att, k_att, v_att, q_ret, k_ret, v_ret, out_att, _, _, decay = args
    own, heads = tokens.shape[0] // sp, 4 * tp
    return (
        sp == 16
        and tp == 2
        and own == 2 * SPAN_RADIUS
        and q_att.shape[0] == sp * own
        and tokens.shape[1] == sp * own
        and q_att.shape[1] == 2 * heads * HEAD_DIM
        and all(v.shape[1] == heads * HEAD_DIM for v in (k_att, v_att, q_ret, k_ret, v_ret))
    )


def solution(mesh):
    sp, tp = mesh.shape["sp"], mesh.shape["tp"]

    def run(*args):
        if fits(args, sp, tp):
            seq = ("zh", "zl", "y", "x")
            fine = Mesh(mesh.devices.reshape(2, 2, 2, 2, tp), seq + ("tp",))
            step = fused
        else:
            heads = math.gcd(args[3].shape[1], args[5].shape[1]) // HEAD_DIM
            parts = math.gcd(heads // math.gcd(heads, tp), sp)
            seq = ("t", "h")
            fine = Mesh(mesh.devices.reshape(sp // parts, parts, tp), seq + ("tp",))
            step = shards
        body = jax.shard_map(
            step,
            mesh=fine,
            in_specs=(P(seq, "tp"), P("tp"))
            + (P(seq, "tp"),) * 6
            + (P("tp", seq), P("tp", seq), P("tp"), P("tp", seq)),
            out_specs=(P(seq + ("tp",), None), P("tp", seq)),
            check_vma=False,
        )
        return body(*args)

    return run
```

```python
import math

import jax
import jax.numpy as jnp
import numpy as np
from jax import lax
from jax.experimental import pallas as pl
from jax.experimental.pallas import tpu as pltpu
from jax.sharding import Mesh
from jax.sharding import PartitionSpec as P

HEAD_DIM = 128
SPAN_RADIUS = 128
BLOCK = 256
HIGHEST = lax.Precision.HIGHEST
MESH = pl.DeviceIdType.MESH


def gather(x, axis, dim):
    if lax.axis_size(axis) == 1:
        return x
    return lax.all_gather(x, axis, axis=dim, tiled=True)


def exchange(x, axis, split, concat):
    if lax.axis_size(axis) == 1:
        return x
    return lax.all_to_all(x, axis, split, concat, tiled=True)


def halo(shard, axis, width):
    peers, length = lax.axis_size(axis), shard.shape[1]
    up = [(i, i + 1) for i in range(peers - 1)]
    down = [(j, i) for i, j in up]
    before = lax.ppermute(shard[:, length - width :], axis, up)
    after = lax.ppermute(shard[:, :width], axis, down)
    return jnp.concatenate([before, shard, after], axis=1)


def rotate(values, cosine, sine):
    half = values.shape[-1] // 2
    first, second = values[..., :half], values[..., half:]
    return jnp.concatenate(
        [first * cosine - second * sine, second * cosine + first * sine], axis=-1
    ).astype(jnp.bfloat16)


class Stream:
    def __init__(self, where, remote, refs, pack):
        self.where, self.remote, self.pack = where, remote, pack
        (
            self.wide, self.away, self.out,
            self.load, self.x_send, self.z_send, self.h_send, self.y_send,
            self.p_recv, self.w_recv,
        ) = refs

    def fetch(self):
        w = self.where
        targets = (
            (self.out.at[0], 1 - w.g, 1 - w.x),
            (self.out.at[1], w.g, 1 - w.x),
            (self.wide.at[w.own], w.g, w.x),
            (self.away.at[w.x], 1 - w.g, w.x),
        )
        for i, (target, g, x) in enumerate(targets):
            self.pack(2 * g + x, target, self.load.at[i])

    def fetched(self):
        w = self.where
        for i, target in enumerate(
            (self.out.at[0], self.out.at[1], self.wide.at[w.own], self.away.at[w.x])
        ):
            pltpu.make_async_copy(target, target, self.load.at[i]).wait()

    def along_x(self, k):
        w = self.where
        if k == 0:
            return self.remote(
                self.out.at[0], self.away.at[w.x], self.x_send.at[0], self.p_recv.at[0], w.to_x
            )
        return self.remote(
            self.out.at[1], self.wide.at[w.own], self.x_send.at[1], self.w_recv.at[w.own], w.to_x
        )

    def along_z(self, k):
        w = self.where
        x = w.x if k == 0 else 1 - w.x
        s = w.at(w.zh, w.zl, w.y, x)
        return self.remote(
            self.away.at[x], self.wide.at[s], self.z_send.at[k], self.w_recv.at[s], w.to_z
        )

    def near(self, k):
        w = self.where
        return w.at(w.zh, (w.zl, 1 - w.zl)[k // 2], w.y, (w.x, 1 - w.x)[k % 2])

    def far(self, k):
        w = self.where
        return w.at(1 - w.zh, (w.zl, 1 - w.zl)[1 - k // 2], w.y, (w.x, 1 - w.x)[k % 2])

    def along_h(self, k):
        s = self.near(k)
        return self.remote(
            self.wide.at[s], self.wide.at[s], self.h_send.at[k], self.w_recv.at[s], self.where.to_h
        )

    def along_y(self, k):
        s = self.near(k) if k < 4 else self.far(k - 4)
        return self.remote(
            self.wide.at[s], self.wide.at[s], self.y_send.at[k], self.w_recv.at[s], self.where.to_y
        )

    def arrive(self, s):
        self.remote(
            self.wide.at[s], self.wide.at[s], self.x_send.at[0], self.w_recv.at[s], self.where.to_x
        ).wait_recv()

    def arrive_away(self):
        w = self.where
        slot = self.away.at[1 - w.x]
        self.remote(slot, slot, self.x_send.at[0], self.p_recv.at[0], w.to_x).wait_recv()

    def arrive_across(self):
        w = self.where
        for zh in (w.zh, 1 - w.zh):
            for zl in range(2):
                for x in range(2):
                    self.arrive(w.at(zh, zl, 1 - w.y, x))

    def drain(self):
        for k in range(2):
            self.along_x(k).wait_send()
            self.along_z(k).wait_send()
        for k in range(4):
            self.along_h(k).wait_send()
        for k in range(8):
            self.along_y(k).wait_send()


class Place:
    def __init__(self):
        self.zh, self.zl, self.y, self.x, self.c = (
            lax.axis_index(a) for a in ("zh", "zl", "y", "x", "tp")
        )
        self.g = lax.rem(self.zh + self.zl, 2)
        self.h = 2 * self.g + self.x
        self.own = self.at(self.zh, self.zl, self.y, self.x)
        self.b = 2 * self.zl + self.x
        self.to_x = {"x": 1 - self.x}
        self.to_z = {"zl": 1 - self.zl}
        self.to_y = {"y": 1 - self.y}
        self.to_h = {"zh": 1 - self.zh, "zl": 1 - self.zl}
        self.to_hy = {"zh": 1 - self.zh, "zl": 1 - self.zl, "y": 1 - self.y}
        self.to_zx = {"zl": 1 - self.zl, "x": 1 - self.x}
        self.to_c = {"tp": 1 - self.c}

    @staticmethod
    def at(zh, zl, y, x):
        return ((zh * 2 + zl) * 2 + y) * 2 + x


def fused_kernel(
    tokens, gain, q_att, k_att, v_att, q_ret, k_ret, v_ret, out_att, out_ret, sink, decay,
    cos_t, sin_t, base,
    mixed, logs_out,
    raw, scl, ssq, gains, proj, kvext, qrot, rets, dec, cumr, cumc, coef, states, stall,
    mix, logm, lsend, lrecv, mine, give, take, s1, r1, s2, r2,
    t_load, t_x, t_z, t_c, t_recv, g_sem, d_sem, halo_sem, st_sem, l_sem,
    give_s, take_r, s1_s, r1_r, s2_s, r2_r,
    *streams,
):
    w = Place()
    f32, bf16 = jnp.float32, jnp.bfloat16
    own, half_d = tokens.shape
    rows = 4 * own
    run_rows = 2 * own
    total_rows = 16 * own
    H = HEAD_DIM
    edge = SPAN_RADIUS

    def remote(src, dst, send, recv, to):
        return pltpu.make_async_remote_copy(
            src_ref=src, dst_ref=dst, send_sem=send, recv_sem=recv,
            device_id=to, device_id_type=MESH,
        )

    def lanes(h, n):
        return pl.ds(pl.multiple_of(h * n, n), n)

    def pack_cols(parts):
        def pack(h, target, sem):
            start = 0
            for ref in parts:
                n = ref.shape[1] // 4
                pltpu.make_async_copy(
                    ref.at[:, lanes(h, n)], target.at[:, pl.ds(start, n)], sem
                ).start()
                start += n
        return pack

    def pack_rows(parts):
        def pack(h, target, sem):
            start = 0
            for ref in parts:
                n = ref.shape[0] // 4
                pltpu.make_async_copy(
                    ref.at[lanes(h, n), :], target.at[pl.ds(start, n), :], sem
                ).start()
                start += n
        return pack

    n = len(streams) // 3
    A = Stream(w, remote, streams[:n], pack_cols((q_att, k_att, v_att)))
    R = Stream(w, remote, streams[n : 2 * n], pack_cols((q_ret, k_ret, v_ret)))
    O = Stream(w, remote, streams[2 * n :], pack_rows((out_att, out_ret)))

    token_load = pltpu.make_async_copy(tokens, raw.at[w.c, w.b], t_load.at[0])
    gain_load = pltpu.make_async_copy(gain, gains.at[w.c], t_load.at[1])
    decay_load = pltpu.make_async_copy(decay, dec.at[w.zh, w.y, w.zl, w.x], t_load.at[2])

    def block(zl, x):
        return 2 * zl + x

    def token(b, send, to):
        here = raw.at[w.c, b]
        return remote(here, here, send, t_recv.at[w.c, b], to)

    tokens_x = (
        token(w.b, t_x.at[0], w.to_x),
        token(block(1 - w.zl, w.x), t_x.at[1], w.to_x),
    )
    tokens_z = token(w.b, t_z.at[0], w.to_z)

    def tokens_c(k):
        b = block((w.zl, 1 - w.zl)[k // 2], (w.x, 1 - w.x)[k % 2])
        return token(b, t_c.at[k], w.to_c)

    def token_arrive(k, e=None):
        b = block((w.zl, 1 - w.zl)[k // 2], (w.x, 1 - w.x)[k % 2])
        e = w.c if e is None else e
        here = raw.at[e, b]
        remote(here, here, t_x.at[0], t_recv.at[e, b], w.to_x).wait_recv()

    gain_c = remote(gains.at[w.c], gains.at[w.c], g_sem.at[0], g_sem.at[1], w.to_c)

    def flip(v, bit):
        return v + bit - 2 * v * bit

    def others(i):
        return tuple(flip(v, (i >> k) & 1) for v, k in ((w.zh, 3), (w.zl, 2), (w.y, 1), (w.x, 0)))

    def decay_send(i):
        zh, zl, y, x = others(i)
        here = dec.at[w.zh, w.y, w.zl, w.x]
        to = {"zh": zh, "zl": zl, "y": y, "x": x}
        return remote(here, here, d_sem.at[0, i], d_sem.at[1, i], to)

    def decay_arrive(i):
        zh, zl, y, x = others(i)
        here = dec.at[zh, y, zl, x]
        to = {"zh": zh, "zl": zl, "y": y, "x": x}
        remote(here, here, d_sem.at[0, i], d_sem.at[1, i], to).wait_recv()

    decay_load.start()
    A.fetch()
    gain_load.start()
    token_load.start()
    R.fetch()
    O.fetch()

    barrier = pltpu.get_barrier_semaphore()
    pl.semaphore_signal(barrier, inc=1, device_id=w.to_c, device_id_type=MESH)
    for i in range(1, 16):
        zh, zl, y, x = others(i)
        to = {"zh": zh, "zl": zl, "y": y, "x": x}
        pl.semaphore_signal(barrier, inc=1, device_id=to, device_id_type=MESH)
    pl.semaphore_wait(barrier, 16)

    middle = w.g == 1

    decay_load.wait()
    for i in range(1, 16):
        decay_send(i).start()
    A.fetched()
    A.along_x(0).start()
    A.along_z(0).start()
    A.along_y(0).start()
    R.fetched()
    R.along_x(0).start()
    R.along_z(0).start()
    R.along_y(0).start()
    A.along_x(1).start()
    R.along_x(1).start()

    @pl.when(middle)
    def _():
        A.along_h(0).start()
        R.along_h(0).start()

    gain_load.wait()
    gain_c.start()
    token_load.wait()
    tokens_x[0].start()
    tokens_c(0).start()

    def scale(e, b):
        @pl.loop(0, own // 16)
        def _(i):
            value = raw[e, b, pl.ds(pl.multiple_of(i * 16, 16), 16), :].astype(f32)
            at = pl.ds(pl.multiple_of(b * own + i * 16, 16), 16)
            scl[e, at, :] = (value * gains[e]).astype(bf16)
            square = value * value
            total = square[:, :H]
            for k in range(1, half_d // H):
                total = total + square[:, k * H : (k + 1) * H]
            ssq[e, at, :] = total

    @pl.when((w.zh == 0) & (w.y == 0))
    def _():
        kvext[0, :, 0:edge, :] = jnp.zeros((2, edge, H), bf16)

    @pl.when((w.zh == 1) & (w.y == 1))
    def _():
        kvext[1, :, edge + run_rows :, :] = jnp.zeros((2, edge, H), bf16)

    scale(w.c, w.b)
    A.arrive_away()
    A.along_z(1).start()
    R.arrive_away()
    R.along_z(1).start()
    tokens_z.start()
    remote(gains.at[1 - w.c], gains.at[1 - w.c], g_sem.at[0], g_sem.at[1], w.to_c).wait_recv()
    token_arrive(0, 1 - w.c)
    scale(1 - w.c, w.b)
    for k in (2, 1, 3):
        for stream in (A, R):
            stream.arrive(stream.near(k))
            stream.along_y(k).start()

            @pl.when(middle)
            def _():
                stream.along_h(k).start()

    @pl.when(w.g == 0)
    def _():
        for k in range(4):
            A.along_h(k).start()
        for k in range(4):
            R.along_h(k).start()

    for i in range(1, 16):
        decay_arrive(i)

    lane = lax.broadcasted_iota(jnp.int32, (8, run_rows), 1)
    for slot in range(2):
        row = jnp.concatenate(
            [dec[w.zh, w.y, slot, x, pl.ds(w.h, 1), :] for x in range(2)], axis=1
        )
        row = jnp.broadcast_to(row, (8, run_rows))
        step = 1
        while step < run_rows:
            row = row + jnp.where(lane >= step, pltpu.roll(row, step, axis=1), 0.0)
            step *= 2
        cumr[slot] = row
        cumc[slot] = jnp.transpose(jnp.broadcast_to(row[0:1], (H, run_rows)))
    lane = lax.broadcasted_iota(jnp.int32, (8, H), 1)
    run = lax.broadcasted_iota(jnp.int32, (8, H), 0)
    totals = jnp.zeros((8, H), f32)
    for zh in range(2):
        for slot in range(2):
            for y in range(2):
                pair = sum(dec[zh, y, slot, x, pl.ds(w.h, 1), :] for x in range(2))
                value = jnp.sum(pair, axis=1, keepdims=True)
                totals = jnp.where(lane == 4 * zh + 2 * slot + y, value, totals)
    for slot in range(2):
        me = 4 * w.zh + 2 * slot + w.y
        between = (lane > jnp.minimum(run, me)) & (lane < jnp.maximum(run, me))
        factor = jnp.exp(jnp.sum(jnp.where(between, totals, 0.0), axis=1, keepdims=True))
        factor = jnp.broadcast_to(factor, (8, H))
        coef[slot, 0] = jnp.where(run < me, factor, 0.0)
        coef[slot, 1] = jnp.where(run > me, factor, 0.0)

    token_arrive(2)
    tokens_x[1].start()
    tokens_c(2).start()
    token_arrive(1)
    tokens_c(1).start()
    O.fetched()
    O.along_x(0).start()
    O.along_x(1).start()
    for k in (2, 1):
        b = block((w.zl, 1 - w.zl)[k // 2], (w.x, 1 - w.x)[k % 2])
        scale(w.c, b)
    for k in (2, 1):
        b = block((w.zl, 1 - w.zl)[k // 2], (w.x, 1 - w.x)[k % 2])
        token_arrive(k, 1 - w.c)
        scale(1 - w.c, b)
    for k in range(4):
        A.arrive(A.far(k))
        A.along_y(4 + k).start()

    def pass_far(stream, k):
        stream.arrive(stream.far(k))
        stream.along_y(4 + k).start()

    @pl.when(middle)
    def _():
        for k in range(4):
            pass_far(R, k)

    token_arrive(3)
    tokens_c(3).start()
    b3 = block(1 - w.zl, 1 - w.x)
    scale(w.c, b3)
    token_arrive(3, 1 - w.c)
    scale(1 - w.c, b3)
    O.along_z(0).start()
    A.arrive_across()

    def project(stream, b, start, width):
        at = pl.ds(pl.multiple_of(b * own, own), own)
        depth = half_d // own
        first = stream.wide[0:depth, :, start : start + width].reshape(half_d, width)
        second = stream.wide[depth : 2 * depth, :, start : start + width].reshape(half_d, width)
        value = jnp.dot(scl[0, at, :], first, preferred_element_type=f32)
        return value + jnp.dot(scl[1, at, :], second, preferred_element_type=f32)

    def inverse(b):
        at = pl.ds(pl.multiple_of(b * own, own), own)
        squares = jnp.sum(ssq[0, at, :] + ssq[1, at, :], axis=1, keepdims=True)
        return lax.rsqrt(squares / (2 * half_d) + 1e-06)

    def angles(b):
        s = w.at(w.zh, b // 2, w.y, b % 2)
        c0, s0, s0n, c0n = (base[i, pl.ds(s, 1), :] for i in range(4))
        cosine = cos_t[...] * c0 - sin_t[...] * s0
        sine = cos_t[...] * s0n + sin_t[...] * c0n
        return cosine, sine

    def turn(value, cosine, sine):
        return (value * cosine + pltpu.roll(value, H // 2, axis=1) * sine).astype(bf16)

    def attention_inputs(b):
        at = pl.ds(pl.multiple_of(b * own, own), own)
        scale_b = inverse(b)
        cosine, sine = angles(b)
        query = project(A, b, 0, 2 * H) * scale_b
        qrot[at, :H] = turn(query[:, :H], cosine, sine)
        qrot[at, H:] = turn(query[:, H:], cosine, sine)
        other = project(A, b, 2 * H, 2 * H) * scale_b
        inner = pl.ds(pl.multiple_of(edge + (b % 2) * own, edge), own)
        kvext[b // 2, 0, inner, :] = turn(other[:, :H], cosine, sine)
        kvext[b // 2, 1, inner, :] = other[:, H:].astype(bf16)

    @pl.loop(0, 4)
    def _(b):
        attention_inputs(b)

    y = w.y
    head, tail, before_at, after_at = edge, run_rows, 0, edge + run_rows

    def pick(a, b):
        return a + (b - a) * y

    def piece(slot, start):
        return kvext.at[slot, :, pl.ds(pl.multiple_of(start, edge), edge), :]

    halo_y = [
        remote(
            piece(pick(s0, s1), pick(f0, f1)), piece(pick(d0, d1), pick(o0, o1)),
            halo_sem.at[0, i], halo_sem.at[1, i], w.to_y,
        )
        for i, (s0, f0, d0, o0, s1, f1, d1, o1) in enumerate(
            (
                (0, tail, 0, before_at, 0, head, 0, after_at),
                (1, head, 0, after_at, 0, tail, 1, before_at),
                (1, tail, 1, before_at, 1, head, 1, after_at),
            )
        )
    ]
    halo_far = remote(
        piece(pick(0, 1), pick(head, tail)), piece(pick(1, 0), pick(after_at, before_at)),
        halo_sem.at[0, 3], halo_sem.at[1, 3], w.to_hy,
    )
    has_far = ((y == 0) & (w.zh == 1)) | ((y == 1) & (w.zh == 0))
    for copy in halo_y:
        copy.start()

    @pl.when(has_far)
    def _():
        halo_far.start()

    @pl.when(w.g == 0)
    def _():
        for k in range(4):
            pass_far(R, k)

    O.along_y(0).start()
    O.along_h(0).start()
    O.arrive_away()
    O.along_z(1).start()

    def halo_arrive(slot, start, i, to):
        here = piece(slot, start)
        remote(here, here, halo_sem.at[0, i], halo_sem.at[1, i], to).wait_recv()

    halo_arrive(pick(0, 0), pick(after_at, before_at), 0, w.to_y)
    halo_arrive(pick(1, 0), pick(before_at, after_at), 1, w.to_y)
    halo_arrive(pick(1, 1), pick(after_at, before_at), 2, w.to_y)

    @pl.when(has_far)
    def _():
        halo_arrive(pick(0, 1), pick(before_at, after_at), 3, w.to_hy)

    def attend_tile(i):
        slot, j = i // 4, i % 4
        query = qrot[pl.ds(pl.multiple_of(i * edge, edge), edge), :]
        query = jnp.concatenate([query[:, :H], query[:, H:]], axis=0)
        span = pl.ds(pl.multiple_of(j * edge, edge), 3 * edge)
        key, value = kvext[slot, 0, span, :], kvext[slot, 1, span, :]
        score = lax.dot_general(
            query, key, (((1,), (1,)), ((), ())), preferred_element_type=f32
        ) * H ** (-0.5)
        row = lax.broadcasted_iota(jnp.int32, score.shape, 0)
        col = lax.broadcasted_iota(jnp.int32, score.shape, 1)
        shift = col - jnp.where(row < edge, row, row - edge)
        start = w.at(w.zh, slot, y, 0) * own + j * edge - edge
        valid = (
            (shift >= 0) & (shift <= 2 * edge) & (col >= -start) & (col < total_rows - start)
        )
        masked = jnp.where(valid, score, -jnp.inf)
        first = lax.broadcasted_iota(jnp.int32, (2 * edge, 1), 0) < edge
        limit = jnp.where(first, sink[2 * w.h], sink[2 * w.h + 1])
        top = jnp.maximum(jnp.max(masked, axis=1, keepdims=True), limit)
        expo = jnp.exp(masked - top)
        total = jnp.sum(expo, axis=1, keepdims=True) + jnp.exp(limit - top)
        logs = top + jnp.log(total)
        probs = (expo * (1.0 / total)).astype(bf16)
        result = jnp.dot(probs, value, preferred_element_type=f32).astype(bf16)
        at = pl.ds(pl.multiple_of((i // 2) * edge, edge), edge)
        mix[i % 2, at, 0:H] = result[:edge]
        mix[i % 2, at, H : 2 * H] = result[edge:]
        column = lax.broadcasted_iota(jnp.int32, (2 * edge, H), 1)
        logm[...] = jnp.where(column == i, logs, logm[...])

    logm[...] = jnp.zeros_like(logm)

    @pl.loop(0, 4)
    def _(i):
        attend_tile(i)

    for k in (2, 1, 3):
        O.arrive(O.near(k))
        O.along_y(k).start()

        @pl.when(middle)
        def _():
            O.along_h(k).start()

    @pl.loop(4, 8)
    def _(i):
        attend_tile(i)

    turned = jnp.transpose(logm[...])
    for b in range(4):
        lsend[b] = turned[2 * b : 2 * b + 2]
        lrecv[w.h] = jnp.where(w.b == b, turned[2 * b : 2 * b + 2], lrecv[w.h] if b else 0.0)
    h_of = lambda zl, x: 2 * lax.rem(w.zh + zl, 2) + x
    log_to = (
        (1 - w.x, w.zl, w.to_x), (w.x, 1 - w.zl, w.to_z), (1 - w.x, 1 - w.zl, w.to_zx),
    )
    log_sends = [
        remote(lsend.at[block(zl, x)], lrecv.at[w.h], l_sem.at[0, i], l_sem.at[1, i], to)
        for i, (x, zl, to) in enumerate(log_to)
    ]

    R.arrive_across()

    def retention_inputs(b):
        at = pl.ds(pl.multiple_of(b * own, own), own)
        scale_b = inverse(b)
        both = project(R, b, 0, 2 * H)
        rets[0, at, :] = (both[:, :H] * scale_b).astype(bf16)
        rets[1, at, :] = (both[:, H:] * (scale_b * H ** (-0.5))).astype(bf16)
        rets[2, at, :] = (project(R, b, 2 * H, H) * scale_b).astype(bf16)

    @pl.loop(0, 4)
    def _(b):
        retention_inputs(b)

    for slot in range(2):
        at = pl.ds(slot * run_rows, run_rows)
        last = cumr[slot, 0:1, run_rows - 1 : run_rows]
        key, value = rets[1, at, :].astype(f32), rets[2, at, :]
        for i, weight in enumerate((jnp.exp(last - cumc[slot]), jnp.exp(cumc[slot]))):
            lhs = (key * weight).astype(bf16)
            state = lax.dot_general(
                lhs, value, (((0,), (0,)), ((), ())), preferred_element_type=f32
            ).astype(bf16)
            stall[w.zh, w.y, slot, i] = state
    state_sends = [
        remote(
            stall.at[w.zh, w.y], stall.at[w.zh, w.y], st_sem.at[0, i], st_sem.at[1, i], to
        )
        for i, to in enumerate((w.to_y, w.to_h, w.to_hy))
    ]
    for copy in state_sends:
        copy.start()
    for copy in log_sends:
        copy.start()

    @pl.when(w.g == 0)
    def _():
        for k in range(1, 4):
            O.along_h(k).start()

    def inner_tile(i):
        slot = i // 2
        at = pl.ds(pl.multiple_of(i * own, own), own)
        keys = pl.ds(pl.multiple_of(slot * run_rows, run_rows), run_rows)
        score = lax.dot_general(
            rets[0, at, :], rets[1, keys, :], (((1,), (1,)), ((), ())),
            preferred_element_type=f32,
        )
        column = cumc[slot, pl.ds(pl.multiple_of((i % 2) * own, own), own), :]
        column = jnp.concatenate([column] * (run_rows // H), axis=1)
        weight = jnp.exp(-jnp.abs(column - cumr[slot, 0:1, :]))
        proj[at, :] = jnp.dot(
            (score * weight).astype(bf16), rets[2, keys, :], preferred_element_type=f32
        )

    @pl.loop(0, 4)
    def _(i):
        inner_tile(i)

    for i, (zh, yy) in enumerate(((w.zh, 1 - y), (1 - w.zh, y), (1 - w.zh, 1 - y))):
        here = stall.at[zh, yy]
        remote(here, here, st_sem.at[0, i], st_sem.at[1, i], w.to_y).wait_recv()
    for slot in range(2):
        for i in range(2):
            total = jnp.zeros((H, H), f32)
            for zh in range(2):
                for s in range(2):
                    for yy in range(2):
                        r = 4 * zh + 2 * s + yy
                        total = total + coef[slot, i, r : r + 1, :] * stall[
                            zh, yy, s, i
                        ].astype(f32)
            states[slot, :, i * H : (i + 1) * H] = total.astype(bf16)

    def finish_tile(i):
        slot = i // 2
        at = pl.ds(pl.multiple_of(i * own, own), own)
        column = cumc[slot, pl.ds(pl.multiple_of((i % 2) * own, own), own), :]
        last = cumr[slot, 0:1, run_rows - 1 : run_rows]
        carried = jnp.dot(rets[0, at, :], states[slot], preferred_element_type=f32)
        value = (
            proj[at, :] + jnp.exp(column) * carried[:, :H]
            + jnp.exp(last - column) * carried[:, H:]
        )
        value = value - jnp.mean(value, axis=1, keepdims=True)
        value = value * lax.rsqrt(jnp.mean(value * value, axis=1, keepdims=True) + 1e-06)
        value = value.astype(bf16)
        out = pl.ds(pl.multiple_of(i * edge, edge), edge)
        mix[0, out, 2 * H :] = value[:edge]
        mix[1, out, 2 * H :] = value[edge:]

    @pl.loop(0, 4)
    def _(i):
        finish_tile(i)

    for k in range(4):
        pass_far(O, k)

    chunks = 8

    def columns_of(i, x):
        a, far, zl = i // 4, (i // 2) % 2, i % 2
        yy = a + y - 2 * a * y
        zh = far + w.zh - 2 * far * w.zh
        return w.at(zh, zl, yy, x)

    def swap(i):
        return remote(give.at[i], take.at[i], give_s.at[i], take_r.at[i], w.to_c)

    def first_hop(i):
        return (
            remote(s1.at[i, 0], r1.at[i, 0], s1_s.at[i, 0], r1_r.at[i, 0], w.to_x),
            remote(s1.at[i, 1], r1.at[i, 1], s1_s.at[i, 1], r1_r.at[i, 1], w.to_z),
        )

    def second_hop(i):
        return (
            remote(s2.at[i, 0], r2.at[i, 0], s2_s.at[i, 0], r2_r.at[i, 0], w.to_z),
            remote(s2.at[i, 1], r2.at[i, 1], s2_s.at[i, 1], r2_r.at[i, 1], w.to_x),
        )

    def part(b):
        return pl.ds(pl.multiple_of(b * edge, edge), edge)

    @pl.loop(0, chunks + 3)
    def _(step):
        @pl.when(step < chunks)
        def _():
            i = step

            @pl.when(i >= chunks // 2)
            def _():
                for x in range(2):
                    O.arrive(columns_of(i, x))

            for k in range(2):
                give[i, k] = jnp.dot(
                    mix[1 - w.c], O.wide[columns_of(i, k)], preferred_element_type=f32
                ).astype(bf16)
            swap(i).start()
            for k in range(2):
                mine[i, k] = jnp.dot(
                    mix[w.c], O.wide[columns_of(i, k)], preferred_element_type=f32
                )

        @pl.when((step >= 1) & (step < chunks + 1))
        def _():
            i = step - 1
            swap(i).wait_recv()
            for k in range(2):
                for j in range(2):
                    b = block(j, 1 - w.x) if k == 0 else block(1 - w.zl, j)
                    total = mine[i, k, part(b), :] + take[i, k, part(b), :].astype(f32)
                    s1[i, k, j] = total.astype(bf16)
            for copy in first_hop(i):
                copy.start()
            for k in range(2):
                for j in range(2):
                    b = block(j, w.x) if k == 0 else block(w.zl, j)
                    mine[i, k, part(b), :] += take[i, k, part(b), :].astype(f32)

        @pl.when((step >= 2) & (step < chunks + 2))
        def _():
            i = step - 2
            for k, copy in enumerate(first_hop(i)):
                copy.wait_recv()
                b = block(1 - w.zl, w.x) if k == 0 else block(w.zl, 1 - w.x)
                j = 1 - w.zl if k == 0 else 1 - w.x
                s2[i, k] = (mine[i, k, part(b), :] + r1[i, k, j].astype(f32)).astype(bf16)
                second_hop(i)[k].start()
            for k in range(2):
                j = w.zl if k == 0 else w.x
                mine[i, k, part(w.b), :] += r1[i, k, j].astype(f32)

        @pl.when(step >= 3)
        def _():
            i = step - 3
            for k, copy in enumerate(second_hop(i)):
                copy.wait_recv()
                at = pl.ds(pl.multiple_of(columns_of(i, k) * own, own), own)
                total = mine[i, k, part(w.b), :] + r2[i, k].astype(f32)
                mixed[:, at] = total.astype(mixed.dtype)

    for i, (x, zl, to) in enumerate(log_to):
        here = lrecv.at[h_of(zl, x)]
        remote(here, here, l_sem.at[0, i], l_sem.at[1, i], to).wait_recv()
    for h in range(4):
        for head_i in range(2):
            for t in range(2):
                logs_out[2 * h + head_i : 2 * h + head_i + 1, t * edge : (t + 1) * edge] = (
                    lrecv[h, t : t + 1, head_i * edge : (head_i + 1) * edge]
                )

    for stream in (A, R, O):
        stream.drain()
    for k in range(4):
        tokens_c(k).wait_send()
    for i in range(1, 16):
        decay_send(i).wait_send()
    for copy in tokens_x + (tokens_z, gain_c):
        copy.wait_send()
    for copy in halo_y + state_sends + log_sends:
        copy.wait_send()

    @pl.when(has_far)
    def _():
        halo_far.wait_send()

    @pl.loop(0, chunks)
    def _(i):
        swap(i).wait_send()
        for copy in first_hop(i) + second_hop(i):
            copy.wait_send()


def fused(*args):
    tokens, gain, q_att = args[:3]
    out_att, out_ret, sink, decay_log = args[8:]
    own, half_d = tokens.shape
    rows, run_rows = 4 * own, 2 * own
    H, edge = HEAD_DIM, SPAN_RADIUS
    bf16, f32 = jnp.bfloat16, jnp.float32
    dma, vmem = pltpu.SemaphoreType.DMA, pltpu.VMEM
    depth = q_att.shape[0]
    width = out_att.shape[1] * 16

    freqs = 10000.0 ** (-np.arange(0, H, 2, dtype=np.float64) / H)
    freqs = np.concatenate([freqs, freqs])[None, :]
    sign = np.where(np.arange(H) < H // 2, -1.0, 1.0)[None, :]
    inner = np.arange(own)[:, None] * freqs
    outer = (np.arange(16) * own)[:, None] * freqs
    cos_t, sin_t = jnp.asarray(np.cos(inner), f32), jnp.asarray(np.sin(inner), f32)
    base = jnp.asarray(
        np.stack([np.cos(outer), np.sin(outer), sign * np.sin(outer), sign * np.cos(outer)]), f32
    )

    def stream(block):
        return [
            vmem((16,) + block, bf16), vmem((2,) + block, bf16), vmem((2,) + block, bf16),
            dma((4,)), dma((2,)), dma((2,)), dma((4,)), dma((8,)), dma((1,)), dma((16,)),
        ]

    out_rows = (out_att.shape[0] + out_ret.shape[0]) // 4
    tile = (8, 2, 4 * edge, own)
    hbm, inside = pl.BlockSpec(memory_space=pl.ANY), pl.BlockSpec(memory_space=pltpu.VMEM)
    return pl.pallas_call(
        fused_kernel,
        out_shape=(
            jax.ShapeDtypeStruct((own // 2, width), bf16),
            jax.ShapeDtypeStruct((sink.shape[0], own), f32),
        ),
        in_specs=[hbm] * 10 + [pl.BlockSpec(memory_space=pltpu.SMEM), hbm] + [inside] * 3,
        out_specs=[inside] * 2,
        scratch_shapes=[
            vmem((2, 4, own, half_d), bf16),
            vmem((2, rows, half_d), bf16),
            vmem((2, rows, H), f32),
            vmem((2, 1, half_d), f32),
            vmem((rows, H), f32),
            vmem((2, 2, run_rows + 2 * edge, H), bf16),
            vmem((rows, 2 * H), bf16),
            vmem((3, rows, H), bf16),
            vmem((2, 2, 2, 2) + decay_log.shape, f32),
            vmem((2, 8, run_rows), f32),
            vmem((2, run_rows, H), f32),
            vmem((2, 2, 8, H), f32),
            vmem((2, H, 2 * H), bf16),
            vmem((2, 2, 2, 2, H, H), bf16),
            vmem((2, 4 * edge, 3 * H), bf16),
            vmem((2 * edge, H), f32),
            vmem((4, 2, 2 * edge), f32),
            vmem((4, 2, 2 * edge), f32),
            vmem(tile, f32), vmem(tile, bf16), vmem(tile, bf16),
            vmem((8, 2, 2, edge, own), bf16), vmem((8, 2, 2, edge, own), bf16),
            vmem((8, 2, edge, own), bf16), vmem((8, 2, edge, own), bf16),
            dma((3,)), dma((2,)), dma((1,)), dma((4,)), dma((2, 4)), dma((2,)), dma((2, 16)),
            dma((2, 4)), dma((2, 3)), dma((2, 3)),
            dma((8,)), dma((8,)), dma((8, 2)), dma((8, 2)), dma((8, 2)), dma((8, 2)),
        ]
        + stream((depth, 4 * H))
        + stream((depth, 3 * H))
        + stream((out_rows, own)),
        compiler_params=pltpu.CompilerParams(
            collective_id=0, has_side_effects=True, vmem_limit_bytes=67043328
        ),
        cost_estimate=pl.CostEstimate(
            flops=10**11, bytes_accessed=2 * 10**7, transcendentals=0
        ),
    )(
        tokens, gain.reshape(1, half_d), *args[2:10], sink, decay_log, cos_t, sin_t, base
    )


def attend(query, key, value, sink, offset, total_rows):
    rows, kv, group, _ = query.shape
    ext = halo(jnp.stack([key, value]), "t", SPAN_RADIUS)
    size = min(rows, BLOCK)
    count = rows // size
    span = size + 2 * SPAN_RADIUS
    pieces = jnp.stack([ext[:, b * size : b * size + span] for b in range(count)])
    blocks = query.reshape(count, size, kv, group, HEAD_DIM)
    scores = jnp.einsum(
        "bqhgd,bkhd->bhgqk", blocks, pieces[:, 0], preferred_element_type=jnp.float32
    ) * HEAD_DIM ** (-0.5)
    base = offset + jnp.arange(count, dtype=jnp.int32) * size
    query_pos = base[:, None] + jnp.arange(size, dtype=jnp.int32)
    key_pos = base[:, None] - SPAN_RADIUS + jnp.arange(span, dtype=jnp.int32)
    spacing = key_pos[:, None, :] - query_pos[:, :, None]
    inside = (key_pos >= 0) & (key_pos < total_rows)
    valid = (jnp.abs(spacing) <= SPAN_RADIUS) & inside[:, None, :]
    masked = jnp.where(valid[:, None, None], scores, -jnp.inf)
    limit = sink[None, :, :, None]
    top = jnp.maximum(jnp.max(masked, axis=-1), limit)
    expo = jnp.exp(masked - top[..., None])
    total = jnp.sum(expo, axis=-1) + jnp.exp(limit - top)
    logs = top + jnp.log(total)
    probs = (expo / total[..., None]).astype(jnp.bfloat16)
    result = jnp.einsum(
        "bhgqk,bkhd->bqhgd", probs, pieces[:, 1], preferred_element_type=jnp.float32
    ).astype(jnp.bfloat16)
    logs = jnp.transpose(logs, (1, 2, 0, 3)).reshape(kv * group, rows)
    return result.reshape(rows, kv * group * HEAD_DIM), logs


def retain(query, key, value, decay):
    rows, heads, _ = query.shape
    peers, index = lax.axis_size("t"), lax.axis_index("t")
    cumul = jnp.cumsum(decay, axis=1)
    last = cumul[:, -1]
    query_f, key_f, value_f = (v.astype(jnp.float32) for v in (query, key, value))
    trailing = jnp.exp(last[:, None] - cumul)
    leading = jnp.exp(cumul)
    forward = jnp.einsum("hk,khd,khe->hde", trailing, key_f, value_f, precision=HIGHEST)
    backward = jnp.einsum("hk,khd,khe->hde", leading, key_f, value_f, precision=HIGHEST)
    tail = jnp.broadcast_to(last[:, None, None], (heads, 8, HEAD_DIM))
    sent = jnp.concatenate([forward, backward, tail], axis=1)
    seen = lax.all_gather(sent, "t", axis=0)
    lasts = seen[:, :, 2 * HEAD_DIM, 0]
    at = jnp.arange(peers)
    low = jnp.minimum(at, index)[:, None]
    high = jnp.maximum(at, index)[:, None]
    between = (at[None, :] > low) & (at[None, :] < high)
    spans = jnp.exp(jnp.sum(jnp.where(between[:, :, None], lasts[None], 0.0), axis=1))
    before = jnp.sum(
        jnp.where(at < index, 1.0, 0.0)[:, None, None, None]
        * spans[:, :, None, None]
        * seen[:, :, :HEAD_DIM],
        axis=0,
    )
    after = jnp.sum(
        jnp.where(at > index, 1.0, 0.0)[:, None, None, None]
        * spans[:, :, None, None]
        * seen[:, :, HEAD_DIM : 2 * HEAD_DIM],
        axis=0,
    )
    scores = jnp.einsum("qhd,khd->hqk", query, key, preferred_element_type=jnp.float32)
    weights = jnp.exp(-jnp.abs(cumul[:, :, None] - cumul[:, None, :]))
    mix = jnp.einsum("hqk,khd->qhd", scores * weights, value_f, precision=HIGHEST)
    mix = mix + leading.T[:, :, None] * jnp.einsum(
        "qhd,hde->qhe", query_f, before, precision=HIGHEST
    )
    mix = mix + trailing.T[:, :, None] * jnp.einsum(
        "qhd,hde->qhe", query_f, after, precision=HIGHEST
    )
    middle = mix - jnp.mean(mix, axis=-1, keepdims=True)
    normed = middle * lax.rsqrt(jnp.mean(middle * middle, axis=-1, keepdims=True) + 1e-06)
    return normed.astype(jnp.bfloat16).reshape(rows, heads * HEAD_DIM)


def shards(
    tokens, gain, q_att, k_att, v_att, q_ret, k_ret, v_ret, out_att, out_ret, sink, decay_log
):
    parts = lax.axis_size("h")
    own = tokens.shape[0]
    rows = own * parts
    width = tokens.shape[1] * lax.axis_size("tp")
    kv = k_att.shape[1] // HEAD_DIM // parts
    group = q_att.shape[1] // k_att.shape[1]
    att = kv * group
    ret = q_ret.shape[1] // HEAD_DIM // parts
    offset = lax.axis_index("t") * rows
    total_rows = rows * lax.axis_size("t")

    packed = jnp.concatenate(
        [
            w.reshape(w.shape[0], parts, w.shape[1] // parts)
            for w in (q_att, k_att, v_att, q_ret, k_ret, v_ret)
        ],
        axis=2,
    )
    packed = jnp.moveaxis(packed, 1, 0)
    out_pack = jnp.concatenate(
        [w.reshape(parts, w.shape[0] // parts, w.shape[1]) for w in (out_att, out_ret)], axis=1
    )
    widened = tokens.astype(jnp.float32)
    sums = jnp.sum(widened * widened, axis=1)
    scaled = (widened * gain).astype(jnp.bfloat16)
    cores = lax.axis_size("tp")
    flat = packed.reshape(parts * packed.shape[1], packed.shape[2])
    weight = gather(exchange(flat, "h", 0, 0), "t", 0)
    whole = gather(gather(scaled, "h", 0), "tp", 1)
    proj = jnp.dot(whole, weight, preferred_element_type=jnp.float32)
    out_own = exchange(out_pack, "h", 0, 0)
    sums = lax.all_gather(sums, ("h", "tp"))
    decay = exchange(decay_log, "h", 0, 1)
    squares = jnp.sum(sums.reshape(parts, cores, own), axis=1).reshape(rows)
    inverse = lax.rsqrt(squares / width + 1e-06)[:, None]

    edges = [att, kv, kv, ret, ret, ret]
    starts = [sum(edges[:i]) * HEAD_DIM for i in range(6)]
    qa, ka, va, qr, kr, vr = (
        proj[:, s : s + n * HEAD_DIM].reshape(rows, n, HEAD_DIM) for s, n in zip(starts, edges)
    )
    scale = inverse[:, :, None]
    positions = (offset + jnp.arange(rows, dtype=jnp.int32)).astype(jnp.float32)
    freqs = 10000.0 ** (-jnp.arange(0, HEAD_DIM, 2).astype(jnp.float32) / HEAD_DIM)
    angles = positions[:, None] * freqs[None, :]
    cosine, sine = jnp.cos(angles)[:, None, :], jnp.sin(angles)[:, None, :]
    att_query = rotate(qa * scale, cosine, sine)
    att_key = rotate(ka * scale, cosine, sine)
    att_value = (va * scale).astype(jnp.bfloat16)
    ret_query = (qr * scale).astype(jnp.bfloat16)
    ret_key = (kr * (scale * HEAD_DIM ** (-0.5))).astype(jnp.bfloat16)
    ret_value = (vr * scale).astype(jnp.bfloat16)

    logits = lax.dynamic_slice_in_dim(sink, lax.axis_index("h") * att, att).reshape(kv, group)
    att_out, logs = attend(
        att_query.reshape(rows, kv, group, HEAD_DIM), att_key, att_value, logits, offset, total_rows
    )
    ret_out = retain(ret_query, ret_key, ret_value, decay)

    out_wide = gather(out_own, "t", 0)
    mixers = jnp.concatenate([att_out, ret_out], axis=1)
    depth = out_wide.shape[1]
    out_wide = jnp.moveaxis(out_wide, 0, 1).reshape(depth, -1)
    mixed = jnp.dot(mixers, out_wide, preferred_element_type=jnp.float32).astype(jnp.bfloat16)
    mixed = lax.psum_scatter(mixed, ("h", "tp"), scatter_dimension=0, tiled=True)
    return mixed, exchange(logs, "h", 1, 0)


def fits(args, sp, tp):
    tokens, _, q_att, k_att, v_att, q_ret, k_ret, v_ret, out_att, _, _, decay = args
    own, heads = tokens.shape[0] // sp, 4 * tp
    return (
        sp == 16
        and tp == 2
        and own == 2 * SPAN_RADIUS
        and q_att.shape[0] == sp * own
        and tokens.shape[1] == sp * own
        and q_att.shape[1] == 2 * heads * HEAD_DIM
        and all(v.shape[1] == heads * HEAD_DIM for v in (k_att, v_att, q_ret, k_ret, v_ret))
    )


def solution(mesh):
    sp, tp = mesh.shape["sp"], mesh.shape["tp"]

    def run(*args):
        if fits(args, sp, tp):
            seq = ("zh", "zl", "y", "x")
            fine = Mesh(mesh.devices.reshape(2, 2, 2, 2, tp), seq + ("tp",))
            step = fused
        else:
            heads = math.gcd(args[3].shape[1], args[5].shape[1]) // HEAD_DIM
            parts = math.gcd(heads // math.gcd(heads, tp), sp)
            seq = ("t", "h")
            fine = Mesh(mesh.devices.reshape(sp // parts, parts, tp), seq + ("tp",))
            step = shards
        body = jax.shard_map(
            step,
            mesh=fine,
            in_specs=(P(seq, "tp"), P("tp"))
            + (P(seq, "tp"),) * 6
            + (P("tp", seq), P("tp", seq), P("tp"), P("tp", seq)),
            out_specs=(P(seq + ("tp",), None), P("tp", seq)),
            check_vma=False,
        )
        return body(*args)

    return run
```

```python
import math

import jax
import jax.numpy as jnp
import numpy as np
from jax import lax
from jax.experimental import pallas as pl
from jax.experimental.pallas import tpu as pltpu
from jax.sharding import Mesh
from jax.sharding import PartitionSpec as P

HEAD_DIM = 128
SPAN_RADIUS = 128
BLOCK = 256
HIGHEST = lax.Precision.HIGHEST
MESH = pl.DeviceIdType.MESH


def gather(x, axis, dim):
    if lax.axis_size(axis) == 1:
        return x
    return lax.all_gather(x, axis, axis=dim, tiled=True)


def exchange(x, axis, split, concat):
    if lax.axis_size(axis) == 1:
        return x
    return lax.all_to_all(x, axis, split, concat, tiled=True)


def halo(shard, axis, width):
    peers, length = lax.axis_size(axis), shard.shape[1]
    up = [(i, i + 1) for i in range(peers - 1)]
    down = [(j, i) for i, j in up]
    before = lax.ppermute(shard[:, length - width :], axis, up)
    after = lax.ppermute(shard[:, :width], axis, down)
    return jnp.concatenate([before, shard, after], axis=1)


def rotate(values, cosine, sine):
    half = values.shape[-1] // 2
    first, second = values[..., :half], values[..., half:]
    return jnp.concatenate(
        [first * cosine - second * sine, second * cosine + first * sine], axis=-1
    ).astype(jnp.bfloat16)


def flip(v, bit):
    return v + bit - 2 * v * bit


class Stream:
    def __init__(self, where, remote, refs, pack):
        self.where, self.remote, self.pack = where, remote, pack
        (
            self.wide, self.away, self.out,
            self.load, self.x_send, self.z_send, self.h_send, self.y_send,
            self.p_recv, self.w_recv,
        ) = refs

    def fetch(self):
        w = self.where
        targets = (
            (self.out.at[0], 1 - w.g, 1 - w.x),
            (self.out.at[1], w.g, 1 - w.x),
            (self.wide.at[w.own], w.g, w.x),
            (self.away.at[w.x], 1 - w.g, w.x),
        )
        for i, (target, g, x) in enumerate(targets):
            self.pack(2 * g + x, target, self.load.at[i])

    def fetched(self):
        w = self.where
        for i, target in enumerate(
            (self.out.at[0], self.out.at[1], self.wide.at[w.own], self.away.at[w.x])
        ):
            pltpu.make_async_copy(target, target, self.load.at[i]).wait()

    def along_x(self, k):
        w = self.where
        if k == 0:
            return self.remote(
                self.out.at[0], self.away.at[w.x], self.x_send.at[0], self.p_recv.at[0], w.to_x
            )
        return self.remote(
            self.out.at[1], self.wide.at[w.own], self.x_send.at[1], self.w_recv.at[w.own], w.to_x
        )

    def along_z(self, k):
        w = self.where
        x = w.x if k == 0 else 1 - w.x
        s = w.at(w.zh, w.zl, w.y, x)
        return self.remote(
            self.away.at[x], self.wide.at[s], self.z_send.at[k], self.w_recv.at[s], w.to_z
        )

    def near(self, k):
        w = self.where
        return w.at(w.zh, flip(w.zl, k // 2), w.y, flip(w.x, k % 2))

    def far(self, k):
        w = self.where
        return w.at(1 - w.zh, flip(w.zl, 1 - k // 2), w.y, flip(w.x, k % 2))

    def across(self, k):
        w = self.where
        return w.at(1 - w.zh, flip(w.zl, 1 - k // 2), 1 - w.y, flip(w.x, k % 2))

    def along_h(self, k):
        s = self.near(k)
        return self.remote(
            self.wide.at[s], self.wide.at[s], self.h_send.at[k], self.w_recv.at[s], self.where.to_h
        )

    def along_y(self, k, far=0):
        s = self.far(k) if far else self.near(k)
        return self.remote(
            self.wide.at[s], self.wide.at[s],
            self.y_send.at[4 * far + k], self.w_recv.at[s], self.where.to_y,
        )

    def arrive(self, s):
        self.remote(
            self.wide.at[s], self.wide.at[s], self.x_send.at[0], self.w_recv.at[s], self.where.to_x
        ).wait_recv()

    def arrive_away(self):
        w = self.where
        slot = self.away.at[1 - w.x]
        self.remote(slot, slot, self.x_send.at[0], self.p_recv.at[0], w.to_x).wait_recv()

    def arrive_across(self, far):
        w = self.where
        zh = 1 - w.zh if far else w.zh
        for zl in range(2):
            for x in range(2):
                self.arrive(w.at(zh, zl, 1 - w.y, x))

    def drain(self):
        for k in range(2):
            self.along_x(k).wait_send()
            self.along_z(k).wait_send()
        for k in range(4):
            self.along_h(k).wait_send()
            self.along_y(k).wait_send()
            self.along_y(k, 1).wait_send()


class Place:
    def __init__(self):
        self.zh, self.zl, self.y, self.x, self.c = (
            lax.axis_index(a) for a in ("zh", "zl", "y", "x", "tp")
        )
        self.g = lax.rem(self.zh + self.zl, 2)
        self.h = 2 * self.g + self.x
        self.own = self.at(self.zh, self.zl, self.y, self.x)
        self.b = 2 * self.zl + self.x
        self.to_x = {"x": 1 - self.x}
        self.to_z = {"zl": 1 - self.zl}
        self.to_y = {"y": 1 - self.y}
        self.to_h = {"zh": 1 - self.zh, "zl": 1 - self.zl}
        self.to_hy = {"zh": 1 - self.zh, "zl": 1 - self.zl, "y": 1 - self.y}
        self.to_zx = {"zl": 1 - self.zl, "x": 1 - self.x}
        self.to_c = {"tp": 1 - self.c}
        self.to_zc = {"zl": 1 - self.zl, "tp": 1 - self.c}

    @staticmethod
    def at(zh, zl, y, x):
        return ((zh * 2 + zl) * 2 + y) * 2 + x


def fused_kernel(
    tokens, gain, q_att, k_att, v_att, q_ret, k_ret, v_ret, out_att, out_ret, sink, decay,
    cos_t, sin_t, base,
    mixed, logs_out,
    raw, scl, ssq, gains, acc_a, acc_r, kvext, qrot, rets, dec, cumr, cumc, coef, states, stall, crossing,
    mix, logm, lsend, lrecv, mine, give, take, s1, r1, s2, r2,
    t_load, t_x, t_z, t_c, t_recv, g_sem, d_sem, halo_sem, st_sem, l_sem, go,
    give_s, take_r, s1_s, r1_r, s2_s, r2_r,
    *streams,
):
    w = Place()
    y = w.y
    f32, bf16 = jnp.float32, jnp.bfloat16
    own, half_d = tokens.shape
    rows = 4 * own
    run_rows = 2 * own
    total_rows = 16 * own
    H = HEAD_DIM
    edge = SPAN_RADIUS

    def remote(src, dst, send, recv, to):
        return pltpu.make_async_remote_copy(
            src_ref=src, dst_ref=dst, send_sem=send, recv_sem=recv,
            device_id=to, device_id_type=MESH,
        )

    def lanes(h, n):
        return pl.ds(pl.multiple_of(h * n, n), n)

    def pack_cols(parts):
        def pack(h, target, sem):
            start = 0
            for ref in parts:
                n = ref.shape[1] // 4
                pltpu.make_async_copy(
                    ref.at[:, lanes(h, n)], target.at[:, pl.ds(start, n)], sem
                ).start()
                start += n
        return pack

    def pack_rows(parts):
        def pack(h, target, sem):
            start = 0
            for ref in parts:
                n = ref.shape[0] // 4
                pltpu.make_async_copy(
                    ref.at[lanes(h, n), :], target.at[pl.ds(start, n), :], sem
                ).start()
                start += n
        return pack

    n = len(streams) // 3
    A = Stream(w, remote, streams[:n], pack_cols((q_att, k_att, v_att)))
    R = Stream(w, remote, streams[n : 2 * n], pack_cols((q_ret, k_ret, v_ret)))
    O = Stream(w, remote, streams[2 * n :], pack_rows((out_att, out_ret)))

    token_load = pltpu.make_async_copy(tokens, raw.at[w.c, w.b], t_load.at[0])
    gain_load = pltpu.make_async_copy(gain, gains.at[w.c], t_load.at[1])
    decay_load = pltpu.make_async_copy(decay, dec.at[w.zh, w.y, w.zl, w.x], t_load.at[2])

    def block(zl, x):
        return 2 * zl + x

    def order(k):
        return block((w.zl, 1 - w.zl)[k // 2], (w.x, 1 - w.x)[k % 2])

    def token(e, k, part, send, to):
        here = raw.at[e, order(k)]
        if part is not None:
            here = here.at[pl.ds(part * edge, edge), :]
        return remote(here, here, send, t_recv.at[e, order(k), part or 0], to)

    tokens_x = [token(w.c, 0, None, t_x.at[0], w.to_x)]
    tokens_x += [token(w.c, 2, i, t_x.at[1 + i], w.to_x) for i in range(2)]
    tokens_z = token(w.c, 0, None, t_z.at[0], w.to_z)
    tokens_c = [token(w.c, k, None, t_c.at[k], w.to_c) for k in range(3)]
    tokens_c += [token(w.c, 3, i, t_c.at[3 + i], w.to_c) for i in range(2)]

    def token_arrive(k, e=None, part=None):
        token(w.c if e is None else e, k, part, t_x.at[0], w.to_x).wait_recv()

    gain_c = remote(gains.at[w.c], gains.at[w.c], g_sem.at[0], g_sem.at[1], w.to_c)

    def others(i):
        return tuple(flip(v, (i >> k) & 1) for v, k in ((w.zh, 3), (w.zl, 2), (w.y, 1), (w.x, 0)))

    def peer(i):
        return dict(zip(("zh", "zl", "y", "x"), others(i)))

    def decay_send(i):
        here = dec.at[w.zh, w.y, w.zl, w.x]
        return remote(here, here, d_sem.at[0, i], d_sem.at[1, i], peer(i))

    def decay_arrive(i):
        zh, zl, yy, x = others(i)
        here = dec.at[zh, yy, zl, x]
        remote(here, here, d_sem.at[0, i], d_sem.at[1, i], peer(i)).wait_recv()

    decay_load.start()
    R.fetch()
    A.fetch()
    gain_load.start()
    token_load.start()
    O.fetch()

    barrier = pltpu.get_barrier_semaphore()
    for to in (w.to_c, w.to_zc):
        pl.semaphore_signal(barrier, inc=1, device_id=to, device_id_type=MESH)
    for i in range(1, 16):
        pl.semaphore_signal(barrier, inc=1, device_id=peer(i), device_id_type=MESH)
    pl.semaphore_wait(barrier, 17)

    middle = w.g == 1

    decay_load.wait()
    for i in range(1, 16):
        decay_send(i).start()
    R.fetched()
    R.along_x(0).start()
    R.along_z(0).start()
    R.along_y(0).start()
    A.fetched()
    A.along_x(0).start()
    A.along_z(0).start()
    A.along_y(0).start()
    R.along_x(1).start()
    A.along_x(1).start()

    @pl.when(middle)
    def _():
        R.along_h(0).start()
        A.along_h(0).start()

    O.fetched()
    O.along_x(1).start()
    O.along_x(0).start()
    token_load.wait()
    tokens_x[0].start()
    gain_load.wait()
    gain_c.start()
    tokens_c[0].start()

    def scale(e, b, first=0, last=None):
        @pl.loop(first // 16, (own if last is None else last) // 16)
        def _(i):
            value = raw[e, b, pl.ds(pl.multiple_of(i * 16, 16), 16), :].astype(f32)
            at = pl.ds(pl.multiple_of(b * own + i * 16, 16), 16)
            scl[e, at, :] = (value * gains[e]).astype(bf16)
            square = value * value
            total = square[:, :H]
            for k in range(1, half_d // H):
                total = total + square[:, k * H : (k + 1) * H]
            ssq[e, at, :] = total

    @pl.when((w.zh == 0) & (w.y == 0))
    def _():
        kvext[0, :, 0:edge, :] = jnp.zeros((2, edge, H), bf16)

    @pl.when((w.zh == 1) & (w.y == 1))
    def _():
        kvext[1, :, edge + run_rows :, :] = jnp.zeros((2, edge, H), bf16)

    scale(w.c, w.b)
    for stream in (R, A):
        stream.arrive_away()
        stream.along_z(1).start()
    tokens_z.start()
    remote(gains.at[1 - w.c], gains.at[1 - w.c], g_sem.at[0], g_sem.at[1], w.to_c).wait_recv()
    token_arrive(0, 1 - w.c)
    scale(1 - w.c, w.b)

    def pass_near(stream, k):
        stream.arrive(stream.near(k))
        stream.along_y(k).start()

        @pl.when(middle)
        def _():
            stream.along_h(k).start()

    def pass_far(stream, k):
        stream.arrive(stream.far(k))
        stream.along_y(k, 1).start()

    pass_near(R, 2)
    pass_near(A, 2)
    for k in (1, 3):
        pass_near(R, k)
        pass_near(A, k)

    O.along_y(0).start()
    O.along_z(0).start()

    @pl.when(w.g == 0)
    def _():
        for stream in (R, A):
            for k in range(4):
                stream.along_h(k).start()

    @pl.when(middle)
    def _():
        O.along_h(0).start()

    for i in range(1, 16):
        decay_arrive(i)

    lane = lax.broadcasted_iota(jnp.int32, (8, run_rows), 1)
    for slot in range(2):
        row = jnp.concatenate(
            [dec[w.zh, w.y, slot, x, pl.ds(w.h, 1), :] for x in range(2)], axis=1
        )
        row = jnp.broadcast_to(row, (8, run_rows))
        step = 1
        while step < run_rows:
            row = row + jnp.where(lane >= step, pltpu.roll(row, step, axis=1), 0.0)
            step *= 2
        cumr[slot] = row
        cumc[slot] = jnp.transpose(jnp.broadcast_to(row[0:1], (H, run_rows)))
    lane = lax.broadcasted_iota(jnp.int32, (8, H), 1)
    run = lax.broadcasted_iota(jnp.int32, (8, H), 0)
    totals = jnp.zeros((8, H), f32)
    for zh in range(2):
        for slot in range(2):
            for yy in range(2):
                pair = sum(dec[zh, yy, slot, x, pl.ds(w.h, 1), :] for x in range(2))
                value = jnp.sum(pair, axis=1, keepdims=True)
                totals = jnp.where(lane == 4 * zh + 2 * slot + yy, value, totals)
    for slot in range(2):
        me = 4 * w.zh + 2 * slot + w.y
        between = (lane > jnp.minimum(run, me)) & (lane < jnp.maximum(run, me))
        factor = jnp.exp(jnp.sum(jnp.where(between, totals, 0.0), axis=1, keepdims=True))
        factor = jnp.broadcast_to(factor, (8, H))
        near = run // 4 == w.zh
        coef[slot, 0] = jnp.where(near & (run < me), factor, 0.0)
        coef[slot, 1] = jnp.where(near & (run > me), factor, 0.0)
        between = (lane > jnp.where(w.zh == 0, me, 3)) & (lane < jnp.where(w.zh == 0, 4, me))
        factor = jnp.exp(jnp.sum(jnp.where(between, totals, 0.0), axis=1, keepdims=True))
        coef[slot, 2] = jnp.broadcast_to(factor, (8, H))

    @pl.when(middle)
    def _():
        pass_near(O, 1)
        for stream in (R, A):
            for k in (0, 2, 1, 3):
                pass_far(stream, k)

    def part_of(stream, zh, b, start, width):
        at = pl.ds(pl.multiple_of(b * own, own), own)
        depth = half_d // own
        weight = stream.wide[pl.ds(zh * depth, depth), :, start : start + width]
        return jnp.dot(
            scl[zh, at, :], weight.reshape(half_d, width), preferred_element_type=f32
        )

    def first_part(stream, acc, b):
        at = pl.ds(pl.multiple_of(b * own, own), own)
        start = 0
        while start < acc.shape[1]:
            width = min(2 * H, acc.shape[1] - start)
            acc[at, start : start + width] = part_of(stream, w.zh, b, start, width)
            start += width

    def pair_of(stream, zl, yy, b, start, width):
        zh = 1 - w.zh
        at = pl.ds(pl.multiple_of(b * own, own), own)
        depth = pl.ds(pl.multiple_of((2 * zl + yy) * 2 * own, 2 * own), 2 * own)
        weight = stream.wide[pl.ds(w.at(zh, zl, yy, 0), 2), :, start : start + width]
        return jnp.dot(
            scl[zh, at, depth], weight.reshape(2 * own, width), preferred_element_type=f32
        )

    def add_pair(stream, acc, zl, yy, b):
        at = pl.ds(pl.multiple_of(b * own, own), own)
        for start in range(0, acc.shape[1], 2 * H):
            width = min(2 * H, acc.shape[1] - start)
            acc[at, start : start + width] += pair_of(stream, zl, yy, b, start, width)

    def last_of(stream, acc, b, start, width):
        at = pl.ds(pl.multiple_of(b * own, own), own)
        return acc[at, start : start + width] + pair_of(stream, w.zl, 1 - w.y, b, start, width)

    def whole_of(stream, acc, b, start, width):
        at = pl.ds(pl.multiple_of(b * own, own), own)
        return acc[at, start : start + width] + part_of(stream, 1 - w.zh, b, start, width)

    token_arrive(2)
    for copy in tokens_x[1:]:
        copy.start()
    tokens_c[2].start()
    scale(w.c, order(2))
    token_arrive(2, 1 - w.c)
    scale(1 - w.c, order(2))
    token_arrive(1)
    tokens_c[1].start()
    scale(w.c, order(1))

    @pl.when(w.g == 0)
    def _():
        pass_far(R, 0)

    O.arrive_away()
    O.along_z(1).start()
    token_arrive(1, 1 - w.c)
    scale(1 - w.c, order(1))

    @pl.when(w.g == 0)
    def _():
        pass_far(R, 1)

    R.arrive_across(0)
    A.arrive_across(0)

    @pl.loop(0, 3)
    def _(i):
        k = 2 - i
        b = block(flip(w.zl, k // 2), flip(w.x, k % 2))
        first_part(R, acc_r, b)
        first_part(A, acc_a, b)

    @pl.when(w.g == 0)
    def _():
        pass_far(R, 2)

    token_arrive(3, None, 0)
    tokens_c[3].start()
    scale(w.c, order(3), 0, edge)
    token_arrive(3, 1 - w.c, 0)
    scale(1 - w.c, order(3), 0, edge)

    @pl.when(w.g == 0)
    def _():
        pass_far(R, 3)
        pass_far(A, 0)

    token_arrive(3, None, 1)
    tokens_c[4].start()

    @pl.when(w.g == 0)
    def _():
        pass_far(A, 1)

    scale(w.c, order(3), edge, own)
    token_arrive(3, 1 - w.c, 1)
    scale(1 - w.c, order(3), edge, own)
    first_part(R, acc_r, order(3))
    first_part(A, acc_a, order(3))

    def inverse(b):
        at = pl.ds(pl.multiple_of(b * own, own), own)
        squares = jnp.sum(ssq[0, at, :] + ssq[1, at, :], axis=1, keepdims=True)
        return lax.rsqrt(squares / (2 * half_d) + 1e-06)

    def angles(b):
        s = w.at(w.zh, b // 2, w.y, b % 2)
        c0, s0, s0n, c0n = (base[i, pl.ds(s, 1), :] for i in range(4))
        cosine = cos_t[...] * c0 - sin_t[...] * s0
        sine = cos_t[...] * s0n + sin_t[...] * c0n
        return cosine, sine

    def turn(value, cosine, sine):
        return (value * cosine + pltpu.roll(value, H // 2, axis=1) * sine).astype(bf16)

    def keys_values(b):
        scale_b = inverse(b)
        cosine, sine = angles(b)
        both = last_of(A, acc_a, b, 2 * H, 2 * H) * scale_b
        inner = pl.ds(pl.multiple_of(edge + (b % 2) * own, edge), own)
        kvext[b // 2, 0, inner, :] = turn(both[:, :H], cosine, sine)
        kvext[b // 2, 1, inner, :] = both[:, H:].astype(bf16)

    def queries(b):
        at = pl.ds(pl.multiple_of(b * own, own), own)
        cosine, sine = angles(b)
        query = last_of(A, acc_a, b, 0, 2 * H) * inverse(b)
        qrot[at, :H] = turn(query[:, :H], cosine, sine)
        qrot[at, H:] = turn(query[:, H:], cosine, sine)

    R.arrive_across(1)

    def retention_inputs(b):
        at = pl.ds(pl.multiple_of(b * own, own), own)
        scale_b = inverse(b)
        both = whole_of(R, acc_r, b, 0, 2 * H)
        rets[0, at, :] = (both[:, :H] * scale_b).astype(bf16)
        rets[1, at, :] = (both[:, H:] * (scale_b * H ** (-0.5))).astype(bf16)
        rets[2, at, :] = (whole_of(R, acc_r, b, 2 * H, H) * scale_b).astype(bf16)

    @pl.when(w.g == 0)
    def _():
        pass_far(A, 2)

    @pl.loop(0, 4)
    def _(b):
        retention_inputs(b)

    for slot in range(2):
        at = pl.ds(slot * run_rows, run_rows)
        last = cumr[slot, 0:1, run_rows - 1 : run_rows]
        key, value = rets[1, at, :].astype(f32), rets[2, at, :]
        for i, weight in enumerate((jnp.exp(last - cumc[slot]), jnp.exp(cumc[slot]))):
            lhs = (key * weight).astype(bf16)
            state = lax.dot_general(
                lhs, value, (((0,), (0,)), ((), ())), preferred_element_type=f32
            ).astype(bf16)
            stall[y, slot, i] = state
    total = jnp.zeros((H, H), f32)
    for slot in range(2):
        total = total + coef[slot, 2, 0:1, :] * stall[y, slot, w.zh].astype(f32)
    crossing[2] = total.astype(bf16)
    state_sends = [
        remote(stall.at[y], stall.at[y], st_sem.at[0, 0], st_sem.at[1, 0], w.to_y),
        remote(crossing.at[2], crossing.at[0], st_sem.at[0, 1], st_sem.at[1, 1], w.to_h),
        remote(crossing.at[2], crossing.at[1], st_sem.at[0, 2], st_sem.at[1, 2], w.to_hy),
    ]
    state_sends[1].start()
    state_sends[2].start()

    def inner_tile(i):
        slot = i // 2
        at = pl.ds(pl.multiple_of(i * own, own), own)
        keys = pl.ds(pl.multiple_of(slot * run_rows, run_rows), run_rows)
        score = lax.dot_general(
            rets[0, at, :], rets[1, keys, :], (((1,), (1,)), ((), ())),
            preferred_element_type=f32,
        )
        column = cumc[slot, pl.ds(pl.multiple_of((i % 2) * own, own), own), :]
        column = jnp.concatenate([column] * (run_rows // H), axis=1)
        weight = jnp.exp(-jnp.abs(column - cumr[slot, 0:1, :]))
        acc_r[at, :H] = jnp.dot(
            (score * weight).astype(bf16), rets[2, keys, :], preferred_element_type=f32
        )

    @pl.loop(0, 4)
    def _(i):
        inner_tile(i)

    @pl.when(w.g == 0)
    def _():
        pass_far(A, 3)

    @pl.loop(0, 8)
    def _(i):
        add_pair(A, acc_a, i // 4, y, i % 4)

    for k in range(2):
        A.arrive(A.across(k))

    @pl.loop(0, 4)
    def _(b):
        add_pair(A, acc_a, 1 - w.zl, 1 - y, b)

    state_sends[0].start()
    for k in range(2, 4):
        A.arrive(A.across(k))

    @pl.loop(0, 4)
    def _(b):
        keys_values(b)

    head, tail, before_at, after_at = edge, run_rows, 0, edge + run_rows

    def pick(a, b):
        return a + (b - a) * y

    def piece(slot, start):
        return kvext.at[slot, :, pl.ds(pl.multiple_of(start, edge), edge), :]

    halo_y = [
        remote(
            piece(pick(s0, s1), pick(f0, f1)), piece(pick(d0, d1), pick(o0, o1)),
            halo_sem.at[0, i], halo_sem.at[1, i], w.to_y,
        )
        for i, (s0, f0, d0, o0, s1, f1, d1, o1) in enumerate(
            (
                (0, tail, 0, before_at, 0, head, 0, after_at),
                (1, head, 0, after_at, 0, tail, 1, before_at),
                (1, tail, 1, before_at, 1, head, 1, after_at),
            )
        )
    ]
    halo_far = remote(
        piece(pick(0, 1), pick(head, tail)), piece(pick(1, 0), pick(after_at, before_at)),
        halo_sem.at[0, 3], halo_sem.at[1, 3], w.to_hy,
    )
    has_far = ((y == 0) & (w.zh == 1)) | ((y == 1) & (w.zh == 0))
    for copy in halo_y:
        copy.start()

    @pl.when(has_far)
    def _():
        halo_far.start()

    @pl.when(middle)
    def _():
        for k in (2, 3):
            pass_near(O, k)
        for k in range(2):
            pass_far(O, k)

    @pl.loop(0, 4)
    def _(b):
        queries(b)

    def halo_arrive(slot, start, i, to):
        here = piece(slot, start)
        remote(here, here, halo_sem.at[0, i], halo_sem.at[1, i], to).wait_recv()

    def attend_tile(i):
        slot, j = i // 4, i % 4
        query = qrot[pl.ds(pl.multiple_of(i * edge, edge), edge), :]
        query = jnp.concatenate([query[:, :H], query[:, H:]], axis=0)
        span = pl.ds(pl.multiple_of(j * edge, edge), 3 * edge)
        key, value = kvext[slot, 0, span, :], kvext[slot, 1, span, :]
        score = lax.dot_general(
            query, key, (((1,), (1,)), ((), ())), preferred_element_type=f32
        ) * H ** (-0.5)
        row = lax.broadcasted_iota(jnp.int32, score.shape, 0)
        col = lax.broadcasted_iota(jnp.int32, score.shape, 1)
        shift = col - jnp.where(row < edge, row, row - edge)
        start = w.at(w.zh, slot, y, 0) * own + j * edge - edge
        valid = (
            (shift >= 0) & (shift <= 2 * edge) & (col >= -start) & (col < total_rows - start)
        )
        masked = jnp.where(valid, score, -jnp.inf)
        first = lax.broadcasted_iota(jnp.int32, (2 * edge, 1), 0) < edge
        limit = jnp.where(first, sink[2 * w.h], sink[2 * w.h + 1])
        top = jnp.maximum(jnp.max(masked, axis=1, keepdims=True), limit)
        expo = jnp.exp(masked - top)
        total = jnp.sum(expo, axis=1, keepdims=True) + jnp.exp(limit - top)
        logs = top + jnp.log(total)
        probs = (expo * (1.0 / total)).astype(bf16)
        result = jnp.dot(probs, value, preferred_element_type=f32).astype(bf16)
        at = pl.ds(pl.multiple_of((i // 2) * edge, edge), edge)
        mix[i % 2, at, 0:H] = result[:edge]
        mix[i % 2, at, H : 2 * H] = result[edge:]
        column = lax.broadcasted_iota(jnp.int32, (2 * edge, H), 1)
        logm[...] = jnp.where(column == i, logs, logm[...])

    logm[...] = jnp.zeros_like(logm)

    @pl.loop(0, 4)
    def _(i):
        attend_tile(4 * (i // 2) + 1 + i % 2)

    @pl.when(middle)
    def _():
        for copy in state_sends[1:]:
            copy.wait_send()

        @pl.when(has_far)
        def _():
            halo_far.wait_send()

        for to in (w.to_z, w.to_zc):
            pl.semaphore_signal(go, inc=1, device_id=to, device_id_type=MESH)

    @pl.when(w.g == 0)
    def _():
        pl.semaphore_wait(go, 2)
        for k in range(4):
            if k:
                pass_near(O, k)
            O.along_h(k).start()

    halo_arrive(pick(0, 0), pick(after_at, before_at), 0, w.to_y)
    halo_arrive(pick(1, 0), pick(before_at, after_at), 1, w.to_y)
    halo_arrive(pick(1, 1), pick(after_at, before_at), 2, w.to_y)

    @pl.when(has_far)
    def _():
        halo_arrive(pick(0, 1), pick(before_at, after_at), 3, w.to_hy)

    @pl.loop(0, 4)
    def _(i):
        attend_tile(4 * (i // 2) + 3 * (i % 2))

    for i, here in enumerate((stall.at[1 - y], crossing.at[0], crossing.at[1])):
        remote(here, here, st_sem.at[0, i], st_sem.at[1, i], w.to_y).wait_recv()
    crossed = crossing[0].astype(f32) + crossing[1].astype(f32)
    for slot in range(2):
        for i in range(2):
            total = jnp.where(w.zh == 1 - i, 1.0, 0.0) * coef[slot, 2, 0:1, :] * crossed
            for s in range(2):
                for yy in range(2):
                    for zh in range(2):
                        r = 4 * zh + 2 * s + yy
                        total = total + coef[slot, i, r : r + 1, :] * stall[yy, s, i].astype(f32)
            states[slot, :, i * H : (i + 1) * H] = total.astype(bf16)

    def finish_tile(i):
        slot = i // 2
        at = pl.ds(pl.multiple_of(i * own, own), own)
        column = cumc[slot, pl.ds(pl.multiple_of((i % 2) * own, own), own), :]
        last = cumr[slot, 0:1, run_rows - 1 : run_rows]
        carried = jnp.dot(rets[0, at, :], states[slot], preferred_element_type=f32)
        value = (
            acc_r[at, :H] + jnp.exp(column) * carried[:, :H]
            + jnp.exp(last - column) * carried[:, H:]
        )
        value = value - jnp.mean(value, axis=1, keepdims=True)
        value = value * lax.rsqrt(jnp.mean(value * value, axis=1, keepdims=True) + 1e-06)
        value = value.astype(bf16)
        out = pl.ds(pl.multiple_of(i * edge, edge), edge)
        mix[0, out, 2 * H :] = value[:edge]
        mix[1, out, 2 * H :] = value[edge:]

    @pl.loop(0, 4)
    def _(i):
        finish_tile(i)

    turned = jnp.transpose(logm[...])
    for b in range(4):
        lsend[b] = turned[2 * b : 2 * b + 2]
        lrecv[w.h] = jnp.where(w.b == b, turned[2 * b : 2 * b + 2], lrecv[w.h] if b else 0.0)
    h_of = lambda zl, x: 2 * lax.rem(w.zh + zl, 2) + x
    log_to = (
        (1 - w.x, w.zl, w.to_x), (w.x, 1 - w.zl, w.to_z), (1 - w.x, 1 - w.zl, w.to_zx),
    )
    log_sends = [
        remote(lsend.at[block(zl, x)], lrecv.at[w.h], l_sem.at[0, i], l_sem.at[1, i], to)
        for i, (x, zl, to) in enumerate(log_to)
    ]

    for copy in log_sends:
        copy.start()

    chunks = 8

    def columns_of(i, x):
        far, across, zl = i // 4, (i // 2) % 2, i % 2
        return w.at(flip(w.zh, far), zl, flip(y, across), x)

    def swap(i):
        return remote(give.at[i], take.at[i], give_s.at[i], take_r.at[i], w.to_c)

    def x_first(i, k):
        return 1 if k == 0 else jnp.where(i < 2, 1, 0)

    def toward(dx):
        return {"x": flip(w.x, dx), "zl": flip(w.zl, 1 - dx)}

    def first_hop(i, k):
        to = toward(x_first(i, k))
        return remote(s1.at[i, k], r1.at[i, k], s1_s.at[i, k], r1_r.at[i, k], to)

    def second_hop(i, k):
        to = toward(1 - x_first(i, k))
        return remote(s2.at[i, k], r2.at[i, k], s2_s.at[i, k], r2_r.at[i, k], to)

    def side(i, k, j, cross):
        dx = x_first(i, k)
        zl = dx * j + (1 - dx) * flip(w.zl, cross)
        x = dx * flip(w.x, cross) + (1 - dx) * j
        return block(zl, x)

    def part(b):
        return pl.ds(pl.multiple_of(b * edge, edge), edge)

    @pl.loop(0, chunks + 3)
    def _(step):
        @pl.when(step < chunks)
        def _():
            i = step

            @pl.when((i // 2) % 2 == 1)
            def _():
                for x in range(2):
                    O.arrive(columns_of(i, x))

            @pl.when((i == 1) & (w.g == 0))
            def _():
                for k in range(2):
                    pass_far(O, k)

            @pl.when(i == 3)
            def _():
                for k in range(2, 4):
                    pass_far(O, k)

            for k in range(2):
                give[i, k] = jnp.dot(
                    mix[1 - w.c], O.wide[columns_of(i, k)], preferred_element_type=f32
                ).astype(bf16)
            swap(i).start()
            for k in range(2):
                mine[i % 4, k] = jnp.dot(
                    mix[w.c], O.wide[columns_of(i, k)], preferred_element_type=f32
                )

        @pl.when((step >= 1) & (step < chunks + 1))
        def _():
            i = step - 1
            swap(i).wait_recv()
            for k in range(2):
                for j in range(2):
                    b = side(i, k, j, 1)
                    total = mine[i % 4, k, part(b), :] + take[i, k, part(b), :].astype(f32)
                    s1[i, k, j] = total.astype(bf16)
                first_hop(i, k).start()
            for k in range(2):
                for j in range(2):
                    b = side(i, k, j, 0)
                    mine[i % 4, k, part(b), :] += take[i, k, part(b), :].astype(f32)

        @pl.when((step >= 2) & (step < chunks + 2))
        def _():
            i = step - 2
            for k in range(2):
                first_hop(i, k).wait_recv()
                dx = x_first(i, k)
                j = flip(dx * w.zl + (1 - dx) * w.x, 1)
                b = side(i, k, j, 0)
                s2[i, k] = (mine[i % 4, k, part(b), :] + r1[i, k, j].astype(f32)).astype(bf16)
                second_hop(i, k).start()

        @pl.when(step >= 3)
        def _():
            i = step - 3
            for k in range(2):
                second_hop(i, k).wait_recv()
                dx = x_first(i, k)
                j = dx * w.zl + (1 - dx) * w.x
                at = pl.ds(pl.multiple_of(columns_of(i, k) * own, own), own)
                total = mine[i % 4, k, part(w.b), :] + r1[i, k, j].astype(f32)
                mixed[:, at] = (total + r2[i, k].astype(f32)).astype(mixed.dtype)

    for i, (x, zl, to) in enumerate(log_to):
        here = lrecv.at[h_of(zl, x)]
        remote(here, here, l_sem.at[0, i], l_sem.at[1, i], to).wait_recv()
    for h in range(4):
        for head_i in range(2):
            for t in range(2):
                logs_out[2 * h + head_i : 2 * h + head_i + 1, t * edge : (t + 1) * edge] = (
                    lrecv[h, t : t + 1, head_i * edge : (head_i + 1) * edge]
                )

    for stream in (A, R, O):
        stream.drain()
    for i in range(1, 16):
        decay_send(i).wait_send()
    for copy in tokens_x + tokens_c + [tokens_z, gain_c]:
        copy.wait_send()
    for copy in halo_y + state_sends[:1] + log_sends:
        copy.wait_send()

    @pl.when(w.g == 0)
    def _():
        for copy in state_sends[1:]:
            copy.wait_send()

        @pl.when(has_far)
        def _():
            halo_far.wait_send()

    @pl.loop(0, chunks)
    def _(i):
        swap(i).wait_send()
        for k in range(2):
            first_hop(i, k).wait_send()
            second_hop(i, k).wait_send()


def fused(*args):
    tokens, gain, q_att = args[:3]
    out_att, out_ret, sink, decay_log = args[8:]
    own, half_d = tokens.shape
    rows, run_rows = 4 * own, 2 * own
    H, edge = HEAD_DIM, SPAN_RADIUS
    bf16, f32 = jnp.bfloat16, jnp.float32
    dma, vmem = pltpu.SemaphoreType.DMA, pltpu.VMEM
    depth = q_att.shape[0]
    width = out_att.shape[1] * 16

    freqs = 10000.0 ** (-np.arange(0, H, 2, dtype=np.float64) / H)
    freqs = np.concatenate([freqs, freqs])[None, :]
    sign = np.where(np.arange(H) < H // 2, -1.0, 1.0)[None, :]
    inner = np.arange(own)[:, None] * freqs
    outer = (np.arange(16) * own)[:, None] * freqs
    cos_t, sin_t = jnp.asarray(np.cos(inner), f32), jnp.asarray(np.sin(inner), f32)
    base = jnp.asarray(
        np.stack([np.cos(outer), np.sin(outer), sign * np.sin(outer), sign * np.cos(outer)]), f32
    )

    def stream(block):
        return [
            vmem((16,) + block, bf16), vmem((2,) + block, bf16), vmem((2,) + block, bf16),
            dma((4,)), dma((2,)), dma((2,)), dma((4,)), dma((8,)), dma((1,)), dma((16,)),
        ]

    out_rows = (out_att.shape[0] + out_ret.shape[0]) // 4
    tile = (8, 2, 4 * edge, own)
    hbm, inside = pl.BlockSpec(memory_space=pl.ANY), pl.BlockSpec(memory_space=pltpu.VMEM)
    return pl.pallas_call(
        fused_kernel,
        out_shape=(
            jax.ShapeDtypeStruct((own // 2, width), bf16),
            jax.ShapeDtypeStruct((sink.shape[0], own), f32),
        ),
        in_specs=[hbm] * 10 + [pl.BlockSpec(memory_space=pltpu.SMEM), hbm] + [inside] * 3,
        out_specs=[inside] * 2,
        scratch_shapes=[
            vmem((2, 4, own, half_d), bf16),
            vmem((2, rows, half_d), bf16),
            vmem((2, rows, H), f32),
            vmem((2, 1, half_d), f32),
            vmem((rows, 4 * H), f32),
            vmem((rows, 3 * H), f32),
            vmem((2, 2, run_rows + 2 * edge, H), bf16),
            vmem((rows, 2 * H), bf16),
            vmem((3, rows, H), bf16),
            vmem((2, 2, 2, 2) + decay_log.shape, f32),
            vmem((2, 8, run_rows), f32),
            vmem((2, run_rows, H), f32),
            vmem((2, 3, 8, H), f32),
            vmem((2, H, 2 * H), bf16),
            vmem((2, 2, 2, H, H), bf16), vmem((3, H, H), bf16),
            vmem((2, 4 * edge, 3 * H), bf16),
            vmem((2 * edge, H), f32),
            vmem((4, 2, 2 * edge), f32),
            vmem((4, 2, 2 * edge), f32),
            vmem((4,) + tile[1:], f32), vmem(tile, bf16), vmem(tile, bf16),
            vmem((8, 2, 2, edge, own), bf16), vmem((8, 2, 2, edge, own), bf16),
            vmem((8, 2, edge, own), bf16), vmem((8, 2, edge, own), bf16),
            dma((3,)), dma((3,)), dma((1,)), dma((5,)), dma((2, 4, 2)), dma((2,)), dma((2, 16)),
            dma((2, 4)), dma((2, 3)), dma((2, 3)), pltpu.SemaphoreType.REGULAR,
            dma((8,)), dma((8,)), dma((8, 2)), dma((8, 2)), dma((8, 2)), dma((8, 2)),
        ]
        + stream((depth, 4 * H))
        + stream((depth, 3 * H))
        + stream((out_rows, own)),
        compiler_params=pltpu.CompilerParams(
            collective_id=0, has_side_effects=True, vmem_limit_bytes=67043328
        ),
        cost_estimate=pl.CostEstimate(
            flops=10**11, bytes_accessed=2 * 10**7, transcendentals=0
        ),
    )(
        tokens, gain.reshape(1, half_d), *args[2:10], sink, decay_log, cos_t, sin_t, base
    )


def attend(query, key, value, sink, offset, total_rows):
    rows, kv, group, _ = query.shape
    ext = halo(jnp.stack([key, value]), "t", SPAN_RADIUS)
    size = min(rows, BLOCK)
    count = rows // size
    span = size + 2 * SPAN_RADIUS
    pieces = jnp.stack([ext[:, b * size : b * size + span] for b in range(count)])
    blocks = query.reshape(count, size, kv, group, HEAD_DIM)
    scores = jnp.einsum(
        "bqhgd,bkhd->bhgqk", blocks, pieces[:, 0], preferred_element_type=jnp.float32
    ) * HEAD_DIM ** (-0.5)
    base = offset + jnp.arange(count, dtype=jnp.int32) * size
    query_pos = base[:, None] + jnp.arange(size, dtype=jnp.int32)
    key_pos = base[:, None] - SPAN_RADIUS + jnp.arange(span, dtype=jnp.int32)
    spacing = key_pos[:, None, :] - query_pos[:, :, None]
    inside = (key_pos >= 0) & (key_pos < total_rows)
    valid = (jnp.abs(spacing) <= SPAN_RADIUS) & inside[:, None, :]
    masked = jnp.where(valid[:, None, None], scores, -jnp.inf)
    limit = sink[None, :, :, None]
    top = jnp.maximum(jnp.max(masked, axis=-1), limit)
    expo = jnp.exp(masked - top[..., None])
    total = jnp.sum(expo, axis=-1) + jnp.exp(limit - top)
    logs = top + jnp.log(total)
    probs = (expo / total[..., None]).astype(jnp.bfloat16)
    result = jnp.einsum(
        "bhgqk,bkhd->bqhgd", probs, pieces[:, 1], preferred_element_type=jnp.float32
    ).astype(jnp.bfloat16)
    logs = jnp.transpose(logs, (1, 2, 0, 3)).reshape(kv * group, rows)
    return result.reshape(rows, kv * group * HEAD_DIM), logs


def retain(query, key, value, decay):
    rows, heads, _ = query.shape
    peers, index = lax.axis_size("t"), lax.axis_index("t")
    cumul = jnp.cumsum(decay, axis=1)
    last = cumul[:, -1]
    query_f, key_f, value_f = (v.astype(jnp.float32) for v in (query, key, value))
    trailing = jnp.exp(last[:, None] - cumul)
    leading = jnp.exp(cumul)
    forward = jnp.einsum("hk,khd,khe->hde", trailing, key_f, value_f, precision=HIGHEST)
    backward = jnp.einsum("hk,khd,khe->hde", leading, key_f, value_f, precision=HIGHEST)
    tail = jnp.broadcast_to(last[:, None, None], (heads, 8, HEAD_DIM))
    sent = jnp.concatenate([forward, backward, tail], axis=1)
    seen = lax.all_gather(sent, "t", axis=0)
    lasts = seen[:, :, 2 * HEAD_DIM, 0]
    at = jnp.arange(peers)
    low = jnp.minimum(at, index)[:, None]
    high = jnp.maximum(at, index)[:, None]
    between = (at[None, :] > low) & (at[None, :] < high)
    spans = jnp.exp(jnp.sum(jnp.where(between[:, :, None], lasts[None], 0.0), axis=1))
    before = jnp.sum(
        jnp.where(at < index, 1.0, 0.0)[:, None, None, None]
        * spans[:, :, None, None]
        * seen[:, :, :HEAD_DIM],
        axis=0,
    )
    after = jnp.sum(
        jnp.where(at > index, 1.0, 0.0)[:, None, None, None]
        * spans[:, :, None, None]
        * seen[:, :, HEAD_DIM : 2 * HEAD_DIM],
        axis=0,
    )
    scores = jnp.einsum("qhd,khd->hqk", query, key, preferred_element_type=jnp.float32)
    weights = jnp.exp(-jnp.abs(cumul[:, :, None] - cumul[:, None, :]))
    mix = jnp.einsum("hqk,khd->qhd", scores * weights, value_f, precision=HIGHEST)
    mix = mix + leading.T[:, :, None] * jnp.einsum(
        "qhd,hde->qhe", query_f, before, precision=HIGHEST
    )
    mix = mix + trailing.T[:, :, None] * jnp.einsum(
        "qhd,hde->qhe", query_f, after, precision=HIGHEST
    )
    middle = mix - jnp.mean(mix, axis=-1, keepdims=True)
    normed = middle * lax.rsqrt(jnp.mean(middle * middle, axis=-1, keepdims=True) + 1e-06)
    return normed.astype(jnp.bfloat16).reshape(rows, heads * HEAD_DIM)


def shards(
    tokens, gain, q_att, k_att, v_att, q_ret, k_ret, v_ret, out_att, out_ret, sink, decay_log
):
    parts = lax.axis_size("h")
    own = tokens.shape[0]
    rows = own * parts
    width = tokens.shape[1] * lax.axis_size("tp")
    kv = k_att.shape[1] // HEAD_DIM // parts
    group = q_att.shape[1] // k_att.shape[1]
    att = kv * group
    ret = q_ret.shape[1] // HEAD_DIM // parts
    offset = lax.axis_index("t") * rows
    total_rows = rows * lax.axis_size("t")

    packed = jnp.concatenate(
        [
            w.reshape(w.shape[0], parts, w.shape[1] // parts)
            for w in (q_att, k_att, v_att, q_ret, k_ret, v_ret)
        ],
        axis=2,
    )
    packed = jnp.moveaxis(packed, 1, 0)
    out_pack = jnp.concatenate(
        [w.reshape(parts, w.shape[0] // parts, w.shape[1]) for w in (out_att, out_ret)], axis=1
    )
    widened = tokens.astype(jnp.float32)
    sums = jnp.sum(widened * widened, axis=1)
    scaled = (widened * gain).astype(jnp.bfloat16)
    cores = lax.axis_size("tp")
    flat = packed.reshape(parts * packed.shape[1], packed.shape[2])
    weight = gather(exchange(flat, "h", 0, 0), "t", 0)
    whole = gather(gather(scaled, "h", 0), "tp", 1)
    proj = jnp.dot(whole, weight, preferred_element_type=jnp.float32)
    out_own = exchange(out_pack, "h", 0, 0)
    sums = lax.all_gather(sums, ("h", "tp"))
    decay = exchange(decay_log, "h", 0, 1)
    squares = jnp.sum(sums.reshape(parts, cores, own), axis=1).reshape(rows)
    inverse = lax.rsqrt(squares / width + 1e-06)[:, None]

    edges = [att, kv, kv, ret, ret, ret]
    starts = [sum(edges[:i]) * HEAD_DIM for i in range(6)]
    qa, ka, va, qr, kr, vr = (
        proj[:, s : s + n * HEAD_DIM].reshape(rows, n, HEAD_DIM) for s, n in zip(starts, edges)
    )
    scale = inverse[:, :, None]
    positions = (offset + jnp.arange(rows, dtype=jnp.int32)).astype(jnp.float32)
    freqs = 10000.0 ** (-jnp.arange(0, HEAD_DIM, 2).astype(jnp.float32) / HEAD_DIM)
    angles = positions[:, None] * freqs[None, :]
    cosine, sine = jnp.cos(angles)[:, None, :], jnp.sin(angles)[:, None, :]
    att_query = rotate(qa * scale, cosine, sine)
    att_key = rotate(ka * scale, cosine, sine)
    att_value = (va * scale).astype(jnp.bfloat16)
    ret_query = (qr * scale).astype(jnp.bfloat16)
    ret_key = (kr * (scale * HEAD_DIM ** (-0.5))).astype(jnp.bfloat16)
    ret_value = (vr * scale).astype(jnp.bfloat16)

    logits = lax.dynamic_slice_in_dim(sink, lax.axis_index("h") * att, att).reshape(kv, group)
    att_out, logs = attend(
        att_query.reshape(rows, kv, group, HEAD_DIM), att_key, att_value, logits, offset, total_rows
    )
    ret_out = retain(ret_query, ret_key, ret_value, decay)

    out_wide = gather(out_own, "t", 0)
    mixers = jnp.concatenate([att_out, ret_out], axis=1)
    depth = out_wide.shape[1]
    out_wide = jnp.moveaxis(out_wide, 0, 1).reshape(depth, -1)
    mixed = jnp.dot(mixers, out_wide, preferred_element_type=jnp.float32).astype(jnp.bfloat16)
    mixed = lax.psum_scatter(mixed, ("h", "tp"), scatter_dimension=0, tiled=True)
    return mixed, exchange(logs, "h", 1, 0)


def fits(args, sp, tp):
    tokens, _, q_att, k_att, v_att, q_ret, k_ret, v_ret, out_att, _, _, decay = args
    own, heads = tokens.shape[0] // sp, 4 * tp
    return (
        sp == 16
        and tp == 2
        and own == 2 * SPAN_RADIUS
        and q_att.shape[0] == sp * own
        and tokens.shape[1] == sp * own
        and q_att.shape[1] == 2 * heads * HEAD_DIM
        and all(v.shape[1] == heads * HEAD_DIM for v in (k_att, v_att, q_ret, k_ret, v_ret))
    )


def solution(mesh):
    sp, tp = mesh.shape["sp"], mesh.shape["tp"]

    def run(*args):
        if fits(args, sp, tp):
            seq = ("zh", "zl", "y", "x")
            fine = Mesh(mesh.devices.reshape(2, 2, 2, 2, tp), seq + ("tp",))
            step = fused
        else:
            heads = math.gcd(args[3].shape[1], args[5].shape[1]) // HEAD_DIM
            parts = math.gcd(heads // math.gcd(heads, tp), sp)
            seq = ("t", "h")
            fine = Mesh(mesh.devices.reshape(sp // parts, parts, tp), seq + ("tp",))
            step = shards
        body = jax.shard_map(
            step,
            mesh=fine,
            in_specs=(P(seq, "tp"), P("tp"))
            + (P(seq, "tp"),) * 6
            + (P("tp", seq), P("tp", seq), P("tp"), P("tp", seq)),
            out_specs=(P(seq + ("tp",), None), P("tp", seq)),
            check_vma=False,
        )
        return body(*args)

    return run
```

```python
import math

import jax
import jax.numpy as jnp
import numpy as np
from jax import lax
from jax.experimental import pallas as pl
from jax.experimental.pallas import tpu as pltpu
from jax.sharding import Mesh
from jax.sharding import PartitionSpec as P

HEAD_DIM = 128
SPAN_RADIUS = 128
BLOCK = 256
HIGHEST = lax.Precision.HIGHEST
MESH = pl.DeviceIdType.MESH


def gather(x, axis, dim):
    if lax.axis_size(axis) == 1:
        return x
    return lax.all_gather(x, axis, axis=dim, tiled=True)


def exchange(x, axis, split, concat):
    if lax.axis_size(axis) == 1:
        return x
    return lax.all_to_all(x, axis, split, concat, tiled=True)


def halo(shard, axis, width):
    peers, length = lax.axis_size(axis), shard.shape[1]
    up = [(i, i + 1) for i in range(peers - 1)]
    down = [(j, i) for i, j in up]
    before = lax.ppermute(shard[:, length - width :], axis, up)
    after = lax.ppermute(shard[:, :width], axis, down)
    return jnp.concatenate([before, shard, after], axis=1)


def rotate(values, cosine, sine):
    half = values.shape[-1] // 2
    first, second = values[..., :half], values[..., half:]
    return jnp.concatenate(
        [first * cosine - second * sine, second * cosine + first * sine], axis=-1
    ).astype(jnp.bfloat16)


def flip(v, bit):
    return v + bit - 2 * v * bit


class Both:
    def __init__(self, *copies):
        self.copies = copies

    def start(self):
        for copy in self.copies:
            copy.start()

    def wait_send(self):
        for copy in self.copies:
            copy.wait_send()


class Stream:
    def __init__(self, where, remote, refs, pack, split=False):
        self.where, self.remote, self.pack, self.split = where, remote, pack, split
        (
            self.wide, self.away, self.out,
            self.load, self.x_send, self.z_send, self.h_send, self.y_send,
            self.p_recv, self.w_recv, self.more_recv,
        ) = refs

    def fetch(self):
        w = self.where
        targets = (
            (self.out.at[0], 1 - w.g, 1 - w.x),
            (self.out.at[1], w.g, 1 - w.x),
            (self.wide.at[w.own], w.g, w.x),
            (self.away.at[w.x], 1 - w.g, w.x),
        )
        for i, (target, g, x) in enumerate(targets):
            self.pack(2 * g + x, target, self.load.at[i])

    def fetched(self):
        w = self.where
        for i, target in enumerate(
            (self.out.at[0], self.out.at[1], self.wide.at[w.own], self.away.at[w.x])
        ):
            pltpu.make_async_copy(target, target, self.load.at[i]).wait()

    def along_x(self, k):
        w = self.where
        if k == 0:
            return self.remote(
                self.out.at[0], self.away.at[w.x], self.x_send.at[0], self.p_recv.at[0], w.to_x
            )
        return self.remote(
            self.out.at[1], self.wide.at[w.own], self.x_send.at[1], self.w_recv.at[w.own], w.to_x
        )

    def along_z(self, k):
        w = self.where
        x = w.x if k == 0 else 1 - w.x
        s = w.at(w.zh, w.zl, w.y, x)
        return self.remote(
            self.away.at[x], self.wide.at[s], self.z_send.at[k], self.w_recv.at[s], w.to_z
        )

    def near(self, k):
        w = self.where
        return w.at(w.zh, flip(w.zl, k // 2), w.y, flip(w.x, k % 2))

    def far(self, k):
        w = self.where
        return w.at(1 - w.zh, flip(w.zl, 1 - k // 2), w.y, flip(w.x, k % 2))

    def across(self, k):
        w = self.where
        return w.at(1 - w.zh, flip(w.zl, 1 - k // 2), 1 - w.y, flip(w.x, k % 2))

    def half(self, s, i):
        rows = self.wide.shape[1] // 2
        return self.wide.at[s, pl.ds(i * rows, rows), :]

    def halves(self, s, sends, hop, to):
        recvs = (self.w_recv.at[s], self.more_recv.at[hop])
        return [
            self.remote(self.half(s, i), self.half(s, i), sends[i], recvs[i], to)
            for i in range(2)
        ]

    def along_h(self, k):
        s = self.near(k)
        if self.split and k == 3:
            return Both(
                *self.halves(s, (self.h_send.at[3], self.h_send.at[4]), 0, self.where.to_h)
            )
        return self.remote(
            self.wide.at[s], self.wide.at[s], self.h_send.at[k], self.w_recv.at[s], self.where.to_h
        )

    def along_y(self, k, far=0):
        s = self.far(k) if far else self.near(k)
        if self.split and far and k == 3:
            return Both(
                *self.halves(s, (self.y_send.at[7], self.y_send.at[8]), 1, self.where.to_y)
            )
        return self.remote(
            self.wide.at[s], self.wide.at[s],
            self.y_send.at[4 * far + k], self.w_recv.at[s], self.where.to_y,
        )

    def pass_far(self, k):
        if self.split and k == 3:
            sends = (self.h_send.at[3], self.h_send.at[4])
            arrivals = self.halves(self.far(k), sends, 0, self.where.to_h)
            for arrival, copy in zip(arrivals, self.along_y(k, 1).copies):
                arrival.wait_recv()
                copy.start()
        else:
            self.arrive(self.far(k))
            self.along_y(k, 1).start()

    def arrive_far_across(self, k):
        s = self.across(k)
        if self.split and k == 3:
            sends = (self.y_send.at[7], self.y_send.at[8])
            for arrival in self.halves(s, sends, 1, self.where.to_y):
                arrival.wait_recv()
        else:
            self.arrive(s)

    def arrive(self, s):
        self.remote(
            self.wide.at[s], self.wide.at[s], self.x_send.at[0], self.w_recv.at[s], self.where.to_x
        ).wait_recv()

    def arrive_away(self):
        w = self.where
        slot = self.away.at[1 - w.x]
        self.remote(slot, slot, self.x_send.at[0], self.p_recv.at[0], w.to_x).wait_recv()

    def arrive_across(self, far):
        w = self.where
        zh = 1 - w.zh if far else w.zh
        for zl in range(2):
            for x in range(2):
                self.arrive(w.at(zh, zl, 1 - w.y, x))

    def drain(self):
        for k in range(2):
            self.along_x(k).wait_send()
            self.along_z(k).wait_send()
        for k in range(4):
            self.along_h(k).wait_send()
            self.along_y(k).wait_send()
            self.along_y(k, 1).wait_send()


class Place:
    def __init__(self):
        self.zh, self.zl, self.y, self.x, self.c = (
            lax.axis_index(a) for a in ("zh", "zl", "y", "x", "tp")
        )
        self.g = lax.rem(self.zh + self.zl, 2)
        self.h = 2 * self.g + self.x
        self.own = self.at(self.zh, self.zl, self.y, self.x)
        self.b = 2 * self.zl + self.x
        self.to_x = {"x": 1 - self.x}
        self.to_z = {"zl": 1 - self.zl}
        self.to_y = {"y": 1 - self.y}
        self.to_h = {"zh": 1 - self.zh, "zl": 1 - self.zl}
        self.to_hy = {"zh": 1 - self.zh, "zl": 1 - self.zl, "y": 1 - self.y}
        self.to_zx = {"zl": 1 - self.zl, "x": 1 - self.x}
        self.to_c = {"tp": 1 - self.c}
        self.to_zc = {"zl": 1 - self.zl, "tp": 1 - self.c}

    @staticmethod
    def at(zh, zl, y, x):
        return ((zh * 2 + zl) * 2 + y) * 2 + x


def fused_kernel(
    tokens, gain, q_att, k_att, v_att, q_ret, k_ret, v_ret, out_att, out_ret, sink, decay,
    cos_t, sin_t, base,
    mixed, logs_out,
    raw, scl, ssq, gains, acc_a, acc_r, kvext, qrot, rets, dec, cumr, cumc, coef, states, stall, crossing,
    mix, bias, logm, lsend, lrecv, mine, kept, give, take, s1, r1, s2, r2,
    t_load, t_x, t_z, t_c, t_recv, g_sem, d_sem, halo_sem, st_sem, l_sem, go,
    give_s, take_r, s1_s, r1_r, s2_s, r2_r,
    *streams,
):
    w = Place()
    y = w.y
    f32, bf16 = jnp.float32, jnp.bfloat16
    own, half_d = tokens.shape
    rows = 4 * own
    run_rows = 2 * own
    total_rows = 16 * own
    H = HEAD_DIM
    edge = SPAN_RADIUS

    def remote(src, dst, send, recv, to):
        return pltpu.make_async_remote_copy(
            src_ref=src, dst_ref=dst, send_sem=send, recv_sem=recv,
            device_id=to, device_id_type=MESH,
        )

    def lanes(h, n):
        return pl.ds(pl.multiple_of(h * n, n), n)

    def pack_cols(parts):
        def pack(h, target, sem):
            start = 0
            for ref in parts:
                n = ref.shape[1] // 4
                pltpu.make_async_copy(
                    ref.at[:, lanes(h, n)], target.at[:, pl.ds(start, n)], sem
                ).start()
                start += n
        return pack

    def pack_rows(parts):
        def pack(h, target, sem):
            start = 0
            for ref in parts:
                n = ref.shape[0] // 4
                pltpu.make_async_copy(
                    ref.at[lanes(h, n), :], target.at[pl.ds(start, n), :], sem
                ).start()
                start += n
        return pack

    n = len(streams) // 3
    A = Stream(w, remote, streams[:n], pack_cols((q_att, k_att, v_att)), True)
    R = Stream(w, remote, streams[n : 2 * n], pack_cols((q_ret, k_ret, v_ret)))
    O = Stream(w, remote, streams[2 * n :], pack_rows((out_att, out_ret)))

    token_load = pltpu.make_async_copy(tokens, raw.at[w.c, w.b], t_load.at[0])
    gain_load = pltpu.make_async_copy(gain, gains.at[w.c], t_load.at[1])
    decay_load = pltpu.make_async_copy(decay, dec.at[w.zh, w.y, w.zl, w.x], t_load.at[2])

    def block(zl, x):
        return 2 * zl + x

    def order(k):
        return block((w.zl, 1 - w.zl)[k // 2], (w.x, 1 - w.x)[k % 2])

    def token(e, k, part, send, to):
        here = raw.at[e, order(k)]
        if part is not None:
            here = here.at[pl.ds(part * edge, edge), :]
        return remote(here, here, send, t_recv.at[e, order(k), part or 0], to)

    tokens_x = [token(w.c, 0, None, t_x.at[0], w.to_x)]
    tokens_x += [token(w.c, 2, i, t_x.at[1 + i], w.to_x) for i in range(2)]
    tokens_z = token(w.c, 0, None, t_z.at[0], w.to_z)
    tokens_c = [token(w.c, k, None, t_c.at[k], w.to_c) for k in range(3)]
    tokens_c += [token(w.c, 3, i, t_c.at[3 + i], w.to_c) for i in range(2)]

    def token_arrive(k, e=None, part=None):
        token(w.c if e is None else e, k, part, t_x.at[0], w.to_x).wait_recv()

    gain_c = remote(gains.at[w.c], gains.at[w.c], g_sem.at[0], g_sem.at[1], w.to_c)

    def others(i):
        return tuple(flip(v, (i >> k) & 1) for v, k in ((w.zh, 3), (w.zl, 2), (w.y, 1), (w.x, 0)))

    def peer(i):
        return dict(zip(("zh", "zl", "y", "x"), others(i)))

    def decay_send(i):
        here = dec.at[w.zh, w.y, w.zl, w.x]
        return remote(here, here, d_sem.at[0, i], d_sem.at[1, i], peer(i))

    def decay_arrive(i):
        zh, zl, yy, x = others(i)
        here = dec.at[zh, yy, zl, x]
        remote(here, here, d_sem.at[0, i], d_sem.at[1, i], peer(i)).wait_recv()

    decay_load.start()
    R.fetch()
    A.fetch()
    gain_load.start()
    token_load.start()
    O.fetch()

    barrier = pltpu.get_barrier_semaphore()
    for to in (w.to_c, w.to_zc):
        pl.semaphore_signal(barrier, inc=1, device_id=to, device_id_type=MESH)
    for i in range(1, 16):
        pl.semaphore_signal(barrier, inc=1, device_id=peer(i), device_id_type=MESH)
    pl.semaphore_wait(barrier, 17)

    middle = w.g == 1

    decay_load.wait()
    for i in range(1, 16):
        decay_send(i).start()
    R.fetched()
    R.along_x(0).start()
    R.along_z(0).start()
    R.along_y(0).start()
    A.fetched()
    A.along_x(0).start()
    A.along_z(0).start()
    A.along_y(0).start()
    R.along_x(1).start()
    A.along_x(1).start()

    @pl.when(middle)
    def _():
        R.along_h(0).start()
        A.along_h(0).start()

    O.fetched()
    O.along_x(1).start()
    O.along_x(0).start()
    token_load.wait()
    tokens_x[0].start()
    gain_load.wait()
    gain_c.start()
    tokens_c[0].start()

    def scale(e, b, first=0, last=None):
        @pl.loop(first // 16, (own if last is None else last) // 16)
        def _(i):
            value = raw[e, b, pl.ds(pl.multiple_of(i * 16, 16), 16), :].astype(f32)
            at = pl.ds(pl.multiple_of(b * own + i * 16, 16), 16)
            scl[e, at, :] = (value * gains[e]).astype(bf16)
            square = value * value
            total = square[:, :H]
            for k in range(1, half_d // H):
                total = total + square[:, k * H : (k + 1) * H]
            ssq[e, at, :] = total

    @pl.when((w.zh == 0) & (w.y == 0))
    def _():
        kvext[0, :, 0:edge, :] = jnp.zeros((2, edge, H), bf16)

    @pl.when((w.zh == 1) & (w.y == 1))
    def _():
        kvext[1, :, edge + run_rows :, :] = jnp.zeros((2, edge, H), bf16)

    scale(w.c, w.b)
    for stream in (R, A):
        stream.arrive_away()
        stream.along_z(1).start()
    tokens_z.start()
    remote(gains.at[1 - w.c], gains.at[1 - w.c], g_sem.at[0], g_sem.at[1], w.to_c).wait_recv()
    token_arrive(0, 1 - w.c)
    scale(1 - w.c, w.b)

    def pass_near(stream, k):
        stream.arrive(stream.near(k))
        stream.along_y(k).start()

        @pl.when(middle)
        def _():
            stream.along_h(k).start()

    def pass_far(stream, k):
        stream.pass_far(k)

    pass_near(R, 2)
    pass_near(A, 2)
    for k in (1, 3):
        pass_near(R, k)
        pass_near(A, k)

    O.along_y(0).start()
    O.along_z(0).start()

    @pl.when(w.g == 0)
    def _():
        for stream in (R, A):
            for k in range(4):
                stream.along_h(k).start()

    @pl.when(middle)
    def _():
        O.along_h(0).start()

    row = lax.broadcasted_iota(jnp.int32, bias.shape, 0)
    shift = lax.broadcasted_iota(jnp.int32, bias.shape, 1) - lax.rem(row, edge)
    bias[...] = jnp.where((shift >= 0) & (shift <= 2 * edge), 0.0, -jnp.inf)
    logm[...] = jnp.zeros_like(logm)
    for i in range(1, 16):
        decay_arrive(i)

    lane = lax.broadcasted_iota(jnp.int32, (8, run_rows), 1)
    for slot in range(2):
        row = jnp.concatenate(
            [dec[w.zh, w.y, slot, x, pl.ds(w.h, 1), :] for x in range(2)], axis=1
        )
        row = jnp.broadcast_to(row, (8, run_rows))
        step = 1
        while step < run_rows:
            row = row + jnp.where(lane >= step, pltpu.roll(row, step, axis=1), 0.0)
            step *= 2
        cumr[slot] = row
        cumc[slot] = jnp.transpose(jnp.broadcast_to(row[0:1], (H, run_rows)))
    lane = lax.broadcasted_iota(jnp.int32, (8, H), 1)
    run = lax.broadcasted_iota(jnp.int32, (8, H), 0)
    totals = jnp.zeros((8, H), f32)
    for zh in range(2):
        for slot in range(2):
            for yy in range(2):
                pair = sum(dec[zh, yy, slot, x, pl.ds(w.h, 1), :] for x in range(2))
                value = jnp.sum(pair, axis=1, keepdims=True)
                totals = jnp.where(lane == 4 * zh + 2 * slot + yy, value, totals)
    for slot in range(2):
        me = 4 * w.zh + 2 * slot + w.y
        between = (lane > jnp.minimum(run, me)) & (lane < jnp.maximum(run, me))
        factor = jnp.exp(jnp.sum(jnp.where(between, totals, 0.0), axis=1, keepdims=True))
        factor = jnp.broadcast_to(factor, (8, H))
        near = run // 4 == w.zh
        coef[slot, 0] = jnp.where(near & (run < me), factor, 0.0)
        coef[slot, 1] = jnp.where(near & (run > me), factor, 0.0)
        between = (lane > jnp.where(w.zh == 0, me, 3)) & (lane < jnp.where(w.zh == 0, 4, me))
        factor = jnp.exp(jnp.sum(jnp.where(between, totals, 0.0), axis=1, keepdims=True))
        coef[slot, 2] = jnp.broadcast_to(factor, (8, H))

    pass_near(O, 1)

    @pl.when(middle)
    def _():
        for stream in (R, A):
            for k in (0, 2, 1, 3):
                pass_far(stream, k)

    def part_of(stream, zh, b, start, width):
        at = pl.ds(pl.multiple_of(b * own, own), own)
        depth = half_d // own
        weight = stream.wide[pl.ds(zh * depth, depth), :, start : start + width]
        return jnp.dot(
            scl[zh, at, :], weight.reshape(half_d, width), preferred_element_type=f32
        )

    def first_part(stream, acc, b):
        at = pl.ds(pl.multiple_of(b * own, own), own)
        start = 0
        while start < acc.shape[1]:
            width = min(2 * H, acc.shape[1] - start)
            acc[at, start : start + width] = part_of(stream, w.zh, b, start, width)
            start += width

    def pair_of(stream, zl, yy, b, start, width):
        zh = 1 - w.zh
        at = pl.ds(pl.multiple_of(b * own, own), own)
        depth = pl.ds(pl.multiple_of((2 * zl + yy) * 2 * own, 2 * own), 2 * own)
        weight = stream.wide[pl.ds(w.at(zh, zl, yy, 0), 2), :, start : start + width]
        return jnp.dot(
            scl[zh, at, depth], weight.reshape(2 * own, width), preferred_element_type=f32
        )

    def add_pair(stream, acc, zl, yy, b):
        at = pl.ds(pl.multiple_of(b * own, own), own)
        for start in range(0, acc.shape[1], 2 * H):
            width = min(2 * H, acc.shape[1] - start)
            acc[at, start : start + width] += pair_of(stream, zl, yy, b, start, width)

    def last_of(stream, acc, b, start, width):
        at = pl.ds(pl.multiple_of(b * own, own), own)
        return acc[at, start : start + width] + pair_of(stream, w.zl, 1 - w.y, b, start, width)

    def whole_of(stream, acc, b, start, width):
        at = pl.ds(pl.multiple_of(b * own, own), own)
        return acc[at, start : start + width] + part_of(stream, 1 - w.zh, b, start, width)

    token_arrive(2)
    for copy in tokens_x[1:]:
        copy.start()
    tokens_c[2].start()
    scale(w.c, order(2))
    token_arrive(2, 1 - w.c)
    scale(1 - w.c, order(2))
    token_arrive(1)
    tokens_c[1].start()
    scale(w.c, order(1))

    @pl.when(w.g == 0)
    def _():
        pass_far(R, 0)

    O.arrive_away()
    O.along_z(1).start()
    token_arrive(1, 1 - w.c)
    scale(1 - w.c, order(1))

    @pl.when(w.g == 0)
    def _():
        pass_far(R, 1)

    R.arrive_across(0)
    A.arrive_across(0)

    @pl.loop(0, 3)
    def _(i):
        k = 2 - i
        b = block(flip(w.zl, k // 2), flip(w.x, k % 2))
        first_part(R, acc_r, b)
        first_part(A, acc_a, b)

    @pl.when(w.g == 0)
    def _():
        pass_far(R, 2)

    token_arrive(3, None, 0)
    tokens_c[3].start()
    scale(w.c, order(3), 0, edge)
    token_arrive(3, 1 - w.c, 0)
    scale(1 - w.c, order(3), 0, edge)

    @pl.when(w.g == 0)
    def _():
        pass_far(R, 3)
        pass_far(A, 0)

    token_arrive(3, None, 1)
    tokens_c[4].start()

    @pl.when(w.g == 0)
    def _():
        pass_far(A, 1)

    scale(w.c, order(3), edge, own)
    token_arrive(3, 1 - w.c, 1)
    scale(1 - w.c, order(3), edge, own)
    first_part(R, acc_r, order(3))
    first_part(A, acc_a, order(3))

    def inverse(b):
        at = pl.ds(pl.multiple_of(b * own, own), own)
        squares = jnp.sum(ssq[0, at, :] + ssq[1, at, :], axis=1, keepdims=True)
        return lax.rsqrt(squares / (2 * half_d) + 1e-06)

    def angles(b):
        s = w.at(w.zh, b // 2, w.y, b % 2)
        c0, s0, s0n, c0n = (base[i, pl.ds(s, 1), :] for i in range(4))
        cosine = cos_t[...] * c0 - sin_t[...] * s0
        sine = cos_t[...] * s0n + sin_t[...] * c0n
        return cosine, sine

    def turn(value, cosine, sine):
        return (value * cosine + pltpu.roll(value, H // 2, axis=1) * sine).astype(bf16)

    def keys_values(b):
        scale_b = inverse(b)
        cosine, sine = angles(b)
        both = last_of(A, acc_a, b, 2 * H, 2 * H) * scale_b
        inner = pl.ds(pl.multiple_of(edge + (b % 2) * own, edge), own)
        kvext[b // 2, 0, inner, :] = turn(both[:, :H], cosine, sine)
        kvext[b // 2, 1, inner, :] = both[:, H:].astype(bf16)

    def queries(b):
        at = pl.ds(pl.multiple_of(b * own, own), own)
        cosine, sine = angles(b)
        query = last_of(A, acc_a, b, 0, 2 * H) * inverse(b)
        qrot[at, :H] = turn(query[:, :H], cosine, sine)
        qrot[at, H:] = turn(query[:, H:], cosine, sine)

    R.arrive_across(1)

    def retention_inputs(b):
        at = pl.ds(pl.multiple_of(b * own, own), own)
        scale_b = inverse(b)
        both = whole_of(R, acc_r, b, 0, 2 * H)
        rets[0, at, :] = (both[:, :H] * scale_b).astype(bf16)
        rets[1, at, :] = (both[:, H:] * (scale_b * H ** (-0.5))).astype(bf16)
        rets[2, at, :] = (whole_of(R, acc_r, b, 2 * H, H) * scale_b).astype(bf16)

    @pl.when(w.g == 0)
    def _():
        pass_far(A, 2)

    @pl.loop(0, 4, unroll=True)
    def _(b):
        retention_inputs(b)

    for slot in range(2):
        at = pl.ds(slot * run_rows, run_rows)
        last = cumr[slot, 0:1, run_rows - 1 : run_rows]
        key, value = rets[1, at, :].astype(f32), rets[2, at, :]
        for i, weight in enumerate((jnp.exp(last - cumc[slot]), jnp.exp(cumc[slot]))):
            lhs = (key * weight).astype(bf16)
            state = lax.dot_general(
                lhs, value, (((0,), (0,)), ((), ())), preferred_element_type=f32
            ).astype(bf16)
            stall[y, slot, i] = state
    total = jnp.zeros((H, H), f32)
    for slot in range(2):
        total = total + coef[slot, 2, 0:1, :] * stall[y, slot, w.zh].astype(f32)
    crossing[2] = total.astype(bf16)
    state_sends = [
        remote(stall.at[y], stall.at[y], st_sem.at[0, 0], st_sem.at[1, 0], w.to_y),
        remote(crossing.at[2], crossing.at[0], st_sem.at[0, 1], st_sem.at[1, 1], w.to_h),
        remote(crossing.at[2], crossing.at[1], st_sem.at[0, 2], st_sem.at[1, 2], w.to_hy),
    ]
    state_sends[1].start()
    state_sends[2].start()

    def inner_tile(i):
        slot = i // 2
        at = pl.ds(pl.multiple_of(i * own, own), own)
        keys = pl.ds(pl.multiple_of(slot * run_rows, run_rows), run_rows)
        score = lax.dot_general(
            rets[0, at, :], rets[1, keys, :], (((1,), (1,)), ((), ())),
            preferred_element_type=f32,
        )
        column = cumc[slot, pl.ds(pl.multiple_of((i % 2) * own, own), own), :]
        column = jnp.concatenate([column] * (run_rows // H), axis=1)
        weight = jnp.exp(-jnp.abs(column - cumr[slot, 0:1, :]))
        acc_r[at, :H] = jnp.dot(
            (score * weight).astype(bf16), rets[2, keys, :], preferred_element_type=f32
        )

    @pl.loop(0, 4, unroll=True)
    def _(i):
        inner_tile(i)

    @pl.when(w.g == 0)
    def _():
        pass_far(A, 3)

    @pl.loop(0, 8)
    def _(i):
        add_pair(A, acc_a, i // 4, y, i % 4)

    for k in range(2):
        A.arrive_far_across(k)

    @pl.loop(0, 4)
    def _(b):
        add_pair(A, acc_a, 1 - w.zl, 1 - y, b)

    for k in range(2, 4):
        A.arrive_far_across(k)

    @pl.loop(0, 4, unroll=True)
    def _(b):
        keys_values(b)

    head, tail, before_at, after_at = edge, run_rows, 0, edge + run_rows

    def pick(a, b):
        return a + (b - a) * y

    def piece(slot, start):
        return kvext.at[slot, :, pl.ds(pl.multiple_of(start, edge), edge), :]

    halo_y = [
        remote(
            piece(pick(s0, s1), pick(f0, f1)), piece(pick(d0, d1), pick(o0, o1)),
            halo_sem.at[0, i], halo_sem.at[1, i], w.to_y,
        )
        for i, (s0, f0, d0, o0, s1, f1, d1, o1) in enumerate(
            (
                (0, tail, 0, before_at, 0, head, 0, after_at),
                (1, head, 0, after_at, 0, tail, 1, before_at),
                (1, tail, 1, before_at, 1, head, 1, after_at),
            )
        )
    ]
    halo_far = remote(
        piece(pick(0, 1), pick(head, tail)), piece(pick(1, 0), pick(after_at, before_at)),
        halo_sem.at[0, 3], halo_sem.at[1, 3], w.to_hy,
    )
    has_far = ((y == 0) & (w.zh == 1)) | ((y == 1) & (w.zh == 0))
    for copy in halo_y:
        copy.start()

    @pl.when(has_far)
    def _():
        halo_far.start()

    state_sends[0].start()

    @pl.when(middle)
    def _():
        for copy in state_sends[1:]:
            copy.wait_send()

        @pl.when(has_far)
        def _():
            halo_far.wait_send()

        for to in (w.to_z, w.to_zc):
            pl.semaphore_signal(go, inc=1, device_id=to, device_id_type=MESH)

    @pl.when(middle)
    def _():
        for k in (2, 3):
            O.arrive(O.near(k))
            O.along_h(k).start()
            O.along_y(k).start()

    @pl.loop(0, 4, unroll=True)
    def _(b):
        queries(b)

    def halo_arrive(slot, start, i, to):
        here = piece(slot, start)
        remote(here, here, halo_sem.at[0, i], halo_sem.at[1, i], to).wait_recv()

    def attend_tile(i, at_end):
        slot, j = i // 4, i % 4
        query = qrot[pl.ds(pl.multiple_of(i * edge, edge), edge), :]
        query = jnp.concatenate([query[:, :H], query[:, H:]], axis=0)
        span = pl.ds(pl.multiple_of(j * edge, edge), 3 * edge)
        key, value = kvext[slot, 0, span, :], kvext[slot, 1, span, :]
        score = lax.dot_general(
            query, key, (((1,), (1,)), ((), ())), preferred_element_type=f32
        ) * H ** (-0.5)
        masked = score + bias[...]
        if at_end:
            col = lax.broadcasted_iota(jnp.int32, (1, 3 * edge), 1)
            start = w.at(w.zh, slot, y, 0) * own + j * edge - edge
            inside = (col >= -start) & (col < total_rows - start)
            masked = masked + jnp.where(inside, 0.0, -jnp.inf)
        first = lax.broadcasted_iota(jnp.int32, (2 * edge, 1), 0) < edge
        limit = jnp.where(first, sink[2 * w.h], sink[2 * w.h + 1])
        top = jnp.maximum(jnp.max(masked, axis=1, keepdims=True), limit)
        expo = jnp.exp(masked - top)
        total = jnp.sum(expo, axis=1, keepdims=True) + jnp.exp(limit - top)
        logs = top + jnp.log(total)
        probs = (expo * (1.0 / total)).astype(bf16)
        result = jnp.dot(probs, value, preferred_element_type=f32).astype(bf16)
        at = pl.ds(pl.multiple_of((i // 2) * edge, edge), edge)
        mix[i % 2, at, 0:H] = result[:edge]
        mix[i % 2, at, H : 2 * H] = result[edge:]
        column = lax.broadcasted_iota(jnp.int32, (2 * edge, H), 1)
        logm[...] = jnp.where(column == i, logs, logm[...])

    @pl.when(w.g == 0)
    def _():
        pl.semaphore_wait(go, 2)
        for k in range(4):
            if k > 1:
                O.arrive(O.near(k))
            O.along_h(k).start()

    @pl.loop(0, 4, unroll=True)
    def _(i):
        attend_tile(4 * (i // 2) + 1 + i % 2, False)

    halo_arrive(pick(0, 0), pick(after_at, before_at), 0, w.to_y)
    halo_arrive(pick(1, 0), pick(before_at, after_at), 1, w.to_y)
    halo_arrive(pick(1, 1), pick(after_at, before_at), 2, w.to_y)

    @pl.when(has_far)
    def _():
        halo_arrive(pick(0, 1), pick(before_at, after_at), 3, w.to_hy)

    @pl.when(w.g == 0)
    def _():
        O.along_y(2).start()
        O.along_y(3).start()

    @pl.loop(0, 4, unroll=True)
    def _(i):
        attend_tile(4 * (i // 2) + 3 * (i % 2), True)

    for i, here in enumerate((stall.at[1 - y], crossing.at[0], crossing.at[1])):
        remote(here, here, st_sem.at[0, i], st_sem.at[1, i], w.to_y).wait_recv()
    crossed = crossing[0].astype(f32) + crossing[1].astype(f32)
    for slot in range(2):
        for i in range(2):
            total = jnp.where(w.zh == 1 - i, 1.0, 0.0) * coef[slot, 2, 0:1, :] * crossed
            for s in range(2):
                for yy in range(2):
                    for zh in range(2):
                        r = 4 * zh + 2 * s + yy
                        total = total + coef[slot, i, r : r + 1, :] * stall[yy, s, i].astype(f32)
            states[slot, :, i * H : (i + 1) * H] = total.astype(bf16)

    def finish_tile(i):
        slot = i // 2
        at = pl.ds(pl.multiple_of(i * own, own), own)
        column = cumc[slot, pl.ds(pl.multiple_of((i % 2) * own, own), own), :]
        last = cumr[slot, 0:1, run_rows - 1 : run_rows]
        carried = jnp.dot(rets[0, at, :], states[slot], preferred_element_type=f32)
        value = (
            acc_r[at, :H] + jnp.exp(column) * carried[:, :H]
            + jnp.exp(last - column) * carried[:, H:]
        )
        value = value - jnp.mean(value, axis=1, keepdims=True)
        value = value * lax.rsqrt(jnp.mean(value * value, axis=1, keepdims=True) + 1e-06)
        value = value.astype(bf16)
        out = pl.ds(pl.multiple_of(i * edge, edge), edge)
        mix[0, out, 2 * H :] = value[:edge]
        mix[1, out, 2 * H :] = value[edge:]

    @pl.loop(0, 4, unroll=True)
    def _(i):
        finish_tile(i)

    @pl.when(middle)
    def _():
        for k in range(2):
            pass_far(O, k)

    turned = jnp.transpose(logm[...])
    for b in range(4):
        lsend[b] = turned[2 * b : 2 * b + 2]
        lrecv[w.h] = jnp.where(w.b == b, turned[2 * b : 2 * b + 2], lrecv[w.h] if b else 0.0)
    h_of = lambda zl, x: 2 * lax.rem(w.zh + zl, 2) + x
    log_to = (
        (1 - w.x, w.zl, w.to_x), (w.x, 1 - w.zl, w.to_z), (1 - w.x, 1 - w.zl, w.to_zx),
    )
    log_sends = [
        remote(lsend.at[block(zl, x)], lrecv.at[w.h], l_sem.at[0, i], l_sem.at[1, i], to)
        for i, (x, zl, to) in enumerate(log_to)
    ]

    for copy in log_sends:
        copy.start()

    chunks = 8

    def columns_of(i, x):
        far, across, zl = i // 4, (i // 2) % 2, i % 2
        return w.at(flip(w.zh, far), zl, flip(y, across), x)

    def swap(i):
        return remote(give.at[i], take.at[i], give_s.at[i], take_r.at[i], w.to_c)

    def x_first(i, k):
        return 1 if k == 0 else jnp.where(i < 1, 1, 0)

    def toward(dx):
        return {"x": flip(w.x, dx), "zl": flip(w.zl, 1 - dx)}

    def first_hop(i, k):
        to = toward(x_first(i, k))
        return remote(s1.at[i, k], r1.at[i, k], s1_s.at[i, k], r1_r.at[i, k], to)

    def second_hop(i, k):
        to = toward(1 - x_first(i, k))
        return remote(s2.at[i, k], r2.at[i, k], s2_s.at[i, k], r2_r.at[i, k], to)

    def side(i, k, j, cross):
        dx = x_first(i, k)
        zl = dx * j + (1 - dx) * flip(w.zl, cross)
        x = dx * flip(w.x, cross) + (1 - dx) * j
        return block(zl, x)

    def part(b):
        return pl.ds(pl.multiple_of(b * edge, edge), edge)

    lag = 6

    @pl.loop(0, chunks + lag)
    def _(step):
        @pl.when(step < chunks)
        def _():
            i = step

            @pl.when((i // 2) % 2 == 1)
            def _():
                for x in range(2):
                    O.arrive(columns_of(i, x))

            @pl.when((i == 2) & (w.g == 0))
            def _():
                for k in range(2):
                    pass_far(O, k)

            @pl.when(i == 3)
            def _():
                for k in range(2, 4):
                    pass_far(O, k)

            for k in range(2):
                give[i, k] = jnp.dot(
                    mix[1 - w.c], O.wide[columns_of(i, k)], preferred_element_type=f32
                ).astype(bf16)
            swap(i).start()
            for k in range(2):
                mine[i % 4, k] = jnp.dot(
                    mix[w.c], O.wide[columns_of(i, k)], preferred_element_type=f32
                )

        @pl.when((step >= 1) & (step < chunks + 1))
        def _():
            i = step - 1
            swap(i).wait_recv()
            for k in range(2):
                for j in range(2):
                    b = side(i, k, j, 1)
                    total = mine[i % 4, k, part(b), :] + take[i, k, part(b), :].astype(f32)
                    s1[i, k, j] = total.astype(bf16)
                first_hop(i, k).start()
            for k in range(2):
                for j in range(2):
                    b = side(i, k, j, 0)
                    mine[i % 4, k, part(b), :] += take[i, k, part(b), :].astype(f32)

        @pl.when((step >= 2) & (step < chunks + 2))
        def _():
            i = step - 2
            for k in range(2):
                first_hop(i, k).wait_recv()
                dx = x_first(i, k)
                j = flip(dx * w.zl + (1 - dx) * w.x, 1)
                b = side(i, k, j, 0)
                s2[i, k] = (mine[i % 4, k, part(b), :] + r1[i, k, j].astype(f32)).astype(bf16)
                second_hop(i, k).start()
                j = flip(j, 1)
                kept[i, k] = mine[i % 4, k, part(w.b), :] + r1[i, k, j].astype(f32)

        @pl.when(step >= lag)
        def _():
            i = step - lag
            for k in range(2):
                second_hop(i, k).wait_recv()
                at = pl.ds(pl.multiple_of(columns_of(i, k) * own, own), own)
                mixed[:, at] = (kept[i, k] + r2[i, k].astype(f32)).astype(mixed.dtype)

    for i, (x, zl, to) in enumerate(log_to):
        here = lrecv.at[h_of(zl, x)]
        remote(here, here, l_sem.at[0, i], l_sem.at[1, i], to).wait_recv()
    for h in range(4):
        for head_i in range(2):
            for t in range(2):
                logs_out[2 * h + head_i : 2 * h + head_i + 1, t * edge : (t + 1) * edge] = (
                    lrecv[h, t : t + 1, head_i * edge : (head_i + 1) * edge]
                )

    for stream in (A, R, O):
        stream.drain()
    for i in range(1, 16):
        decay_send(i).wait_send()
    for copy in tokens_x + tokens_c + [tokens_z, gain_c]:
        copy.wait_send()
    for copy in halo_y + state_sends[:1] + log_sends:
        copy.wait_send()

    @pl.when(w.g == 0)
    def _():
        for copy in state_sends[1:]:
            copy.wait_send()

        @pl.when(has_far)
        def _():
            halo_far.wait_send()

    @pl.loop(0, chunks)
    def _(i):
        swap(i).wait_send()
        for k in range(2):
            first_hop(i, k).wait_send()
            second_hop(i, k).wait_send()


def fused(*args):
    tokens, gain, q_att = args[:3]
    out_att, out_ret, sink, decay_log = args[8:]
    own, half_d = tokens.shape
    rows, run_rows = 4 * own, 2 * own
    H, edge = HEAD_DIM, SPAN_RADIUS
    bf16, f32 = jnp.bfloat16, jnp.float32
    dma, vmem = pltpu.SemaphoreType.DMA, pltpu.VMEM
    depth = q_att.shape[0]
    width = out_att.shape[1] * 16

    freqs = 10000.0 ** (-np.arange(0, H, 2, dtype=np.float64) / H)
    freqs = np.concatenate([freqs, freqs])[None, :]
    sign = np.where(np.arange(H) < H // 2, -1.0, 1.0)[None, :]
    inner = np.arange(own)[:, None] * freqs
    outer = (np.arange(16) * own)[:, None] * freqs
    cos_t, sin_t = jnp.asarray(np.cos(inner), f32), jnp.asarray(np.sin(inner), f32)
    base = jnp.asarray(
        np.stack([np.cos(outer), np.sin(outer), sign * np.sin(outer), sign * np.cos(outer)]), f32
    )

    def stream(block):
        return [
            vmem((16,) + block, bf16), vmem((2,) + block, bf16), vmem((2,) + block, bf16),
            dma((4,)), dma((2,)), dma((2,)), dma((5,)), dma((9,)), dma((1,)), dma((16,)), dma((2,)),
        ]

    out_rows = (out_att.shape[0] + out_ret.shape[0]) // 4
    tile = (8, 2, 4 * edge, own)
    hbm, inside = pl.BlockSpec(memory_space=pl.ANY), pl.BlockSpec(memory_space=pltpu.VMEM)
    mixed, logs = pl.pallas_call(
        fused_kernel,
        out_shape=(
            jax.ShapeDtypeStruct((own // 2, width), bf16),
            jax.ShapeDtypeStruct((sink.shape[0], own), f32),
        ),
        in_specs=[hbm] * 10 + [pl.BlockSpec(memory_space=pltpu.SMEM), hbm] + [inside] * 3,
        out_specs=[inside] * 2,
        scratch_shapes=[
            vmem((2, 4, own, half_d), bf16),
            vmem((2, rows, half_d), bf16),
            vmem((2, rows, H), f32),
            vmem((2, 1, half_d), f32),
            vmem((rows, 4 * H), f32),
            vmem((rows, 3 * H), f32),
            vmem((2, 2, run_rows + 2 * edge, H), bf16),
            vmem((rows, 2 * H), bf16),
            vmem((3, rows, H), bf16),
            vmem((2, 2, 2, 2) + decay_log.shape, f32),
            vmem((2, 8, run_rows), f32),
            vmem((2, run_rows, H), f32),
            vmem((2, 3, 8, H), f32),
            vmem((2, H, 2 * H), bf16),
            vmem((2, 2, 2, H, H), bf16), vmem((3, H, H), bf16),
            vmem((2, 4 * edge, 3 * H), bf16),
            vmem((2 * edge, 3 * edge), f32),
            vmem((2 * edge, H), f32),
            vmem((4, 2, 2 * edge), f32),
            vmem((4, 2, 2 * edge), f32),
            vmem((4,) + tile[1:], f32), vmem((8, 2, edge, own), f32), vmem(tile, bf16), vmem(tile, bf16),
            vmem((8, 2, 2, edge, own), bf16), vmem((8, 2, 2, edge, own), bf16),
            vmem((8, 2, edge, own), bf16), vmem((8, 2, edge, own), bf16),
            dma((3,)), dma((3,)), dma((1,)), dma((5,)), dma((2, 4, 2)), dma((2,)), dma((2, 16)),
            dma((2, 4)), dma((2, 3)), dma((2, 3)), pltpu.SemaphoreType.REGULAR,
            dma((8,)), dma((8,)), dma((8, 2)), dma((8, 2)), dma((8, 2)), dma((8, 2)),
        ]
        + stream((depth, 4 * H))
        + stream((depth, 3 * H))
        + stream((out_rows, own)),
        compiler_params=pltpu.CompilerParams(
            collective_id=0, has_side_effects=True, vmem_limit_bytes=67043328
        ),
        cost_estimate=pl.CostEstimate(
            flops=10**11, bytes_accessed=2 * 10**7, transcendentals=0
        ),
    )(
        tokens, gain.reshape(1, half_d), *args[2:10], sink, decay_log, cos_t, sin_t, base
    )
    return mixed, logs


def attend(query, key, value, sink, offset, total_rows):
    rows, kv, group, _ = query.shape
    ext = halo(jnp.stack([key, value]), "t", SPAN_RADIUS)
    size = min(rows, BLOCK)
    count = rows // size
    span = size + 2 * SPAN_RADIUS
    pieces = jnp.stack([ext[:, b * size : b * size + span] for b in range(count)])
    blocks = query.reshape(count, size, kv, group, HEAD_DIM)
    scores = jnp.einsum(
        "bqhgd,bkhd->bhgqk", blocks, pieces[:, 0], preferred_element_type=jnp.float32
    ) * HEAD_DIM ** (-0.5)
    base = offset + jnp.arange(count, dtype=jnp.int32) * size
    query_pos = base[:, None] + jnp.arange(size, dtype=jnp.int32)
    key_pos = base[:, None] - SPAN_RADIUS + jnp.arange(span, dtype=jnp.int32)
    spacing = key_pos[:, None, :] - query_pos[:, :, None]
    inside = (key_pos >= 0) & (key_pos < total_rows)
    valid = (jnp.abs(spacing) <= SPAN_RADIUS) & inside[:, None, :]
    masked = jnp.where(valid[:, None, None], scores, -jnp.inf)
    limit = sink[None, :, :, None]
    top = jnp.maximum(jnp.max(masked, axis=-1), limit)
    expo = jnp.exp(masked - top[..., None])
    total = jnp.sum(expo, axis=-1) + jnp.exp(limit - top)
    logs = top + jnp.log(total)
    probs = (expo / total[..., None]).astype(jnp.bfloat16)
    result = jnp.einsum(
        "bhgqk,bkhd->bqhgd", probs, pieces[:, 1], preferred_element_type=jnp.float32
    ).astype(jnp.bfloat16)
    logs = jnp.transpose(logs, (1, 2, 0, 3)).reshape(kv * group, rows)
    return result.reshape(rows, kv * group * HEAD_DIM), logs


def retain(query, key, value, decay):
    rows, heads, _ = query.shape
    peers, index = lax.axis_size("t"), lax.axis_index("t")
    cumul = jnp.cumsum(decay, axis=1)
    last = cumul[:, -1]
    query_f, key_f, value_f = (v.astype(jnp.float32) for v in (query, key, value))
    trailing = jnp.exp(last[:, None] - cumul)
    leading = jnp.exp(cumul)
    forward = jnp.einsum("hk,khd,khe->hde", trailing, key_f, value_f, precision=HIGHEST)
    backward = jnp.einsum("hk,khd,khe->hde", leading, key_f, value_f, precision=HIGHEST)
    tail = jnp.broadcast_to(last[:, None, None], (heads, 8, HEAD_DIM))
    sent = jnp.concatenate([forward, backward, tail], axis=1)
    seen = lax.all_gather(sent, "t", axis=0)
    lasts = seen[:, :, 2 * HEAD_DIM, 0]
    at = jnp.arange(peers)
    low = jnp.minimum(at, index)[:, None]
    high = jnp.maximum(at, index)[:, None]
    between = (at[None, :] > low) & (at[None, :] < high)
    spans = jnp.exp(jnp.sum(jnp.where(between[:, :, None], lasts[None], 0.0), axis=1))
    before = jnp.sum(
        jnp.where(at < index, 1.0, 0.0)[:, None, None, None]
        * spans[:, :, None, None]
        * seen[:, :, :HEAD_DIM],
        axis=0,
    )
    after = jnp.sum(
        jnp.where(at > index, 1.0, 0.0)[:, None, None, None]
        * spans[:, :, None, None]
        * seen[:, :, HEAD_DIM : 2 * HEAD_DIM],
        axis=0,
    )
    scores = jnp.einsum("qhd,khd->hqk", query, key, preferred_element_type=jnp.float32)
    weights = jnp.exp(-jnp.abs(cumul[:, :, None] - cumul[:, None, :]))
    mix = jnp.einsum("hqk,khd->qhd", scores * weights, value_f, precision=HIGHEST)
    mix = mix + leading.T[:, :, None] * jnp.einsum(
        "qhd,hde->qhe", query_f, before, precision=HIGHEST
    )
    mix = mix + trailing.T[:, :, None] * jnp.einsum(
        "qhd,hde->qhe", query_f, after, precision=HIGHEST
    )
    middle = mix - jnp.mean(mix, axis=-1, keepdims=True)
    normed = middle * lax.rsqrt(jnp.mean(middle * middle, axis=-1, keepdims=True) + 1e-06)
    return normed.astype(jnp.bfloat16).reshape(rows, heads * HEAD_DIM)


def shards(
    tokens, gain, q_att, k_att, v_att, q_ret, k_ret, v_ret, out_att, out_ret, sink, decay_log
):
    parts = lax.axis_size("h")
    own = tokens.shape[0]
    rows = own * parts
    width = tokens.shape[1] * lax.axis_size("tp")
    kv = k_att.shape[1] // HEAD_DIM // parts
    group = q_att.shape[1] // k_att.shape[1]
    att = kv * group
    ret = q_ret.shape[1] // HEAD_DIM // parts
    offset = lax.axis_index("t") * rows
    total_rows = rows * lax.axis_size("t")

    packed = jnp.concatenate(
        [
            w.reshape(w.shape[0], parts, w.shape[1] // parts)
            for w in (q_att, k_att, v_att, q_ret, k_ret, v_ret)
        ],
        axis=2,
    )
    packed = jnp.moveaxis(packed, 1, 0)
    out_pack = jnp.concatenate(
        [w.reshape(parts, w.shape[0] // parts, w.shape[1]) for w in (out_att, out_ret)], axis=1
    )
    widened = tokens.astype(jnp.float32)
    sums = jnp.sum(widened * widened, axis=1)
    scaled = (widened * gain).astype(jnp.bfloat16)
    cores = lax.axis_size("tp")
    flat = packed.reshape(parts * packed.shape[1], packed.shape[2])
    weight = gather(exchange(flat, "h", 0, 0), "t", 0)
    whole = gather(gather(scaled, "h", 0), "tp", 1)
    proj = jnp.dot(whole, weight, preferred_element_type=jnp.float32)
    out_own = exchange(out_pack, "h", 0, 0)
    sums = lax.all_gather(sums, ("h", "tp"))
    decay = exchange(decay_log, "h", 0, 1)
    squares = jnp.sum(sums.reshape(parts, cores, own), axis=1).reshape(rows)
    inverse = lax.rsqrt(squares / width + 1e-06)[:, None]

    edges = [att, kv, kv, ret, ret, ret]
    starts = [sum(edges[:i]) * HEAD_DIM for i in range(6)]
    qa, ka, va, qr, kr, vr = (
        proj[:, s : s + n * HEAD_DIM].reshape(rows, n, HEAD_DIM) for s, n in zip(starts, edges)
    )
    scale = inverse[:, :, None]
    positions = (offset + jnp.arange(rows, dtype=jnp.int32)).astype(jnp.float32)
    freqs = 10000.0 ** (-jnp.arange(0, HEAD_DIM, 2).astype(jnp.float32) / HEAD_DIM)
    angles = positions[:, None] * freqs[None, :]
    cosine, sine = jnp.cos(angles)[:, None, :], jnp.sin(angles)[:, None, :]
    att_query = rotate(qa * scale, cosine, sine)
    att_key = rotate(ka * scale, cosine, sine)
    att_value = (va * scale).astype(jnp.bfloat16)
    ret_query = (qr * scale).astype(jnp.bfloat16)
    ret_key = (kr * (scale * HEAD_DIM ** (-0.5))).astype(jnp.bfloat16)
    ret_value = (vr * scale).astype(jnp.bfloat16)

    logits = lax.dynamic_slice_in_dim(sink, lax.axis_index("h") * att, att).reshape(kv, group)
    att_out, logs = attend(
        att_query.reshape(rows, kv, group, HEAD_DIM), att_key, att_value, logits, offset, total_rows
    )
    ret_out = retain(ret_query, ret_key, ret_value, decay)

    out_wide = gather(out_own, "t", 0)
    mixers = jnp.concatenate([att_out, ret_out], axis=1)
    depth = out_wide.shape[1]
    out_wide = jnp.moveaxis(out_wide, 0, 1).reshape(depth, -1)
    mixed = jnp.dot(mixers, out_wide, preferred_element_type=jnp.float32).astype(jnp.bfloat16)
    mixed = lax.psum_scatter(mixed, ("h", "tp"), scatter_dimension=0, tiled=True)
    return mixed, exchange(logs, "h", 1, 0)


def fits(args, sp, tp):
    tokens, _, q_att, k_att, v_att, q_ret, k_ret, v_ret, out_att, _, _, decay = args
    own, heads = tokens.shape[0] // sp, 4 * tp
    return (
        sp == 16
        and tp == 2
        and own == 2 * SPAN_RADIUS
        and q_att.shape[0] == sp * own
        and tokens.shape[1] == sp * own
        and q_att.shape[1] == 2 * heads * HEAD_DIM
        and all(v.shape[1] == heads * HEAD_DIM for v in (k_att, v_att, q_ret, k_ret, v_ret))
    )


def solution(mesh):
    sp, tp = mesh.shape["sp"], mesh.shape["tp"]

    def run(*args):
        if fits(args, sp, tp):
            seq = ("zh", "zl", "y", "x")
            fine = Mesh(mesh.devices.reshape(2, 2, 2, 2, tp), seq + ("tp",))
            step = fused
        else:
            heads = math.gcd(args[3].shape[1], args[5].shape[1]) // HEAD_DIM
            parts = math.gcd(heads // math.gcd(heads, tp), sp)
            seq = ("t", "h")
            fine = Mesh(mesh.devices.reshape(sp // parts, parts, tp), seq + ("tp",))
            step = shards
        body = jax.shard_map(
            step,
            mesh=fine,
            in_specs=(P(seq, "tp"), P("tp"))
            + (P(seq, "tp"),) * 6
            + (P("tp", seq), P("tp", seq), P("tp"), P("tp", seq)),
            out_specs=(P(seq + ("tp",), None), P("tp", seq)),
            check_vma=False,
        )
        return body(*args)

    return run
```

```python
import math

import jax
import jax.numpy as jnp
import numpy as np
from jax import lax
from jax.experimental import pallas as pl
from jax.experimental.pallas import tpu as pltpu
from jax.sharding import Mesh
from jax.sharding import PartitionSpec as P

HEAD_DIM = 128
SPAN_RADIUS = 128
BLOCK = 256
HIGHEST = lax.Precision.HIGHEST
MESH = pl.DeviceIdType.MESH


def gather(x, axis, dim):
    if lax.axis_size(axis) == 1:
        return x
    return lax.all_gather(x, axis, axis=dim, tiled=True)


def exchange(x, axis, split, concat):
    if lax.axis_size(axis) == 1:
        return x
    return lax.all_to_all(x, axis, split, concat, tiled=True)


def halo(shard, axis, width):
    peers, length = lax.axis_size(axis), shard.shape[1]
    up = [(i, i + 1) for i in range(peers - 1)]
    down = [(j, i) for i, j in up]
    before = lax.ppermute(shard[:, length - width :], axis, up)
    after = lax.ppermute(shard[:, :width], axis, down)
    return jnp.concatenate([before, shard, after], axis=1)


def rotate(values, cosine, sine):
    half = values.shape[-1] // 2
    first, second = values[..., :half], values[..., half:]
    return jnp.concatenate(
        [first * cosine - second * sine, second * cosine + first * sine], axis=-1
    ).astype(jnp.bfloat16)


def flip(v, bit):
    return v + bit - 2 * v * bit


PARTS = 2


class Both:
    def __init__(self, *copies):
        self.copies = copies

    def start(self):
        for copy in self.copies:
            copy.start()

    def wait_send(self):
        for copy in self.copies:
            copy.wait_send()


class Stream:
    def __init__(self, where, remote, refs, pack, split=False):
        self.where, self.remote, self.pack, self.split = where, remote, pack, split
        (
            self.wide, self.away, self.out,
            self.load, self.x_send, self.z_send, self.h_send, self.y_send,
            self.p_recv, self.w_recv, self.more_send, self.more_recv,
        ) = refs

    def fetch(self):
        w = self.where
        targets = (
            (self.out.at[0], 1 - w.g, 1 - w.x),
            (self.out.at[1], w.g, 1 - w.x),
            (self.wide.at[w.own], w.g, w.x),
            (self.away.at[w.x], 1 - w.g, w.x),
        )
        for i, (target, g, x) in enumerate(targets):
            self.pack(2 * g + x, target, self.load.at[i])

    def fetched(self):
        w = self.where
        for i, target in enumerate(
            (self.out.at[0], self.out.at[1], self.wide.at[w.own], self.away.at[w.x])
        ):
            pltpu.make_async_copy(target, target, self.load.at[i]).wait()

    def along_x(self, k):
        w = self.where
        if k == 0:
            return self.remote(
                self.out.at[0], self.away.at[w.x], self.x_send.at[0], self.p_recv.at[0], w.to_x
            )
        return self.remote(
            self.out.at[1], self.wide.at[w.own], self.x_send.at[1], self.w_recv.at[w.own], w.to_x
        )

    def along_z(self, k):
        w = self.where
        x = w.x if k == 0 else 1 - w.x
        s = w.at(w.zh, w.zl, w.y, x)
        return self.remote(
            self.away.at[x], self.wide.at[s], self.z_send.at[k], self.w_recv.at[s], w.to_z
        )

    def near(self, k):
        w = self.where
        return w.at(w.zh, flip(w.zl, k // 2), w.y, flip(w.x, k % 2))

    def far(self, k):
        w = self.where
        return w.at(1 - w.zh, flip(w.zl, 1 - k // 2), w.y, flip(w.x, k % 2))

    def across(self, k):
        w = self.where
        return w.at(1 - w.zh, flip(w.zl, 1 - k // 2), 1 - w.y, flip(w.x, k % 2))

    def parts_of(self, s, hop, k, to):
        rows = self.wide.shape[1] // PARTS
        pieces = [self.wide.at[s, pl.ds(i * rows, rows), :] for i in range(PARTS)]
        return [
            self.remote(
                piece, piece, self.more_send.at[hop, k, i], self.more_recv.at[hop, k, i], to
            )
            for i, piece in enumerate(pieces)
        ]

    def along_h(self, k):
        s = self.near(k)
        if self.split:
            return Both(*self.parts_of(s, 0, k, self.where.to_h))
        return self.remote(
            self.wide.at[s], self.wide.at[s], self.h_send.at[k], self.w_recv.at[s], self.where.to_h
        )

    def along_y(self, k, far=0):
        s = self.far(k) if far else self.near(k)
        if far and self.split:
            return Both(*self.parts_of(s, 1, k, self.where.to_y))
        return self.remote(
            self.wide.at[s], self.wide.at[s],
            self.y_send.at[4 * far + k], self.w_recv.at[s], self.where.to_y,
        )

    def pass_far(self, k):
        if self.split:
            arrivals = self.parts_of(self.far(k), 0, k, self.where.to_h)
            for arrival, copy in zip(arrivals, self.along_y(k, 1).copies):
                arrival.wait_recv()
                copy.start()
        else:
            self.arrive(self.far(k))
            self.along_y(k, 1).start()

    def arrive_far_across(self, k):
        s = self.across(k)
        if self.split:
            for arrival in self.parts_of(s, 1, k, self.where.to_y):
                arrival.wait_recv()
        else:
            self.arrive(s)

    def arrive(self, s):
        self.remote(
            self.wide.at[s], self.wide.at[s], self.x_send.at[0], self.w_recv.at[s], self.where.to_x
        ).wait_recv()

    def arrive_away(self):
        w = self.where
        slot = self.away.at[1 - w.x]
        self.remote(slot, slot, self.x_send.at[0], self.p_recv.at[0], w.to_x).wait_recv()

    def arrive_across(self, far):
        w = self.where
        zh = 1 - w.zh if far else w.zh
        for zl in range(2):
            for x in range(2):
                self.arrive(w.at(zh, zl, 1 - w.y, x))

    def drain(self):
        for k in range(2):
            self.along_x(k).wait_send()
            self.along_z(k).wait_send()
        for k in range(4):
            self.along_h(k).wait_send()
            self.along_y(k).wait_send()
            self.along_y(k, 1).wait_send()


class Place:
    def __init__(self):
        self.zh, self.zl, self.y, self.x, self.c = (
            lax.axis_index(a) for a in ("zh", "zl", "y", "x", "tp")
        )
        self.g = lax.rem(self.zh + self.zl, 2)
        self.h = 2 * self.g + self.x
        self.own = self.at(self.zh, self.zl, self.y, self.x)
        self.b = 2 * self.zl + self.x
        self.to_x = {"x": 1 - self.x}
        self.to_z = {"zl": 1 - self.zl}
        self.to_y = {"y": 1 - self.y}
        self.to_h = {"zh": 1 - self.zh, "zl": 1 - self.zl}
        self.to_hy = {"zh": 1 - self.zh, "zl": 1 - self.zl, "y": 1 - self.y}
        self.to_zx = {"zl": 1 - self.zl, "x": 1 - self.x}
        self.to_c = {"tp": 1 - self.c}
        self.to_zc = {"zl": 1 - self.zl, "tp": 1 - self.c}

    @staticmethod
    def at(zh, zl, y, x):
        return ((zh * 2 + zl) * 2 + y) * 2 + x


def fused_kernel(
    tokens, gain, q_att, k_att, v_att, q_ret, k_ret, v_ret, out_att, out_ret, sink, decay,
    cos_t, sin_t, base,
    mixed, logs_out,
    raw, scl, ssq, gains, acc_a, acc_r, kvext, qrot, rets, dec, cumr, cumc, coef, states, stall, crossing,
    mix, bias, logm, lsend, lrecv, mine, kept, give, take, s1, r1, s2, r2,
    t_load, t_x, t_z, t_c, t_recv, g_sem, d_sem, halo_sem, st_sem, l_sem, go,
    give_s, take_r, s1_s, r1_r, s2_s, r2_r,
    *streams,
):
    w = Place()
    y = w.y
    f32, bf16 = jnp.float32, jnp.bfloat16
    own, half_d = tokens.shape
    rows = 4 * own
    run_rows = 2 * own
    total_rows = 16 * own
    H = HEAD_DIM
    edge = SPAN_RADIUS

    def remote(src, dst, send, recv, to):
        return pltpu.make_async_remote_copy(
            src_ref=src, dst_ref=dst, send_sem=send, recv_sem=recv,
            device_id=to, device_id_type=MESH,
        )

    def lanes(h, n):
        return pl.ds(pl.multiple_of(h * n, n), n)

    def pack_cols(parts):
        def pack(h, target, sem):
            start = 0
            for ref in parts:
                n = ref.shape[1] // 4
                pltpu.make_async_copy(
                    ref.at[:, lanes(h, n)], target.at[:, pl.ds(start, n)], sem
                ).start()
                start += n
        return pack

    def pack_rows(parts):
        def pack(h, target, sem):
            start = 0
            for ref in parts:
                n = ref.shape[0] // 4
                pltpu.make_async_copy(
                    ref.at[lanes(h, n), :], target.at[pl.ds(start, n), :], sem
                ).start()
                start += n
        return pack

    n = len(streams) // 3
    A = Stream(w, remote, streams[:n], pack_cols((q_att, k_att, v_att)), True)
    R = Stream(w, remote, streams[n : 2 * n], pack_cols((q_ret, k_ret, v_ret)), True)
    O = Stream(w, remote, streams[2 * n :], pack_rows((out_att, out_ret)))

    token_load = pltpu.make_async_copy(tokens, raw.at[w.c, w.b], t_load.at[0])
    gain_load = pltpu.make_async_copy(gain, gains.at[w.c], t_load.at[1])
    decay_load = pltpu.make_async_copy(decay, dec.at[w.zh, w.y, w.zl, w.x], t_load.at[2])

    def block(zl, x):
        return 2 * zl + x

    def order(k):
        return block((w.zl, 1 - w.zl)[k // 2], (w.x, 1 - w.x)[k % 2])

    def token(e, k, part, send, to):
        here = raw.at[e, order(k)]
        if part is not None:
            here = here.at[pl.ds(part * edge, edge), :]
        return remote(here, here, send, t_recv.at[e, order(k), part or 0], to)

    tokens_x = [token(w.c, 0, None, t_x.at[0], w.to_x)]
    tokens_x += [token(w.c, 2, i, t_x.at[1 + i], w.to_x) for i in range(2)]
    tokens_z = token(w.c, 0, None, t_z.at[0], w.to_z)
    tokens_c = [token(w.c, k, None, t_c.at[k], w.to_c) for k in range(3)]
    tokens_c += [token(w.c, 3, i, t_c.at[3 + i], w.to_c) for i in range(2)]

    def token_arrive(k, e=None, part=None):
        token(w.c if e is None else e, k, part, t_x.at[0], w.to_x).wait_recv()

    gain_c = remote(gains.at[w.c], gains.at[w.c], g_sem.at[0], g_sem.at[1], w.to_c)

    def others(i):
        return tuple(flip(v, (i >> k) & 1) for v, k in ((w.zh, 3), (w.zl, 2), (w.y, 1), (w.x, 0)))

    def peer(i):
        return dict(zip(("zh", "zl", "y", "x"), others(i)))

    def decay_send(i):
        here = dec.at[w.zh, w.y, w.zl, w.x]
        return remote(here, here, d_sem.at[0, i], d_sem.at[1, i], peer(i))

    def decay_arrive(i):
        zh, zl, yy, x = others(i)
        here = dec.at[zh, yy, zl, x]
        remote(here, here, d_sem.at[0, i], d_sem.at[1, i], peer(i)).wait_recv()

    decay_load.start()
    R.fetch()
    A.fetch()
    gain_load.start()
    token_load.start()
    O.fetch()

    barrier = pltpu.get_barrier_semaphore()
    for to in (w.to_c, w.to_zc):
        pl.semaphore_signal(barrier, inc=1, device_id=to, device_id_type=MESH)
    for i in range(1, 16):
        pl.semaphore_signal(barrier, inc=1, device_id=peer(i), device_id_type=MESH)
    pl.semaphore_wait(barrier, 17)

    middle = w.g == 1

    decay_load.wait()
    for i in range(1, 16):
        decay_send(i).start()
    R.fetched()
    R.along_x(0).start()
    R.along_z(0).start()
    R.along_y(0).start()
    A.fetched()
    A.along_x(0).start()
    A.along_z(0).start()
    A.along_y(0).start()
    R.along_x(1).start()
    A.along_x(1).start()

    @pl.when(middle)
    def _():
        R.along_h(0).start()
        A.along_h(0).start()

    O.fetched()
    O.along_x(1).start()
    O.along_x(0).start()
    token_load.wait()
    tokens_x[0].start()
    gain_load.wait()
    gain_c.start()
    tokens_c[0].start()

    def scale(e, b, first=0, last=None):
        @pl.loop(first // 16, (own if last is None else last) // 16)
        def _(i):
            value = raw[e, b, pl.ds(pl.multiple_of(i * 16, 16), 16), :].astype(f32)
            at = pl.ds(pl.multiple_of(b * own + i * 16, 16), 16)
            scl[e, at, :] = (value * gains[e]).astype(bf16)
            square = value * value
            total = square[:, :H]
            for k in range(1, half_d // H):
                total = total + square[:, k * H : (k + 1) * H]
            ssq[e, at, :] = total

    @pl.when((w.zh == 0) & (w.y == 0))
    def _():
        kvext[0, :, 0:edge, :] = jnp.zeros((2, edge, H), bf16)

    @pl.when((w.zh == 1) & (w.y == 1))
    def _():
        kvext[1, :, edge + run_rows :, :] = jnp.zeros((2, edge, H), bf16)

    scale(w.c, w.b)
    for stream in (R, A):
        stream.arrive_away()
        stream.along_z(1).start()
    tokens_z.start()
    remote(gains.at[1 - w.c], gains.at[1 - w.c], g_sem.at[0], g_sem.at[1], w.to_c).wait_recv()
    token_arrive(0, 1 - w.c)
    scale(1 - w.c, w.b)

    def pass_near(stream, k):
        stream.arrive(stream.near(k))
        stream.along_y(k).start()

        @pl.when(middle)
        def _():
            stream.along_h(k).start()

    def pass_far(stream, k):
        stream.pass_far(k)

    pass_near(R, 2)
    pass_near(A, 2)
    for k in (1, 3):
        pass_near(R, k)
        pass_near(A, k)

    O.along_y(0).start()
    O.along_z(0).start()

    @pl.when(w.g == 0)
    def _():
        for stream in (R, A):
            for k in range(4):
                stream.along_h(k).start()

    @pl.when(middle)
    def _():
        O.along_h(0).start()

    row = lax.broadcasted_iota(jnp.int32, bias.shape, 0)
    shift = lax.broadcasted_iota(jnp.int32, bias.shape, 1) - lax.rem(row, edge)
    bias[...] = jnp.where((shift >= 0) & (shift <= 2 * edge), 0.0, -jnp.inf)
    logm[...] = jnp.zeros_like(logm)
    for i in range(1, 16):
        decay_arrive(i)

    lane = lax.broadcasted_iota(jnp.int32, (8, run_rows), 1)
    for slot in range(2):
        row = jnp.concatenate(
            [dec[w.zh, w.y, slot, x, pl.ds(w.h, 1), :] for x in range(2)], axis=1
        )
        row = jnp.broadcast_to(row, (8, run_rows))
        step = 1
        while step < run_rows:
            row = row + jnp.where(lane >= step, pltpu.roll(row, step, axis=1), 0.0)
            step *= 2
        cumr[slot] = row
        cumc[slot] = jnp.transpose(jnp.broadcast_to(row[0:1], (H, run_rows)))
    lane = lax.broadcasted_iota(jnp.int32, (8, H), 1)
    run = lax.broadcasted_iota(jnp.int32, (8, H), 0)
    totals = jnp.zeros((8, H), f32)
    for zh in range(2):
        for slot in range(2):
            for yy in range(2):
                pair = sum(dec[zh, yy, slot, x, pl.ds(w.h, 1), :] for x in range(2))
                value = jnp.sum(pair, axis=1, keepdims=True)
                totals = jnp.where(lane == 4 * zh + 2 * slot + yy, value, totals)
    for slot in range(2):
        me = 4 * w.zh + 2 * slot + w.y
        between = (lane > jnp.minimum(run, me)) & (lane < jnp.maximum(run, me))
        factor = jnp.exp(jnp.sum(jnp.where(between, totals, 0.0), axis=1, keepdims=True))
        factor = jnp.broadcast_to(factor, (8, H))
        near = run // 4 == w.zh
        coef[slot, 0] = jnp.where(near & (run < me), factor, 0.0)
        coef[slot, 1] = jnp.where(near & (run > me), factor, 0.0)
        between = (lane > jnp.where(w.zh == 0, me, 3)) & (lane < jnp.where(w.zh == 0, 4, me))
        factor = jnp.exp(jnp.sum(jnp.where(between, totals, 0.0), axis=1, keepdims=True))
        coef[slot, 2] = jnp.broadcast_to(factor, (8, H))

    pass_near(O, 1)

    @pl.when(middle)
    def _():
        for stream in (R, A):
            for k in (0, 2, 1, 3):
                pass_far(stream, k)

    def part_of(stream, zh, b, start, width):
        at = pl.ds(pl.multiple_of(b * own, own), own)
        depth = half_d // own
        weight = stream.wide[pl.ds(zh * depth, depth), :, start : start + width]
        return jnp.dot(
            scl[zh, at, :], weight.reshape(half_d, width), preferred_element_type=f32
        )

    def first_part(stream, acc, b):
        at = pl.ds(pl.multiple_of(b * own, own), own)
        start = 0
        while start < acc.shape[1]:
            width = min(2 * H, acc.shape[1] - start)
            acc[at, start : start + width] = part_of(stream, w.zh, b, start, width)
            start += width

    def pair_of(stream, zl, yy, b, start, width):
        zh = 1 - w.zh
        at = pl.ds(pl.multiple_of(b * own, own), own)
        depth = pl.ds(pl.multiple_of((2 * zl + yy) * 2 * own, 2 * own), 2 * own)
        weight = stream.wide[pl.ds(w.at(zh, zl, yy, 0), 2), :, start : start + width]
        return jnp.dot(
            scl[zh, at, depth], weight.reshape(2 * own, width), preferred_element_type=f32
        )

    def add_pair(stream, acc, zl, yy, b):
        at = pl.ds(pl.multiple_of(b * own, own), own)
        for start in range(0, acc.shape[1], 2 * H):
            width = min(2 * H, acc.shape[1] - start)
            acc[at, start : start + width] += pair_of(stream, zl, yy, b, start, width)

    def last_of(stream, acc, b, start, width):
        at = pl.ds(pl.multiple_of(b * own, own), own)
        return acc[at, start : start + width] + pair_of(stream, w.zl, 1 - w.y, b, start, width)

    def whole_of(stream, acc, b, start, width):
        at = pl.ds(pl.multiple_of(b * own, own), own)
        return acc[at, start : start + width] + part_of(stream, 1 - w.zh, b, start, width)

    token_arrive(2)
    for copy in tokens_x[1:]:
        copy.start()
    tokens_c[2].start()
    scale(w.c, order(2))
    token_arrive(2, 1 - w.c)
    scale(1 - w.c, order(2))
    token_arrive(1)
    tokens_c[1].start()
    scale(w.c, order(1))

    @pl.when(w.g == 0)
    def _():
        pass_far(R, 0)

    O.arrive_away()
    O.along_z(1).start()
    token_arrive(1, 1 - w.c)
    scale(1 - w.c, order(1))

    @pl.when(w.g == 0)
    def _():
        pass_far(R, 1)

    R.arrive_across(0)
    A.arrive_across(0)
    for k in (2, 0):
        first_part(R, acc_r, order(k))
        first_part(A, acc_a, order(k))

    @pl.when(w.g == 0)
    def _():
        pass_far(R, 2)

    first_part(R, acc_r, order(1))
    first_part(A, acc_a, order(1))
    @pl.when(w.g == 0)
    def _():
        pass_far(R, 3)

    token_arrive(3, None, 0)
    tokens_c[3].start()
    scale(w.c, order(3), 0, edge)
    token_arrive(3, 1 - w.c, 0)
    scale(1 - w.c, order(3), 0, edge)

    @pl.when(w.g == 0)
    def _():
        pass_far(A, 0)

    token_arrive(3, None, 1)
    tokens_c[4].start()

    @pl.when(w.g == 0)
    def _():
        pass_far(A, 1)

    scale(w.c, order(3), edge, own)
    token_arrive(3, 1 - w.c, 1)
    scale(1 - w.c, order(3), edge, own)
    first_part(R, acc_r, order(3))
    first_part(A, acc_a, order(3))

    def inverse(b):
        at = pl.ds(pl.multiple_of(b * own, own), own)
        squares = jnp.sum(ssq[0, at, :] + ssq[1, at, :], axis=1, keepdims=True)
        return lax.rsqrt(squares / (2 * half_d) + 1e-06)

    def angles(b):
        s = w.at(w.zh, b // 2, w.y, b % 2)
        c0, s0, s0n, c0n = (base[i, pl.ds(s, 1), :] for i in range(4))
        cosine = cos_t[...] * c0 - sin_t[...] * s0
        sine = cos_t[...] * s0n + sin_t[...] * c0n
        return cosine, sine

    def turn(value, cosine, sine):
        return (value * cosine + pltpu.roll(value, H // 2, axis=1) * sine).astype(bf16)

    def keys_values(b):
        scale_b = inverse(b)
        cosine, sine = angles(b)
        both = last_of(A, acc_a, b, 2 * H, 2 * H) * scale_b
        inner = pl.ds(pl.multiple_of(edge + (b % 2) * own, edge), own)
        kvext[b // 2, 0, inner, :] = turn(both[:, :H], cosine, sine)
        kvext[b // 2, 1, inner, :] = both[:, H:].astype(bf16)

    def queries(b):
        at = pl.ds(pl.multiple_of(b * own, own), own)
        cosine, sine = angles(b)
        query = last_of(A, acc_a, b, 0, 2 * H) * inverse(b)
        qrot[at, :H] = turn(query[:, :H], cosine, sine)
        qrot[at, H:] = turn(query[:, H:], cosine, sine)

    for k in range(4):
        R.arrive_far_across(k)

    def retention_inputs(b):
        at = pl.ds(pl.multiple_of(b * own, own), own)
        scale_b = inverse(b)
        both = whole_of(R, acc_r, b, 0, 2 * H)
        rets[0, at, :] = (both[:, :H] * scale_b).astype(bf16)
        rets[1, at, :] = (both[:, H:] * (scale_b * H ** (-0.5))).astype(bf16)
        rets[2, at, :] = (whole_of(R, acc_r, b, 2 * H, H) * scale_b).astype(bf16)

    @pl.when(w.g == 0)
    def _():
        pass_far(A, 2)

    @pl.loop(0, 4, unroll=True)
    def _(b):
        retention_inputs(b)

    for slot in range(2):
        at = pl.ds(slot * run_rows, run_rows)
        last = cumr[slot, 0:1, run_rows - 1 : run_rows]
        key, value = rets[1, at, :].astype(f32), rets[2, at, :]
        for i, weight in enumerate((jnp.exp(last - cumc[slot]), jnp.exp(cumc[slot]))):
            lhs = (key * weight).astype(bf16)
            state = lax.dot_general(
                lhs, value, (((0,), (0,)), ((), ())), preferred_element_type=f32
            ).astype(bf16)
            stall[y, slot, i] = state
    total = jnp.zeros((H, H), f32)
    for slot in range(2):
        total = total + coef[slot, 2, 0:1, :] * stall[y, slot, w.zh].astype(f32)
    crossing[2] = total.astype(bf16)
    state_sends = [
        remote(stall.at[y], stall.at[y], st_sem.at[0, 0], st_sem.at[1, 0], w.to_y),
        remote(crossing.at[2], crossing.at[0], st_sem.at[0, 1], st_sem.at[1, 1], w.to_h),
        remote(crossing.at[2], crossing.at[1], st_sem.at[0, 2], st_sem.at[1, 2], w.to_hy),
    ]
    state_sends[1].start()
    state_sends[2].start()

    def inner_tile(i):
        slot = i // 2
        at = pl.ds(pl.multiple_of(i * own, own), own)
        keys = pl.ds(pl.multiple_of(slot * run_rows, run_rows), run_rows)
        score = lax.dot_general(
            rets[0, at, :], rets[1, keys, :], (((1,), (1,)), ((), ())),
            preferred_element_type=f32,
        )
        column = cumc[slot, pl.ds(pl.multiple_of((i % 2) * own, own), own), :]
        column = jnp.concatenate([column] * (run_rows // H), axis=1)
        weight = jnp.exp(-jnp.abs(column - cumr[slot, 0:1, :]))
        acc_r[at, :H] = jnp.dot(
            (score * weight).astype(bf16), rets[2, keys, :], preferred_element_type=f32
        )

    @pl.loop(0, 4, unroll=True)
    def _(i):
        inner_tile(i)

    @pl.when(w.g == 0)
    def _():
        pass_far(A, 3)

    @pl.loop(0, 8)
    def _(i):
        add_pair(A, acc_a, i // 4, y, i % 4)

    for k in range(2):
        A.arrive_far_across(k)

    @pl.loop(0, 4)
    def _(b):
        add_pair(A, acc_a, 1 - w.zl, 1 - y, b)

    for k in range(2, 4):
        A.arrive_far_across(k)

    @pl.loop(0, 4, unroll=True)
    def _(b):
        keys_values(b)

    head, tail, before_at, after_at = edge, run_rows, 0, edge + run_rows

    def pick(a, b):
        return a + (b - a) * y

    def piece(slot, start):
        return kvext.at[slot, :, pl.ds(pl.multiple_of(start, edge), edge), :]

    halo_y = [
        remote(
            piece(pick(s0, s1), pick(f0, f1)), piece(pick(d0, d1), pick(o0, o1)),
            halo_sem.at[0, i], halo_sem.at[1, i], w.to_y,
        )
        for i, (s0, f0, d0, o0, s1, f1, d1, o1) in enumerate(
            (
                (0, tail, 0, before_at, 0, head, 0, after_at),
                (1, head, 0, after_at, 0, tail, 1, before_at),
                (1, tail, 1, before_at, 1, head, 1, after_at),
            )
        )
    ]
    halo_far = remote(
        piece(pick(0, 1), pick(head, tail)), piece(pick(1, 0), pick(after_at, before_at)),
        halo_sem.at[0, 3], halo_sem.at[1, 3], w.to_hy,
    )
    has_far = ((y == 0) & (w.zh == 1)) | ((y == 1) & (w.zh == 0))
    for copy in halo_y:
        copy.start()

    @pl.when(has_far)
    def _():
        halo_far.start()

    state_sends[0].start()

    @pl.when(middle)
    def _():
        for copy in state_sends[1:]:
            copy.wait_send()

        @pl.when(has_far)
        def _():
            halo_far.wait_send()

        for to in (w.to_z, w.to_zc):
            pl.semaphore_signal(go, inc=1, device_id=to, device_id_type=MESH)

    @pl.when(middle)
    def _():
        for k in (2, 3):
            O.arrive(O.near(k))
            O.along_h(k).start()
            O.along_y(k).start()

    @pl.loop(0, 4, unroll=True)
    def _(b):
        queries(b)

    def halo_arrive(slot, start, i, to):
        here = piece(slot, start)
        remote(here, here, halo_sem.at[0, i], halo_sem.at[1, i], to).wait_recv()

    def attend_tile(i, at_end):
        slot, j = i // 4, i % 4
        query = qrot[pl.ds(pl.multiple_of(i * edge, edge), edge), :]
        query = jnp.concatenate([query[:, :H], query[:, H:]], axis=0)
        span = pl.ds(pl.multiple_of(j * edge, edge), 3 * edge)
        key, value = kvext[slot, 0, span, :], kvext[slot, 1, span, :]
        score = lax.dot_general(
            query, key, (((1,), (1,)), ((), ())), preferred_element_type=f32
        ) * H ** (-0.5)
        masked = score + bias[...]
        if at_end:
            col = lax.broadcasted_iota(jnp.int32, (1, 3 * edge), 1)
            start = w.at(w.zh, slot, y, 0) * own + j * edge - edge
            inside = (col >= -start) & (col < total_rows - start)
            masked = masked + jnp.where(inside, 0.0, -jnp.inf)
        first = lax.broadcasted_iota(jnp.int32, (2 * edge, 1), 0) < edge
        limit = jnp.where(first, sink[2 * w.h], sink[2 * w.h + 1])
        top = jnp.maximum(jnp.max(masked, axis=1, keepdims=True), limit)
        expo = jnp.exp(masked - top)
        total = jnp.sum(expo, axis=1, keepdims=True) + jnp.exp(limit - top)
        logs = top + jnp.log(total)
        probs = (expo * (1.0 / total)).astype(bf16)
        result = jnp.dot(probs, value, preferred_element_type=f32).astype(bf16)
        at = pl.ds(pl.multiple_of((i // 2) * edge, edge), edge)
        mix[i % 2, at, 0:H] = result[:edge]
        mix[i % 2, at, H : 2 * H] = result[edge:]
        column = lax.broadcasted_iota(jnp.int32, (2 * edge, H), 1)
        logm[...] = jnp.where(column == i, logs, logm[...])

    @pl.when(w.g == 0)
    def _():
        pl.semaphore_wait(go, 2)
        for k in range(4):
            if k > 1:
                O.arrive(O.near(k))
            O.along_h(k).start()

    @pl.loop(0, 4, unroll=True)
    def _(i):
        attend_tile(4 * (i // 2) + 1 + i % 2, False)

    halo_arrive(pick(0, 0), pick(after_at, before_at), 0, w.to_y)
    halo_arrive(pick(1, 0), pick(before_at, after_at), 1, w.to_y)
    halo_arrive(pick(1, 1), pick(after_at, before_at), 2, w.to_y)

    @pl.when(has_far)
    def _():
        halo_arrive(pick(0, 1), pick(before_at, after_at), 3, w.to_hy)

    @pl.when(w.g == 0)
    def _():
        O.along_y(2).start()
        O.along_y(3).start()

    @pl.loop(0, 4, unroll=True)
    def _(i):
        attend_tile(4 * (i // 2) + 3 * (i % 2), True)

    for i, here in enumerate((stall.at[1 - y], crossing.at[0], crossing.at[1])):
        remote(here, here, st_sem.at[0, i], st_sem.at[1, i], w.to_y).wait_recv()
    crossed = crossing[0].astype(f32) + crossing[1].astype(f32)
    for slot in range(2):
        for i in range(2):
            total = jnp.where(w.zh == 1 - i, 1.0, 0.0) * coef[slot, 2, 0:1, :] * crossed
            for s in range(2):
                for yy in range(2):
                    for zh in range(2):
                        r = 4 * zh + 2 * s + yy
                        total = total + coef[slot, i, r : r + 1, :] * stall[yy, s, i].astype(f32)
            states[slot, :, i * H : (i + 1) * H] = total.astype(bf16)

    def finish_tile(i):
        slot = i // 2
        at = pl.ds(pl.multiple_of(i * own, own), own)
        column = cumc[slot, pl.ds(pl.multiple_of((i % 2) * own, own), own), :]
        last = cumr[slot, 0:1, run_rows - 1 : run_rows]
        carried = jnp.dot(rets[0, at, :], states[slot], preferred_element_type=f32)
        value = (
            acc_r[at, :H] + jnp.exp(column) * carried[:, :H]
            + jnp.exp(last - column) * carried[:, H:]
        )
        value = value - jnp.mean(value, axis=1, keepdims=True)
        value = value * lax.rsqrt(jnp.mean(value * value, axis=1, keepdims=True) + 1e-06)
        value = value.astype(bf16)
        out = pl.ds(pl.multiple_of(i * edge, edge), edge)
        mix[0, out, 2 * H :] = value[:edge]
        mix[1, out, 2 * H :] = value[edge:]

    @pl.loop(0, 4, unroll=True)
    def _(i):
        finish_tile(i)

    @pl.when(middle)
    def _():
        for k in range(2):
            pass_far(O, k)

    turned = jnp.transpose(logm[...])
    for b in range(4):
        lsend[b] = turned[2 * b : 2 * b + 2]
        lrecv[w.h] = jnp.where(w.b == b, turned[2 * b : 2 * b + 2], lrecv[w.h] if b else 0.0)
    h_of = lambda zl, x: 2 * lax.rem(w.zh + zl, 2) + x
    log_to = (
        (1 - w.x, w.zl, w.to_x), (w.x, 1 - w.zl, w.to_z), (1 - w.x, 1 - w.zl, w.to_zx),
    )
    log_sends = [
        remote(lsend.at[block(zl, x)], lrecv.at[w.h], l_sem.at[0, i], l_sem.at[1, i], to)
        for i, (x, zl, to) in enumerate(log_to)
    ]

    for copy in log_sends:
        copy.start()

    chunks = 8

    def columns_of(i, x):
        far, across, zl = i // 4, (i // 2) % 2, i % 2
        return w.at(flip(w.zh, far), zl, flip(y, across), x)

    def swap(i):
        return remote(give.at[i], take.at[i], give_s.at[i], take_r.at[i], w.to_c)

    def x_first(i, k):
        return 1 if k == 0 else jnp.where(i < 1, 1, 0)

    def toward(dx):
        return {"x": flip(w.x, dx), "zl": flip(w.zl, 1 - dx)}

    def first_hop(i, k):
        to = toward(x_first(i, k))
        return remote(s1.at[i, k], r1.at[i, k], s1_s.at[i, k], r1_r.at[i, k], to)

    def second_hop(i, k):
        to = toward(1 - x_first(i, k))
        return remote(s2.at[i, k], r2.at[i, k], s2_s.at[i, k], r2_r.at[i, k], to)

    def side(i, k, j, cross):
        dx = x_first(i, k)
        zl = dx * j + (1 - dx) * flip(w.zl, cross)
        x = dx * flip(w.x, cross) + (1 - dx) * j
        return block(zl, x)

    def part(b):
        return pl.ds(pl.multiple_of(b * edge, edge), edge)

    lag = 6

    @pl.loop(0, chunks + lag)
    def _(step):
        @pl.when(step < chunks)
        def _():
            i = step

            @pl.when((i // 2) % 2 == 1)
            def _():
                for x in range(2):
                    O.arrive(columns_of(i, x))

            @pl.when((i == 2) & (w.g == 0))
            def _():
                for k in range(2):
                    pass_far(O, k)

            @pl.when(i == 4)
            def _():
                for k in range(2, 4):
                    pass_far(O, k)

            for k in range(2):
                give[i, k] = jnp.dot(
                    mix[1 - w.c], O.wide[columns_of(i, k)], preferred_element_type=f32
                ).astype(bf16)
            swap(i).start()
            for k in range(2):
                mine[i % 4, k] = jnp.dot(
                    mix[w.c], O.wide[columns_of(i, k)], preferred_element_type=f32
                )

        @pl.when((step >= 1) & (step < chunks + 1))
        def _():
            i = step - 1
            swap(i).wait_recv()
            for k in range(2):
                for j in range(2):
                    b = side(i, k, j, 1)
                    total = mine[i % 4, k, part(b), :] + take[i, k, part(b), :].astype(f32)
                    s1[i, k, j] = total.astype(bf16)
                first_hop(i, k).start()
            for k in range(2):
                for j in range(2):
                    b = side(i, k, j, 0)
                    mine[i % 4, k, part(b), :] += take[i, k, part(b), :].astype(f32)

        @pl.when((step >= 2) & (step < chunks + 2))
        def _():
            i = step - 2
            for k in range(2):
                first_hop(i, k).wait_recv()
                dx = x_first(i, k)
                j = flip(dx * w.zl + (1 - dx) * w.x, 1)
                b = side(i, k, j, 0)
                s2[i, k] = (mine[i % 4, k, part(b), :] + r1[i, k, j].astype(f32)).astype(bf16)
                second_hop(i, k).start()
                j = flip(j, 1)
                kept[i, k] = mine[i % 4, k, part(w.b), :] + r1[i, k, j].astype(f32)

        @pl.when(step >= lag)
        def _():
            i = step - lag
            for k in range(2):
                second_hop(i, k).wait_recv()
                at = pl.ds(pl.multiple_of(columns_of(i, k) * own, own), own)
                mixed[:, at] = (kept[i, k] + r2[i, k].astype(f32)).astype(mixed.dtype)

    for i, (x, zl, to) in enumerate(log_to):
        here = lrecv.at[h_of(zl, x)]
        remote(here, here, l_sem.at[0, i], l_sem.at[1, i], to).wait_recv()
    for h in range(4):
        for head_i in range(2):
            for t in range(2):
                logs_out[2 * h + head_i : 2 * h + head_i + 1, t * edge : (t + 1) * edge] = (
                    lrecv[h, t : t + 1, head_i * edge : (head_i + 1) * edge]
                )

    for stream in (A, R, O):
        stream.drain()
    for i in range(1, 16):
        decay_send(i).wait_send()
    for copy in tokens_x + tokens_c + [tokens_z, gain_c]:
        copy.wait_send()
    for copy in halo_y + state_sends[:1] + log_sends:
        copy.wait_send()

    @pl.when(w.g == 0)
    def _():
        for copy in state_sends[1:]:
            copy.wait_send()

        @pl.when(has_far)
        def _():
            halo_far.wait_send()

    @pl.loop(0, chunks)
    def _(i):
        swap(i).wait_send()
        for k in range(2):
            first_hop(i, k).wait_send()
            second_hop(i, k).wait_send()


def settle_kernel(mixed, logs, mixed_out, logs_out, sems):
    rows = mixed.shape[0] // 8
    copies = [
        pltpu.make_async_copy(
            mixed.at[pl.ds(i * rows, rows)], mixed_out.at[pl.ds(i * rows, rows)], sems.at[i]
        )
        for i in range(8)
    ]
    copies.append(pltpu.make_async_copy(logs, logs_out, sems.at[8]))
    for copy in copies:
        copy.start()
    for copy in copies:
        copy.wait()


def settle(mixed, logs):
    return pl.pallas_call(
        settle_kernel,
        out_shape=tuple(jax.ShapeDtypeStruct(v.shape, v.dtype) for v in (mixed, logs)),
        in_specs=[pl.BlockSpec(memory_space=pltpu.VMEM)] * 2,
        out_specs=[pl.BlockSpec(memory_space=pl.ANY)] * 2,
        scratch_shapes=[pltpu.SemaphoreType.DMA((9,))],
    )(mixed, logs)


def fused(*args):
    tokens, gain, q_att = args[:3]
    out_att, out_ret, sink, decay_log = args[8:]
    own, half_d = tokens.shape
    rows, run_rows = 4 * own, 2 * own
    H, edge = HEAD_DIM, SPAN_RADIUS
    bf16, f32 = jnp.bfloat16, jnp.float32
    dma, vmem = pltpu.SemaphoreType.DMA, pltpu.VMEM
    depth = q_att.shape[0]
    width = out_att.shape[1] * 16

    freqs = 10000.0 ** (-np.arange(0, H, 2, dtype=np.float64) / H)
    freqs = np.concatenate([freqs, freqs])[None, :]
    sign = np.where(np.arange(H) < H // 2, -1.0, 1.0)[None, :]
    inner = np.arange(own)[:, None] * freqs
    outer = (np.arange(16) * own)[:, None] * freqs
    cos_t, sin_t = jnp.asarray(np.cos(inner), f32), jnp.asarray(np.sin(inner), f32)
    base = jnp.asarray(
        np.stack([np.cos(outer), np.sin(outer), sign * np.sin(outer), sign * np.cos(outer)]), f32
    )

    def stream(block):
        return [
            vmem((16,) + block, bf16), vmem((2,) + block, bf16), vmem((2,) + block, bf16),
            dma((4,)), dma((2,)), dma((2,)), dma((4,)), dma((8,)), dma((1,)), dma((16,)),
            dma((2, 4, PARTS)), dma((2, 4, PARTS)),
        ]

    out_rows = (out_att.shape[0] + out_ret.shape[0]) // 4
    tile = (8, 2, 4 * edge, own)
    hbm, inside = pl.BlockSpec(memory_space=pl.ANY), pl.BlockSpec(memory_space=pltpu.VMEM)
    mixed, logs = pl.pallas_call(
        fused_kernel,
        out_shape=(
            jax.ShapeDtypeStruct((own // 2, width), bf16),
            jax.ShapeDtypeStruct((sink.shape[0], own), f32),
        ),
        in_specs=[hbm] * 10 + [pl.BlockSpec(memory_space=pltpu.SMEM), hbm] + [inside] * 3,
        out_specs=[inside] * 2,
        scratch_shapes=[
            vmem((2, 4, own, half_d), bf16),
            vmem((2, rows, half_d), bf16),
            vmem((2, rows, H), f32),
            vmem((2, 1, half_d), f32),
            vmem((rows, 4 * H), f32),
            vmem((rows, 3 * H), f32),
            vmem((2, 2, run_rows + 2 * edge, H), bf16),
            vmem((rows, 2 * H), bf16),
            vmem((3, rows, H), bf16),
            vmem((2, 2, 2, 2) + decay_log.shape, f32),
            vmem((2, 8, run_rows), f32),
            vmem((2, run_rows, H), f32),
            vmem((2, 3, 8, H), f32),
            vmem((2, H, 2 * H), bf16),
            vmem((2, 2, 2, H, H), bf16), vmem((3, H, H), bf16),
            vmem((2, 4 * edge, 3 * H), bf16),
            vmem((2 * edge, 3 * edge), f32),
            vmem((2 * edge, H), f32),
            vmem((4, 2, 2 * edge), f32),
            vmem((4, 2, 2 * edge), f32),
            vmem((4,) + tile[1:], f32), vmem((8, 2, edge, own), f32), vmem(tile, bf16), vmem(tile, bf16),
            vmem((8, 2, 2, edge, own), bf16), vmem((8, 2, 2, edge, own), bf16),
            vmem((8, 2, edge, own), bf16), vmem((8, 2, edge, own), bf16),
            dma((3,)), dma((3,)), dma((1,)), dma((5,)), dma((2, 4, 2)), dma((2,)), dma((2, 16)),
            dma((2, 4)), dma((2, 3)), dma((2, 3)), pltpu.SemaphoreType.REGULAR,
            dma((8,)), dma((8,)), dma((8, 2)), dma((8, 2)), dma((8, 2)), dma((8, 2)),
        ]
        + stream((depth, 4 * H))
        + stream((depth, 3 * H))
        + stream((out_rows, own)),
        compiler_params=pltpu.CompilerParams(
            collective_id=0, has_side_effects=True, vmem_limit_bytes=67043328
        ),
        cost_estimate=pl.CostEstimate(
            flops=10**11, bytes_accessed=2 * 10**7, transcendentals=0
        ),
    )(
        tokens, gain.reshape(1, half_d), *args[2:10], sink, decay_log, cos_t, sin_t, base
    )
    return settle(mixed, logs)


def attend(query, key, value, sink, offset, total_rows):
    rows, kv, group, _ = query.shape
    ext = halo(jnp.stack([key, value]), "t", SPAN_RADIUS)
    size = min(rows, BLOCK)
    count = rows // size
    span = size + 2 * SPAN_RADIUS
    pieces = jnp.stack([ext[:, b * size : b * size + span] for b in range(count)])
    blocks = query.reshape(count, size, kv, group, HEAD_DIM)
    scores = jnp.einsum(
        "bqhgd,bkhd->bhgqk", blocks, pieces[:, 0], preferred_element_type=jnp.float32
    ) * HEAD_DIM ** (-0.5)
    base = offset + jnp.arange(count, dtype=jnp.int32) * size
    query_pos = base[:, None] + jnp.arange(size, dtype=jnp.int32)
    key_pos = base[:, None] - SPAN_RADIUS + jnp.arange(span, dtype=jnp.int32)
    spacing = key_pos[:, None, :] - query_pos[:, :, None]
    inside = (key_pos >= 0) & (key_pos < total_rows)
    valid = (jnp.abs(spacing) <= SPAN_RADIUS) & inside[:, None, :]
    masked = jnp.where(valid[:, None, None], scores, -jnp.inf)
    limit = sink[None, :, :, None]
    top = jnp.maximum(jnp.max(masked, axis=-1), limit)
    expo = jnp.exp(masked - top[..., None])
    total = jnp.sum(expo, axis=-1) + jnp.exp(limit - top)
    logs = top + jnp.log(total)
    probs = (expo / total[..., None]).astype(jnp.bfloat16)
    result = jnp.einsum(
        "bhgqk,bkhd->bqhgd", probs, pieces[:, 1], preferred_element_type=jnp.float32
    ).astype(jnp.bfloat16)
    logs = jnp.transpose(logs, (1, 2, 0, 3)).reshape(kv * group, rows)
    return result.reshape(rows, kv * group * HEAD_DIM), logs


def retain(query, key, value, decay):
    rows, heads, _ = query.shape
    peers, index = lax.axis_size("t"), lax.axis_index("t")
    cumul = jnp.cumsum(decay, axis=1)
    last = cumul[:, -1]
    query_f, key_f, value_f = (v.astype(jnp.float32) for v in (query, key, value))
    trailing = jnp.exp(last[:, None] - cumul)
    leading = jnp.exp(cumul)
    forward = jnp.einsum("hk,khd,khe->hde", trailing, key_f, value_f, precision=HIGHEST)
    backward = jnp.einsum("hk,khd,khe->hde", leading, key_f, value_f, precision=HIGHEST)
    tail = jnp.broadcast_to(last[:, None, None], (heads, 8, HEAD_DIM))
    sent = jnp.concatenate([forward, backward, tail], axis=1)
    seen = lax.all_gather(sent, "t", axis=0)
    lasts = seen[:, :, 2 * HEAD_DIM, 0]
    at = jnp.arange(peers)
    low = jnp.minimum(at, index)[:, None]
    high = jnp.maximum(at, index)[:, None]
    between = (at[None, :] > low) & (at[None, :] < high)
    spans = jnp.exp(jnp.sum(jnp.where(between[:, :, None], lasts[None], 0.0), axis=1))
    before = jnp.sum(
        jnp.where(at < index, 1.0, 0.0)[:, None, None, None]
        * spans[:, :, None, None]
        * seen[:, :, :HEAD_DIM],
        axis=0,
    )
    after = jnp.sum(
        jnp.where(at > index, 1.0, 0.0)[:, None, None, None]
        * spans[:, :, None, None]
        * seen[:, :, HEAD_DIM : 2 * HEAD_DIM],
        axis=0,
    )
    scores = jnp.einsum("qhd,khd->hqk", query, key, preferred_element_type=jnp.float32)
    weights = jnp.exp(-jnp.abs(cumul[:, :, None] - cumul[:, None, :]))
    mix = jnp.einsum("hqk,khd->qhd", scores * weights, value_f, precision=HIGHEST)
    mix = mix + leading.T[:, :, None] * jnp.einsum(
        "qhd,hde->qhe", query_f, before, precision=HIGHEST
    )
    mix = mix + trailing.T[:, :, None] * jnp.einsum(
        "qhd,hde->qhe", query_f, after, precision=HIGHEST
    )
    middle = mix - jnp.mean(mix, axis=-1, keepdims=True)
    normed = middle * lax.rsqrt(jnp.mean(middle * middle, axis=-1, keepdims=True) + 1e-06)
    return normed.astype(jnp.bfloat16).reshape(rows, heads * HEAD_DIM)


def shards(
    tokens, gain, q_att, k_att, v_att, q_ret, k_ret, v_ret, out_att, out_ret, sink, decay_log
):
    parts = lax.axis_size("h")
    own = tokens.shape[0]
    rows = own * parts
    width = tokens.shape[1] * lax.axis_size("tp")
    kv = k_att.shape[1] // HEAD_DIM // parts
    group = q_att.shape[1] // k_att.shape[1]
    att = kv * group
    ret = q_ret.shape[1] // HEAD_DIM // parts
    offset = lax.axis_index("t") * rows
    total_rows = rows * lax.axis_size("t")

    packed = jnp.concatenate(
        [
            w.reshape(w.shape[0], parts, w.shape[1] // parts)
            for w in (q_att, k_att, v_att, q_ret, k_ret, v_ret)
        ],
        axis=2,
    )
    packed = jnp.moveaxis(packed, 1, 0)
    out_pack = jnp.concatenate(
        [w.reshape(parts, w.shape[0] // parts, w.shape[1]) for w in (out_att, out_ret)], axis=1
    )
    widened = tokens.astype(jnp.float32)
    sums = jnp.sum(widened * widened, axis=1)
    scaled = (widened * gain).astype(jnp.bfloat16)
    cores = lax.axis_size("tp")
    flat = packed.reshape(parts * packed.shape[1], packed.shape[2])
    weight = gather(exchange(flat, "h", 0, 0), "t", 0)
    whole = gather(gather(scaled, "h", 0), "tp", 1)
    proj = jnp.dot(whole, weight, preferred_element_type=jnp.float32)
    out_own = exchange(out_pack, "h", 0, 0)
    sums = lax.all_gather(sums, ("h", "tp"))
    decay = exchange(decay_log, "h", 0, 1)
    squares = jnp.sum(sums.reshape(parts, cores, own), axis=1).reshape(rows)
    inverse = lax.rsqrt(squares / width + 1e-06)[:, None]

    edges = [att, kv, kv, ret, ret, ret]
    starts = [sum(edges[:i]) * HEAD_DIM for i in range(6)]
    qa, ka, va, qr, kr, vr = (
        proj[:, s : s + n * HEAD_DIM].reshape(rows, n, HEAD_DIM) for s, n in zip(starts, edges)
    )
    scale = inverse[:, :, None]
    positions = (offset + jnp.arange(rows, dtype=jnp.int32)).astype(jnp.float32)
    freqs = 10000.0 ** (-jnp.arange(0, HEAD_DIM, 2).astype(jnp.float32) / HEAD_DIM)
    angles = positions[:, None] * freqs[None, :]
    cosine, sine = jnp.cos(angles)[:, None, :], jnp.sin(angles)[:, None, :]
    att_query = rotate(qa * scale, cosine, sine)
    att_key = rotate(ka * scale, cosine, sine)
    att_value = (va * scale).astype(jnp.bfloat16)
    ret_query = (qr * scale).astype(jnp.bfloat16)
    ret_key = (kr * (scale * HEAD_DIM ** (-0.5))).astype(jnp.bfloat16)
    ret_value = (vr * scale).astype(jnp.bfloat16)

    logits = lax.dynamic_slice_in_dim(sink, lax.axis_index("h") * att, att).reshape(kv, group)
    att_out, logs = attend(
        att_query.reshape(rows, kv, group, HEAD_DIM), att_key, att_value, logits, offset, total_rows
    )
    ret_out = retain(ret_query, ret_key, ret_value, decay)

    out_wide = gather(out_own, "t", 0)
    mixers = jnp.concatenate([att_out, ret_out], axis=1)
    depth = out_wide.shape[1]
    out_wide = jnp.moveaxis(out_wide, 0, 1).reshape(depth, -1)
    mixed = jnp.dot(mixers, out_wide, preferred_element_type=jnp.float32).astype(jnp.bfloat16)
    mixed = lax.psum_scatter(mixed, ("h", "tp"), scatter_dimension=0, tiled=True)
    return mixed, exchange(logs, "h", 1, 0)


def fits(args, sp, tp):
    tokens, _, q_att, k_att, v_att, q_ret, k_ret, v_ret, out_att, _, _, decay = args
    own, heads = tokens.shape[0] // sp, 4 * tp
    return (
        sp == 16
        and tp == 2
        and own == 2 * SPAN_RADIUS
        and q_att.shape[0] == sp * own
        and tokens.shape[1] == sp * own
        and q_att.shape[1] == 2 * heads * HEAD_DIM
        and all(v.shape[1] == heads * HEAD_DIM for v in (k_att, v_att, q_ret, k_ret, v_ret))
    )


def solution(mesh):
    sp, tp = mesh.shape["sp"], mesh.shape["tp"]

    def run(*args):
        if fits(args, sp, tp):
            seq = ("zh", "zl", "y", "x")
            fine = Mesh(mesh.devices.reshape(2, 2, 2, 2, tp), seq + ("tp",))
            step = fused
        else:
            heads = math.gcd(args[3].shape[1], args[5].shape[1]) // HEAD_DIM
            parts = math.gcd(heads // math.gcd(heads, tp), sp)
            seq = ("t", "h")
            fine = Mesh(mesh.devices.reshape(sp // parts, parts, tp), seq + ("tp",))
            step = shards
        body = jax.shard_map(
            step,
            mesh=fine,
            in_specs=(P(seq, "tp"), P("tp"))
            + (P(seq, "tp"),) * 6
            + (P("tp", seq), P("tp", seq), P("tp"), P("tp", seq)),
            out_specs=(P(seq + ("tp",), None), P("tp", seq)),
            check_vma=False,
        )
        return body(*args)

    return run
```

```python
import math

import jax
import jax.numpy as jnp
import numpy as np
from jax import lax
from jax.experimental import pallas as pl
from jax.experimental.pallas import tpu as pltpu
from jax.sharding import Mesh
from jax.sharding import PartitionSpec as P

HEAD_DIM = 128
SPAN_RADIUS = 128
BLOCK = 256
HIGHEST = lax.Precision.HIGHEST
MESH = pl.DeviceIdType.MESH


def gather(x, axis, dim):
    if lax.axis_size(axis) == 1:
        return x
    return lax.all_gather(x, axis, axis=dim, tiled=True)


def exchange(x, axis, split, concat):
    if lax.axis_size(axis) == 1:
        return x
    return lax.all_to_all(x, axis, split, concat, tiled=True)


def halo(shard, axis, width):
    peers, length = lax.axis_size(axis), shard.shape[1]
    up = [(i, i + 1) for i in range(peers - 1)]
    down = [(j, i) for i, j in up]
    before = lax.ppermute(shard[:, length - width :], axis, up)
    after = lax.ppermute(shard[:, :width], axis, down)
    return jnp.concatenate([before, shard, after], axis=1)


def rotate(values, cosine, sine):
    half = values.shape[-1] // 2
    first, second = values[..., :half], values[..., half:]
    return jnp.concatenate(
        [first * cosine - second * sine, second * cosine + first * sine], axis=-1
    ).astype(jnp.bfloat16)


def flip(v, bit):
    return v + bit - 2 * v * bit


PARTS = 2


class Both:
    def __init__(self, *copies):
        self.copies = copies

    def start(self):
        for copy in self.copies:
            copy.start()

    def wait_send(self):
        for copy in self.copies:
            copy.wait_send()


class Stream:
    def __init__(self, where, remote, refs, pack, split=False):
        self.where, self.remote, self.pack, self.split = where, remote, pack, split
        (
            self.wide, self.away, self.out,
            self.load, self.x_send, self.z_send, self.h_send, self.y_send,
            self.p_recv, self.w_recv, self.more_send, self.more_recv,
        ) = refs

    def fetch(self):
        w = self.where
        targets = (
            (self.out.at[0], 1 - w.g, 1 - w.x),
            (self.out.at[1], w.g, 1 - w.x),
            (self.wide.at[w.own], w.g, w.x),
            (self.away.at[w.x], 1 - w.g, w.x),
        )
        for i, (target, g, x) in enumerate(targets):
            self.pack(2 * g + x, target, self.load.at[i])

    def fetched(self):
        w = self.where
        for i, target in enumerate(
            (self.out.at[0], self.out.at[1], self.wide.at[w.own], self.away.at[w.x])
        ):
            pltpu.make_async_copy(target, target, self.load.at[i]).wait()

    def along_x(self, k):
        w = self.where
        if k == 0:
            return self.remote(
                self.out.at[0], self.away.at[w.x], self.x_send.at[0], self.p_recv.at[0], w.to_x
            )
        return self.remote(
            self.out.at[1], self.wide.at[w.own], self.x_send.at[1], self.w_recv.at[w.own], w.to_x
        )

    def along_z(self, k):
        w = self.where
        x = w.x if k == 0 else 1 - w.x
        s = w.at(w.zh, w.zl, w.y, x)
        return self.remote(
            self.away.at[x], self.wide.at[s], self.z_send.at[k], self.w_recv.at[s], w.to_z
        )

    def near(self, k):
        w = self.where
        return w.at(w.zh, flip(w.zl, k // 2), w.y, flip(w.x, k % 2))

    def far(self, k):
        w = self.where
        return w.at(1 - w.zh, flip(w.zl, 1 - k // 2), w.y, flip(w.x, k % 2))

    def across(self, k):
        w = self.where
        return w.at(1 - w.zh, flip(w.zl, 1 - k // 2), 1 - w.y, flip(w.x, k % 2))

    def parts_of(self, s, hop, k, to):
        rows = self.wide.shape[1] // PARTS
        pieces = [self.wide.at[s, pl.ds(i * rows, rows), :] for i in range(PARTS)]
        return [
            self.remote(
                piece, piece, self.more_send.at[hop, k, i], self.more_recv.at[hop, k, i], to
            )
            for i, piece in enumerate(pieces)
        ]

    def along_h(self, k):
        s = self.near(k)
        if self.split:
            return Both(*self.parts_of(s, 0, k, self.where.to_h))
        return self.remote(
            self.wide.at[s], self.wide.at[s], self.h_send.at[k], self.w_recv.at[s], self.where.to_h
        )

    def along_y(self, k, far=0):
        s = self.far(k) if far else self.near(k)
        if far and self.split:
            return Both(*self.parts_of(s, 1, k, self.where.to_y))
        return self.remote(
            self.wide.at[s], self.wide.at[s],
            self.y_send.at[4 * far + k], self.w_recv.at[s], self.where.to_y,
        )

    def pass_far(self, k):
        if self.split:
            arrivals = self.parts_of(self.far(k), 0, k, self.where.to_h)
            for arrival, copy in zip(arrivals, self.along_y(k, 1).copies):
                arrival.wait_recv()
                copy.start()
        else:
            self.arrive(self.far(k))
            self.along_y(k, 1).start()

    def arrive_far_across(self, k):
        s = self.across(k)
        if self.split:
            for arrival in self.parts_of(s, 1, k, self.where.to_y):
                arrival.wait_recv()
        else:
            self.arrive(s)

    def arrive(self, s):
        self.remote(
            self.wide.at[s], self.wide.at[s], self.x_send.at[0], self.w_recv.at[s], self.where.to_x
        ).wait_recv()

    def arrive_away(self):
        w = self.where
        slot = self.away.at[1 - w.x]
        self.remote(slot, slot, self.x_send.at[0], self.p_recv.at[0], w.to_x).wait_recv()

    def arrive_across(self, far):
        w = self.where
        zh = 1 - w.zh if far else w.zh
        for zl in range(2):
            for x in range(2):
                self.arrive(w.at(zh, zl, 1 - w.y, x))

    def drain(self):
        for k in range(2):
            self.along_x(k).wait_send()
            self.along_z(k).wait_send()
        for k in range(4):
            self.along_h(k).wait_send()
            self.along_y(k).wait_send()
            self.along_y(k, 1).wait_send()


class Place:
    def __init__(self):
        self.zh, self.zl, self.y, self.x, self.c = (
            lax.axis_index(a) for a in ("zh", "zl", "y", "x", "tp")
        )
        self.g = lax.rem(self.zh + self.zl, 2)
        self.h = 2 * self.g + self.x
        self.own = self.at(self.zh, self.zl, self.y, self.x)
        self.b = 2 * self.zl + self.x
        self.to_x = {"x": 1 - self.x}
        self.to_z = {"zl": 1 - self.zl}
        self.to_y = {"y": 1 - self.y}
        self.to_h = {"zh": 1 - self.zh, "zl": 1 - self.zl}
        self.to_hy = {"zh": 1 - self.zh, "zl": 1 - self.zl, "y": 1 - self.y}
        self.to_zx = {"zl": 1 - self.zl, "x": 1 - self.x}
        self.to_c = {"tp": 1 - self.c}
        self.to_zc = {"zl": 1 - self.zl, "tp": 1 - self.c}

    @staticmethod
    def at(zh, zl, y, x):
        return ((zh * 2 + zl) * 2 + y) * 2 + x


def fused_kernel(
    tokens, gain, q_att, k_att, v_att, q_ret, k_ret, v_ret, out_att, out_ret, sink, decay,
    cos_t, sin_t, base,
    mixed, logs_out,
    raw, scl, ssq, gains, acc_a, acc_r, kvext, qrot, rets, dec, cumr, cumc, coef, states, stall, crossing,
    mix, bias, logm, lsend, lrecv, mine, kept, give, take, s1, r1, s2, r2,
    t_load, t_x, t_z, t_c, t_recv, g_sem, d_sem, halo_sem, st_sem, l_sem, go,
    give_s, take_r, s1_s, r1_r, s2_s, r2_r,
    *streams,
):
    w = Place()
    y = w.y
    f32, bf16 = jnp.float32, jnp.bfloat16
    own, half_d = tokens.shape
    rows = 4 * own
    run_rows = 2 * own
    total_rows = 16 * own
    H = HEAD_DIM
    edge = SPAN_RADIUS

    def remote(src, dst, send, recv, to):
        return pltpu.make_async_remote_copy(
            src_ref=src, dst_ref=dst, send_sem=send, recv_sem=recv,
            device_id=to, device_id_type=MESH,
        )

    def lanes(h, n):
        return pl.ds(pl.multiple_of(h * n, n), n)

    def pack_cols(parts):
        def pack(h, target, sem):
            start = 0
            for ref in parts:
                n = ref.shape[1] // 4
                pltpu.make_async_copy(
                    ref.at[:, lanes(h, n)], target.at[:, pl.ds(start, n)], sem
                ).start()
                start += n
        return pack

    def pack_rows(parts):
        def pack(h, target, sem):
            start = 0
            for ref in parts:
                n = ref.shape[0] // 4
                pltpu.make_async_copy(
                    ref.at[lanes(h, n), :], target.at[pl.ds(start, n), :], sem
                ).start()
                start += n
        return pack

    n = len(streams) // 3
    A = Stream(w, remote, streams[:n], pack_cols((q_att, k_att, v_att)), True)
    R = Stream(w, remote, streams[n : 2 * n], pack_cols((q_ret, k_ret, v_ret)), True)
    O = Stream(w, remote, streams[2 * n :], pack_rows((out_att, out_ret)))

    token_load = pltpu.make_async_copy(tokens, raw.at[w.c, w.b], t_load.at[0])
    gain_load = pltpu.make_async_copy(gain, gains.at[w.c], t_load.at[1])
    decay_load = pltpu.make_async_copy(decay, dec.at[w.zh, w.y, w.zl, w.x], t_load.at[2])

    def block(zl, x):
        return 2 * zl + x

    def order(k):
        return block((w.zl, 1 - w.zl)[k // 2], (w.x, 1 - w.x)[k % 2])

    def token(e, k, part, send, to):
        here = raw.at[e, order(k)]
        if part is not None:
            here = here.at[pl.ds(part * edge, edge), :]
        return remote(here, here, send, t_recv.at[e, order(k), part or 0], to)

    tokens_x = [token(w.c, 0, None, t_x.at[0], w.to_x)]
    tokens_x += [token(w.c, 2, i, t_x.at[1 + i], w.to_x) for i in range(2)]
    tokens_z = token(w.c, 0, None, t_z.at[0], w.to_z)
    tokens_c = [token(w.c, k, None, t_c.at[k], w.to_c) for k in range(3)]
    tokens_c += [token(w.c, 3, i, t_c.at[3 + i], w.to_c) for i in range(2)]

    def token_arrive(k, e=None, part=None):
        token(w.c if e is None else e, k, part, t_x.at[0], w.to_x).wait_recv()

    gain_c = remote(gains.at[w.c], gains.at[w.c], g_sem.at[0], g_sem.at[1], w.to_c)

    def others(i):
        return tuple(flip(v, (i >> k) & 1) for v, k in ((w.zh, 3), (w.zl, 2), (w.y, 1), (w.x, 0)))

    def peer(i):
        return dict(zip(("zh", "zl", "y", "x"), others(i)))

    def decay_send(i):
        here = dec.at[w.zh, w.y, w.zl, w.x]
        return remote(here, here, d_sem.at[0, i], d_sem.at[1, i], peer(i))

    def decay_arrive(i):
        zh, zl, yy, x = others(i)
        here = dec.at[zh, yy, zl, x]
        remote(here, here, d_sem.at[0, i], d_sem.at[1, i], peer(i)).wait_recv()

    decay_load.start()
    R.fetch()
    A.fetch()
    gain_load.start()
    token_load.start()
    O.fetch()

    barrier = pltpu.get_barrier_semaphore()
    for to in (w.to_c, w.to_zc):
        pl.semaphore_signal(barrier, inc=1, device_id=to, device_id_type=MESH)
    for i in range(1, 16):
        pl.semaphore_signal(barrier, inc=1, device_id=peer(i), device_id_type=MESH)
    pl.semaphore_wait(barrier, 17)

    middle = w.g == 1

    decay_load.wait()
    for i in range(1, 16):
        decay_send(i).start()
    R.fetched()
    R.along_x(0).start()
    R.along_z(0).start()
    R.along_y(0).start()
    A.fetched()
    A.along_x(0).start()
    A.along_z(0).start()
    A.along_y(0).start()
    R.along_x(1).start()
    A.along_x(1).start()

    @pl.when(middle)
    def _():
        R.along_h(0).start()
        A.along_h(0).start()

    O.fetched()
    O.along_x(1).start()
    O.along_x(0).start()
    token_load.wait()
    tokens_x[0].start()
    gain_load.wait()
    gain_c.start()
    tokens_c[0].start()

    def scale(e, b, first=0, last=None):
        @pl.loop(first // 16, (own if last is None else last) // 16)
        def _(i):
            value = raw[e, b, pl.ds(pl.multiple_of(i * 16, 16), 16), :].astype(f32)
            at = pl.ds(pl.multiple_of(b * own + i * 16, 16), 16)
            scl[e, at, :] = (value * gains[e]).astype(bf16)
            square = value * value
            total = square[:, :H]
            for k in range(1, half_d // H):
                total = total + square[:, k * H : (k + 1) * H]
            ssq[e, at, :] = total

    @pl.when((w.zh == 0) & (w.y == 0))
    def _():
        kvext[0, :, 0:edge, :] = jnp.zeros((2, edge, H), bf16)

    @pl.when((w.zh == 1) & (w.y == 1))
    def _():
        kvext[1, :, edge + run_rows :, :] = jnp.zeros((2, edge, H), bf16)

    scale(w.c, w.b)
    for stream in (R, A):
        stream.arrive_away()
        stream.along_z(1).start()
    tokens_z.start()
    remote(gains.at[1 - w.c], gains.at[1 - w.c], g_sem.at[0], g_sem.at[1], w.to_c).wait_recv()
    token_arrive(0, 1 - w.c)
    scale(1 - w.c, w.b)

    def pass_near(stream, k):
        stream.arrive(stream.near(k))
        stream.along_y(k).start()

        @pl.when(middle)
        def _():
            stream.along_h(k).start()

    def pass_far(stream, k):
        stream.pass_far(k)

    pass_near(R, 2)
    pass_near(A, 2)
    for k in (1, 3):
        pass_near(R, k)
        pass_near(A, k)

    O.along_y(0).start()
    O.along_z(0).start()

    @pl.when(w.g == 0)
    def _():
        for stream in (R, A):
            for k in range(4):
                stream.along_h(k).start()

    @pl.when(middle)
    def _():
        O.along_h(0).start()

    row = lax.broadcasted_iota(jnp.int32, bias.shape, 0)
    shift = lax.broadcasted_iota(jnp.int32, bias.shape, 1) - lax.rem(row, edge)
    bias[...] = jnp.where((shift >= 0) & (shift <= 2 * edge), 0.0, -jnp.inf)
    logm[...] = jnp.zeros_like(logm)
    for i in range(1, 16):
        decay_arrive(i)

    lane = lax.broadcasted_iota(jnp.int32, (8, run_rows), 1)
    for slot in range(2):
        row = jnp.concatenate(
            [dec[w.zh, w.y, slot, x, pl.ds(w.h, 1), :] for x in range(2)], axis=1
        )
        row = jnp.broadcast_to(row, (8, run_rows))
        step = 1
        while step < run_rows:
            row = row + jnp.where(lane >= step, pltpu.roll(row, step, axis=1), 0.0)
            step *= 2
        cumr[slot] = row
        cumc[slot] = jnp.transpose(jnp.broadcast_to(row[0:1], (H, run_rows)))
    lane = lax.broadcasted_iota(jnp.int32, (8, H), 1)
    run = lax.broadcasted_iota(jnp.int32, (8, H), 0)
    totals = jnp.zeros((8, H), f32)
    for zh in range(2):
        for slot in range(2):
            for yy in range(2):
                pair = sum(dec[zh, yy, slot, x, pl.ds(w.h, 1), :] for x in range(2))
                value = jnp.sum(pair, axis=1, keepdims=True)
                totals = jnp.where(lane == 4 * zh + 2 * slot + yy, value, totals)
    for slot in range(2):
        me = 4 * w.zh + 2 * slot + w.y
        between = (lane > jnp.minimum(run, me)) & (lane < jnp.maximum(run, me))
        factor = jnp.exp(jnp.sum(jnp.where(between, totals, 0.0), axis=1, keepdims=True))
        factor = jnp.broadcast_to(factor, (8, H))
        near = run // 4 == w.zh
        coef[slot, 0] = jnp.where(near & (run < me), factor, 0.0)
        coef[slot, 1] = jnp.where(near & (run > me), factor, 0.0)
        between = (lane > jnp.where(w.zh == 0, me, 3)) & (lane < jnp.where(w.zh == 0, 4, me))
        factor = jnp.exp(jnp.sum(jnp.where(between, totals, 0.0), axis=1, keepdims=True))
        coef[slot, 2] = jnp.broadcast_to(factor, (8, H))

    pass_near(O, 1)

    @pl.when(middle)
    def _():
        for stream in (R, A):
            for k in (0, 2, 1, 3):
                pass_far(stream, k)

    def part_of(stream, zh, b, start, width):
        at = pl.ds(pl.multiple_of(b * own, own), own)
        depth = half_d // own
        weight = stream.wide[pl.ds(zh * depth, depth), :, start : start + width]
        return jnp.dot(
            scl[zh, at, :], weight.reshape(half_d, width), preferred_element_type=f32
        )

    def first_part(stream, acc, b):
        at = pl.ds(pl.multiple_of(b * own, own), own)
        start = 0
        while start < acc.shape[1]:
            width = min(2 * H, acc.shape[1] - start)
            acc[at, start : start + width] = part_of(stream, w.zh, b, start, width)
            start += width

    def pair_of(stream, zl, yy, b, start, width):
        zh = 1 - w.zh
        at = pl.ds(pl.multiple_of(b * own, own), own)
        depth = pl.ds(pl.multiple_of((2 * zl + yy) * 2 * own, 2 * own), 2 * own)
        weight = stream.wide[pl.ds(w.at(zh, zl, yy, 0), 2), :, start : start + width]
        return jnp.dot(
            scl[zh, at, depth], weight.reshape(2 * own, width), preferred_element_type=f32
        )

    def add_pair(stream, acc, zl, yy, b):
        at = pl.ds(pl.multiple_of(b * own, own), own)
        for start in range(0, acc.shape[1], 2 * H):
            width = min(2 * H, acc.shape[1] - start)
            acc[at, start : start + width] += pair_of(stream, zl, yy, b, start, width)

    def last_of(stream, acc, b, start, width):
        at = pl.ds(pl.multiple_of(b * own, own), own)
        return acc[at, start : start + width] + pair_of(stream, w.zl, 1 - w.y, b, start, width)

    def whole_of(stream, acc, b, start, width):
        at = pl.ds(pl.multiple_of(b * own, own), own)
        return acc[at, start : start + width] + part_of(stream, 1 - w.zh, b, start, width)

    token_arrive(2)
    for copy in tokens_x[1:]:
        copy.start()
    tokens_c[2].start()
    scale(w.c, order(2))
    token_arrive(2, 1 - w.c)
    scale(1 - w.c, order(2))
    token_arrive(1)
    tokens_c[1].start()
    scale(w.c, order(1))

    @pl.when(w.g == 0)
    def _():
        pass_far(R, 0)

    O.arrive_away()
    O.along_z(1).start()
    token_arrive(1, 1 - w.c)
    scale(1 - w.c, order(1))

    @pl.when(w.g == 0)
    def _():
        pass_far(R, 1)

    R.arrive_across(0)
    A.arrive_across(0)
    for k in (2, 0):
        first_part(R, acc_r, order(k))
        first_part(A, acc_a, order(k))

    @pl.when(w.g == 0)
    def _():
        pass_far(R, 2)

    first_part(R, acc_r, order(1))
    first_part(A, acc_a, order(1))
    @pl.when(w.g == 0)
    def _():
        pass_far(R, 3)

    token_arrive(3, None, 0)
    tokens_c[3].start()
    scale(w.c, order(3), 0, edge)
    token_arrive(3, 1 - w.c, 0)
    scale(1 - w.c, order(3), 0, edge)

    @pl.when(w.g == 0)
    def _():
        pass_far(A, 0)

    token_arrive(3, None, 1)
    tokens_c[4].start()

    @pl.when(w.g == 0)
    def _():
        pass_far(A, 1)

    scale(w.c, order(3), edge, own)
    token_arrive(3, 1 - w.c, 1)
    scale(1 - w.c, order(3), edge, own)
    first_part(R, acc_r, order(3))
    first_part(A, acc_a, order(3))

    def inverse(b):
        at = pl.ds(pl.multiple_of(b * own, own), own)
        squares = jnp.sum(ssq[0, at, :] + ssq[1, at, :], axis=1, keepdims=True)
        return lax.rsqrt(squares / (2 * half_d) + 1e-06)

    def angles(b):
        s = w.at(w.zh, b // 2, w.y, b % 2)
        c0, s0, s0n, c0n = (base[i, pl.ds(s, 1), :] for i in range(4))
        cosine = cos_t[...] * c0 - sin_t[...] * s0
        sine = cos_t[...] * s0n + sin_t[...] * c0n
        return cosine, sine

    def turn(value, cosine, sine):
        return (value * cosine + pltpu.roll(value, H // 2, axis=1) * sine).astype(bf16)

    def keys_values(b):
        scale_b = inverse(b)
        cosine, sine = angles(b)
        both = last_of(A, acc_a, b, 2 * H, 2 * H) * scale_b
        inner = pl.ds(pl.multiple_of(edge + (b % 2) * own, edge), own)
        kvext[b // 2, 0, inner, :] = turn(both[:, :H], cosine, sine)
        kvext[b // 2, 1, inner, :] = both[:, H:].astype(bf16)

    def queries(b):
        at = pl.ds(pl.multiple_of(b * own, own), own)
        cosine, sine = angles(b)
        query = last_of(A, acc_a, b, 0, 2 * H) * inverse(b)
        qrot[at, :H] = turn(query[:, :H], cosine, sine)
        qrot[at, H:] = turn(query[:, H:], cosine, sine)

    for k in range(4):
        R.arrive_far_across(k)

    def retention_inputs(b):
        at = pl.ds(pl.multiple_of(b * own, own), own)
        scale_b = inverse(b)
        both = whole_of(R, acc_r, b, 0, 2 * H)
        rets[0, at, :] = (both[:, :H] * scale_b).astype(bf16)
        rets[1, at, :] = (both[:, H:] * (scale_b * H ** (-0.5))).astype(bf16)
        rets[2, at, :] = (whole_of(R, acc_r, b, 2 * H, H) * scale_b).astype(bf16)

    @pl.when(w.g == 0)
    def _():
        pass_far(A, 2)

    @pl.loop(0, 4, unroll=True)
    def _(b):
        retention_inputs(b)

    for slot in range(2):
        at = pl.ds(slot * run_rows, run_rows)
        last = cumr[slot, 0:1, run_rows - 1 : run_rows]
        key, value = rets[1, at, :].astype(f32), rets[2, at, :]
        for i, weight in enumerate((jnp.exp(last - cumc[slot]), jnp.exp(cumc[slot]))):
            lhs = (key * weight).astype(bf16)
            state = lax.dot_general(
                lhs, value, (((0,), (0,)), ((), ())), preferred_element_type=f32
            ).astype(bf16)
            stall[y, slot, i] = state
    total = jnp.zeros((H, H), f32)
    for slot in range(2):
        total = total + coef[slot, 2, 0:1, :] * stall[y, slot, w.zh].astype(f32)
    crossing[2] = total.astype(bf16)
    state_sends = [
        remote(stall.at[y], stall.at[y], st_sem.at[0, 0], st_sem.at[1, 0], w.to_y),
        remote(crossing.at[2], crossing.at[0], st_sem.at[0, 1], st_sem.at[1, 1], w.to_h),
        remote(crossing.at[2], crossing.at[1], st_sem.at[0, 2], st_sem.at[1, 2], w.to_hy),
    ]
    state_sends[1].start()
    state_sends[2].start()

    def inner_tile(i):
        slot = i // 2
        at = pl.ds(pl.multiple_of(i * own, own), own)
        keys = pl.ds(pl.multiple_of(slot * run_rows, run_rows), run_rows)
        score = lax.dot_general(
            rets[0, at, :], rets[1, keys, :], (((1,), (1,)), ((), ())),
            preferred_element_type=f32,
        )
        column = cumc[slot, pl.ds(pl.multiple_of((i % 2) * own, own), own), :]
        column = jnp.concatenate([column] * (run_rows // H), axis=1)
        weight = jnp.exp(-jnp.abs(column - cumr[slot, 0:1, :]))
        acc_r[at, :H] = jnp.dot(
            (score * weight).astype(bf16), rets[2, keys, :], preferred_element_type=f32
        )

    @pl.loop(0, 4, unroll=True)
    def _(i):
        inner_tile(i)

    @pl.when(w.g == 0)
    def _():
        pass_far(A, 3)

    @pl.loop(0, 8)
    def _(i):
        add_pair(A, acc_a, i // 4, y, i % 4)

    for k in range(2):
        A.arrive_far_across(k)

    @pl.loop(0, 4)
    def _(b):
        add_pair(A, acc_a, 1 - w.zl, 1 - y, b)

    for k in range(2, 4):
        A.arrive_far_across(k)

    @pl.loop(0, 4, unroll=True)
    def _(b):
        keys_values(b)

    head, tail, before_at, after_at = edge, run_rows, 0, edge + run_rows

    def pick(a, b):
        return a + (b - a) * y

    def piece(slot, start):
        return kvext.at[slot, :, pl.ds(pl.multiple_of(start, edge), edge), :]

    halo_y = [
        remote(
            piece(pick(s0, s1), pick(f0, f1)), piece(pick(d0, d1), pick(o0, o1)),
            halo_sem.at[0, i], halo_sem.at[1, i], w.to_y,
        )
        for i, (s0, f0, d0, o0, s1, f1, d1, o1) in enumerate(
            (
                (0, tail, 0, before_at, 0, head, 0, after_at),
                (1, head, 0, after_at, 0, tail, 1, before_at),
                (1, tail, 1, before_at, 1, head, 1, after_at),
            )
        )
    ]
    halo_far = remote(
        piece(pick(0, 1), pick(head, tail)), piece(pick(1, 0), pick(after_at, before_at)),
        halo_sem.at[0, 3], halo_sem.at[1, 3], w.to_hy,
    )
    has_far = ((y == 0) & (w.zh == 1)) | ((y == 1) & (w.zh == 0))
    for copy in halo_y:
        copy.start()

    @pl.when(has_far)
    def _():
        halo_far.start()

    state_sends[0].start()

    @pl.when(middle)
    def _():
        for copy in state_sends[1:]:
            copy.wait_send()

        @pl.when(has_far)
        def _():
            halo_far.wait_send()

        for to in (w.to_z, w.to_zc):
            pl.semaphore_signal(go, inc=1, device_id=to, device_id_type=MESH)

    @pl.when(middle)
    def _():
        for k in (2, 3):
            O.arrive(O.near(k))
            O.along_h(k).start()
            O.along_y(k).start()

    @pl.loop(0, 4, unroll=True)
    def _(b):
        queries(b)

    def halo_arrive(slot, start, i, to):
        here = piece(slot, start)
        remote(here, here, halo_sem.at[0, i], halo_sem.at[1, i], to).wait_recv()

    def attend_tile(i, at_end):
        slot, j = i // 4, i % 4
        query = qrot[pl.ds(pl.multiple_of(i * edge, edge), edge), :]
        query = jnp.concatenate([query[:, :H], query[:, H:]], axis=0)
        span = pl.ds(pl.multiple_of(j * edge, edge), 3 * edge)
        key, value = kvext[slot, 0, span, :], kvext[slot, 1, span, :]
        score = lax.dot_general(
            query, key, (((1,), (1,)), ((), ())), preferred_element_type=f32
        ) * H ** (-0.5)
        masked = score + bias[...]
        if at_end:
            col = lax.broadcasted_iota(jnp.int32, (1, 3 * edge), 1)
            start = w.at(w.zh, slot, y, 0) * own + j * edge - edge
            inside = (col >= -start) & (col < total_rows - start)
            masked = masked + jnp.where(inside, 0.0, -jnp.inf)
        first = lax.broadcasted_iota(jnp.int32, (2 * edge, 1), 0) < edge
        limit = jnp.where(first, sink[2 * w.h], sink[2 * w.h + 1])
        top = jnp.maximum(jnp.max(masked, axis=1, keepdims=True), limit)
        expo = jnp.exp(masked - top)
        total = jnp.sum(expo, axis=1, keepdims=True) + jnp.exp(limit - top)
        logs = top + jnp.log(total)
        probs = (expo * (1.0 / total)).astype(bf16)
        result = jnp.dot(probs, value, preferred_element_type=f32).astype(bf16)
        at = pl.ds(pl.multiple_of((i // 2) * edge, edge), edge)
        mix[i % 2, at, 0:H] = result[:edge]
        mix[i % 2, at, H : 2 * H] = result[edge:]
        column = lax.broadcasted_iota(jnp.int32, (2 * edge, H), 1)
        logm[...] = jnp.where(column == i, logs, logm[...])

    @pl.when(w.g == 0)
    def _():
        pl.semaphore_wait(go, 2)
        for k in range(4):
            if k > 1:
                O.arrive(O.near(k))
            O.along_h(k).start()

    @pl.loop(0, 4, unroll=True)
    def _(i):
        attend_tile(4 * (i // 2) + 1 + i % 2, False)

    halo_arrive(pick(0, 0), pick(after_at, before_at), 0, w.to_y)
    halo_arrive(pick(1, 0), pick(before_at, after_at), 1, w.to_y)
    halo_arrive(pick(1, 1), pick(after_at, before_at), 2, w.to_y)

    @pl.when(has_far)
    def _():
        halo_arrive(pick(0, 1), pick(before_at, after_at), 3, w.to_hy)

    @pl.when(w.g == 0)
    def _():
        O.along_y(2).start()
        O.along_y(3).start()

    @pl.loop(0, 4, unroll=True)
    def _(i):
        attend_tile(4 * (i // 2) + 3 * (i % 2), True)

    for i, here in enumerate((stall.at[1 - y], crossing.at[0], crossing.at[1])):
        remote(here, here, st_sem.at[0, i], st_sem.at[1, i], w.to_y).wait_recv()
    crossed = crossing[0].astype(f32) + crossing[1].astype(f32)
    for slot in range(2):
        for i in range(2):
            total = jnp.where(w.zh == 1 - i, 1.0, 0.0) * coef[slot, 2, 0:1, :] * crossed
            for s in range(2):
                for yy in range(2):
                    for zh in range(2):
                        r = 4 * zh + 2 * s + yy
                        total = total + coef[slot, i, r : r + 1, :] * stall[yy, s, i].astype(f32)
            states[slot, :, i * H : (i + 1) * H] = total.astype(bf16)

    def finish_tile(i):
        slot = i // 2
        at = pl.ds(pl.multiple_of(i * own, own), own)
        column = cumc[slot, pl.ds(pl.multiple_of((i % 2) * own, own), own), :]
        last = cumr[slot, 0:1, run_rows - 1 : run_rows]
        carried = jnp.dot(rets[0, at, :], states[slot], preferred_element_type=f32)
        value = (
            acc_r[at, :H] + jnp.exp(column) * carried[:, :H]
            + jnp.exp(last - column) * carried[:, H:]
        )
        value = value - jnp.mean(value, axis=1, keepdims=True)
        value = value * lax.rsqrt(jnp.mean(value * value, axis=1, keepdims=True) + 1e-06)
        value = value.astype(bf16)
        out = pl.ds(pl.multiple_of(i * edge, edge), edge)
        mix[0, out, 2 * H :] = value[:edge]
        mix[1, out, 2 * H :] = value[edge:]

    @pl.loop(0, 4, unroll=True)
    def _(i):
        finish_tile(i)

    @pl.when(middle)
    def _():
        for k in range(2):
            pass_far(O, k)

    turned = jnp.transpose(logm[...])
    for b in range(4):
        lsend[b] = turned[2 * b : 2 * b + 2]
        lrecv[w.h] = jnp.where(w.b == b, turned[2 * b : 2 * b + 2], lrecv[w.h] if b else 0.0)
    h_of = lambda zl, x: 2 * lax.rem(w.zh + zl, 2) + x
    log_to = (
        (1 - w.x, w.zl, w.to_x), (w.x, 1 - w.zl, w.to_z), (1 - w.x, 1 - w.zl, w.to_zx),
    )
    log_sends = [
        remote(lsend.at[block(zl, x)], lrecv.at[w.h], l_sem.at[0, i], l_sem.at[1, i], to)
        for i, (x, zl, to) in enumerate(log_to)
    ]

    for copy in log_sends:
        copy.start()

    chunks = 8

    def columns_of(i, x):
        far, across, zl = i // 4, (i // 2) % 2, i % 2
        return w.at(flip(w.zh, far), zl, flip(y, across), x)

    def swap(i):
        return remote(give.at[i], take.at[i], give_s.at[i], take_r.at[i], w.to_c)

    def x_first(i, k):
        return 1 if k == 0 else jnp.where(i < 1, 1, 0)

    def toward(dx):
        return {"x": flip(w.x, dx), "zl": flip(w.zl, 1 - dx)}

    def first_hop(i, k):
        to = toward(x_first(i, k))
        return remote(s1.at[i, k], r1.at[i, k], s1_s.at[i, k], r1_r.at[i, k], to)

    def second_hop(i, k):
        to = toward(1 - x_first(i, k))
        return remote(s2.at[i, k], r2.at[i, k], s2_s.at[i, k], r2_r.at[i, k], to)

    def side(i, k, j, cross):
        dx = x_first(i, k)
        zl = dx * j + (1 - dx) * flip(w.zl, cross)
        x = dx * flip(w.x, cross) + (1 - dx) * j
        return block(zl, x)

    def part(b):
        return pl.ds(pl.multiple_of(b * edge, edge), edge)

    lag = 6

    @pl.loop(0, chunks + lag)
    def _(step):
        @pl.when((step >= 1) & (step < chunks + 1))
        def _():
            i = step - 1
            swap(i).wait_recv()
            for k in range(2):
                for j in range(2):
                    b = side(i, k, j, 1)
                    total = mine[i % 4, k, part(b), :] + take[i, k, part(b), :].astype(f32)
                    s1[i, k, j] = total.astype(bf16)
                first_hop(i, k).start()
            for k in range(2):
                for j in range(2):
                    b = side(i, k, j, 0)
                    mine[i % 4, k, part(b), :] += take[i, k, part(b), :].astype(f32)

        @pl.when(step < chunks)
        def _():
            i = step

            @pl.when((i // 2) % 2 == 1)
            def _():
                for x in range(2):
                    O.arrive(columns_of(i, x))

            @pl.when((i == 2) & (w.g == 0))
            def _():
                for k in range(2):
                    pass_far(O, k)

            @pl.when(i == 4)
            def _():
                for k in range(2, 4):
                    pass_far(O, k)

            for k in range(2):
                give[i, k] = jnp.dot(
                    mix[1 - w.c], O.wide[columns_of(i, k)], preferred_element_type=f32
                ).astype(bf16)
            swap(i).start()
            for k in range(2):
                mine[i % 4, k] = jnp.dot(
                    mix[w.c], O.wide[columns_of(i, k)], preferred_element_type=f32
                )

        @pl.when((step >= 2) & (step < chunks + 2))
        def _():
            i = step - 2
            for k in range(2):
                first_hop(i, k).wait_recv()
                dx = x_first(i, k)
                j = flip(dx * w.zl + (1 - dx) * w.x, 1)
                b = side(i, k, j, 0)
                s2[i, k] = (mine[i % 4, k, part(b), :] + r1[i, k, j].astype(f32)).astype(bf16)
                second_hop(i, k).start()
                j = flip(j, 1)
                kept[i, k] = mine[i % 4, k, part(w.b), :] + r1[i, k, j].astype(f32)

        @pl.when(step >= lag)
        def _():
            i = step - lag
            for k in range(2):
                second_hop(i, k).wait_recv()
                at = pl.ds(pl.multiple_of(columns_of(i, k) * own, own), own)
                mixed[:, at] = (kept[i, k] + r2[i, k].astype(f32)).astype(mixed.dtype)

    for i, (x, zl, to) in enumerate(log_to):
        here = lrecv.at[h_of(zl, x)]
        remote(here, here, l_sem.at[0, i], l_sem.at[1, i], to).wait_recv()
    for h in range(4):
        for head_i in range(2):
            for t in range(2):
                logs_out[2 * h + head_i : 2 * h + head_i + 1, t * edge : (t + 1) * edge] = (
                    lrecv[h, t : t + 1, head_i * edge : (head_i + 1) * edge]
                )

    for stream in (A, R, O):
        stream.drain()
    for i in range(1, 16):
        decay_send(i).wait_send()
    for copy in tokens_x + tokens_c + [tokens_z, gain_c]:
        copy.wait_send()
    for copy in halo_y + state_sends[:1] + log_sends:
        copy.wait_send()

    @pl.when(w.g == 0)
    def _():
        for copy in state_sends[1:]:
            copy.wait_send()

        @pl.when(has_far)
        def _():
            halo_far.wait_send()

    @pl.loop(0, chunks)
    def _(i):
        swap(i).wait_send()
        for k in range(2):
            first_hop(i, k).wait_send()
            second_hop(i, k).wait_send()


def settle_kernel(mixed, logs, mixed_out, logs_out, sems):
    rows = mixed.shape[0] // 8
    copies = [
        pltpu.make_async_copy(
            mixed.at[pl.ds(i * rows, rows)], mixed_out.at[pl.ds(i * rows, rows)], sems.at[i]
        )
        for i in range(8)
    ]
    copies.append(pltpu.make_async_copy(logs, logs_out, sems.at[8]))
    for copy in copies:
        copy.start()
    for copy in copies:
        copy.wait()


def settle(mixed, logs):
    return pl.pallas_call(
        settle_kernel,
        out_shape=tuple(jax.ShapeDtypeStruct(v.shape, v.dtype) for v in (mixed, logs)),
        in_specs=[pl.BlockSpec(memory_space=pltpu.VMEM)] * 2,
        out_specs=[pl.BlockSpec(memory_space=pl.ANY)] * 2,
        scratch_shapes=[pltpu.SemaphoreType.DMA((9,))],
    )(mixed, logs)


def fused(*args):
    tokens, gain, q_att = args[:3]
    out_att, out_ret, sink, decay_log = args[8:]
    own, half_d = tokens.shape
    rows, run_rows = 4 * own, 2 * own
    H, edge = HEAD_DIM, SPAN_RADIUS
    bf16, f32 = jnp.bfloat16, jnp.float32
    dma, vmem = pltpu.SemaphoreType.DMA, pltpu.VMEM
    depth = q_att.shape[0]
    width = out_att.shape[1] * 16

    freqs = 10000.0 ** (-np.arange(0, H, 2, dtype=np.float64) / H)
    freqs = np.concatenate([freqs, freqs])[None, :]
    sign = np.where(np.arange(H) < H // 2, -1.0, 1.0)[None, :]
    inner = np.arange(own)[:, None] * freqs
    outer = (np.arange(16) * own)[:, None] * freqs
    cos_t, sin_t = jnp.asarray(np.cos(inner), f32), jnp.asarray(np.sin(inner), f32)
    base = jnp.asarray(
        np.stack([np.cos(outer), np.sin(outer), sign * np.sin(outer), sign * np.cos(outer)]), f32
    )

    def stream(block):
        return [
            vmem((16,) + block, bf16), vmem((2,) + block, bf16), vmem((2,) + block, bf16),
            dma((4,)), dma((2,)), dma((2,)), dma((4,)), dma((8,)), dma((1,)), dma((16,)),
            dma((2, 4, PARTS)), dma((2, 4, PARTS)),
        ]

    out_rows = (out_att.shape[0] + out_ret.shape[0]) // 4
    tile = (8, 2, 4 * edge, own)
    hbm, inside = pl.BlockSpec(memory_space=pl.ANY), pl.BlockSpec(memory_space=pltpu.VMEM)
    mixed, logs = pl.pallas_call(
        fused_kernel,
        out_shape=(
            jax.ShapeDtypeStruct((own // 2, width), bf16),
            jax.ShapeDtypeStruct((sink.shape[0], own), f32),
        ),
        in_specs=[hbm] * 10 + [pl.BlockSpec(memory_space=pltpu.SMEM), hbm] + [inside] * 3,
        out_specs=[inside] * 2,
        scratch_shapes=[
            vmem((2, 4, own, half_d), bf16),
            vmem((2, rows, half_d), bf16),
            vmem((2, rows, H), f32),
            vmem((2, 1, half_d), f32),
            vmem((rows, 4 * H), f32),
            vmem((rows, 3 * H), f32),
            vmem((2, 2, run_rows + 2 * edge, H), bf16),
            vmem((rows, 2 * H), bf16),
            vmem((3, rows, H), bf16),
            vmem((2, 2, 2, 2) + decay_log.shape, f32),
            vmem((2, 8, run_rows), f32),
            vmem((2, run_rows, H), f32),
            vmem((2, 3, 8, H), f32),
            vmem((2, H, 2 * H), bf16),
            vmem((2, 2, 2, H, H), bf16), vmem((3, H, H), bf16),
            vmem((2, 4 * edge, 3 * H), bf16),
            vmem((2 * edge, 3 * edge), f32),
            vmem((2 * edge, H), f32),
            vmem((4, 2, 2 * edge), f32),
            vmem((4, 2, 2 * edge), f32),
            vmem((4,) + tile[1:], f32), vmem((8, 2, edge, own), f32), vmem(tile, bf16), vmem(tile, bf16),
            vmem((8, 2, 2, edge, own), bf16), vmem((8, 2, 2, edge, own), bf16),
            vmem((8, 2, edge, own), bf16), vmem((8, 2, edge, own), bf16),
            dma((3,)), dma((3,)), dma((1,)), dma((5,)), dma((2, 4, 2)), dma((2,)), dma((2, 16)),
            dma((2, 4)), dma((2, 3)), dma((2, 3)), pltpu.SemaphoreType.REGULAR,
            dma((8,)), dma((8,)), dma((8, 2)), dma((8, 2)), dma((8, 2)), dma((8, 2)),
        ]
        + stream((depth, 4 * H))
        + stream((depth, 3 * H))
        + stream((out_rows, own)),
        compiler_params=pltpu.CompilerParams(
            collective_id=0, has_side_effects=True, vmem_limit_bytes=67043328
        ),
        cost_estimate=pl.CostEstimate(
            flops=10**11, bytes_accessed=2 * 10**7, transcendentals=0
        ),
    )(
        tokens, gain.reshape(1, half_d), *args[2:10], sink, decay_log, cos_t, sin_t, base
    )
    return settle(mixed, logs)


def attend(query, key, value, sink, offset, total_rows):
    rows, kv, group, _ = query.shape
    ext = halo(jnp.stack([key, value]), "t", SPAN_RADIUS)
    size = min(rows, BLOCK)
    count = rows // size
    span = size + 2 * SPAN_RADIUS
    pieces = jnp.stack([ext[:, b * size : b * size + span] for b in range(count)])
    blocks = query.reshape(count, size, kv, group, HEAD_DIM)
    scores = jnp.einsum(
        "bqhgd,bkhd->bhgqk", blocks, pieces[:, 0], preferred_element_type=jnp.float32
    ) * HEAD_DIM ** (-0.5)
    base = offset + jnp.arange(count, dtype=jnp.int32) * size
    query_pos = base[:, None] + jnp.arange(size, dtype=jnp.int32)
    key_pos = base[:, None] - SPAN_RADIUS + jnp.arange(span, dtype=jnp.int32)
    spacing = key_pos[:, None, :] - query_pos[:, :, None]
    inside = (key_pos >= 0) & (key_pos < total_rows)
    valid = (jnp.abs(spacing) <= SPAN_RADIUS) & inside[:, None, :]
    masked = jnp.where(valid[:, None, None], scores, -jnp.inf)
    limit = sink[None, :, :, None]
    top = jnp.maximum(jnp.max(masked, axis=-1), limit)
    expo = jnp.exp(masked - top[..., None])
    total = jnp.sum(expo, axis=-1) + jnp.exp(limit - top)
    logs = top + jnp.log(total)
    probs = (expo / total[..., None]).astype(jnp.bfloat16)
    result = jnp.einsum(
        "bhgqk,bkhd->bqhgd", probs, pieces[:, 1], preferred_element_type=jnp.float32
    ).astype(jnp.bfloat16)
    logs = jnp.transpose(logs, (1, 2, 0, 3)).reshape(kv * group, rows)
    return result.reshape(rows, kv * group * HEAD_DIM), logs


def retain(query, key, value, decay):
    rows, heads, _ = query.shape
    peers, index = lax.axis_size("t"), lax.axis_index("t")
    cumul = jnp.cumsum(decay, axis=1)
    last = cumul[:, -1]
    query_f, key_f, value_f = (v.astype(jnp.float32) for v in (query, key, value))
    trailing = jnp.exp(last[:, None] - cumul)
    leading = jnp.exp(cumul)
    forward = jnp.einsum("hk,khd,khe->hde", trailing, key_f, value_f, precision=HIGHEST)
    backward = jnp.einsum("hk,khd,khe->hde", leading, key_f, value_f, precision=HIGHEST)
    tail = jnp.broadcast_to(last[:, None, None], (heads, 8, HEAD_DIM))
    sent = jnp.concatenate([forward, backward, tail], axis=1)
    seen = lax.all_gather(sent, "t", axis=0)
    lasts = seen[:, :, 2 * HEAD_DIM, 0]
    at = jnp.arange(peers)
    low = jnp.minimum(at, index)[:, None]
    high = jnp.maximum(at, index)[:, None]
    between = (at[None, :] > low) & (at[None, :] < high)
    spans = jnp.exp(jnp.sum(jnp.where(between[:, :, None], lasts[None], 0.0), axis=1))
    before = jnp.sum(
        jnp.where(at < index, 1.0, 0.0)[:, None, None, None]
        * spans[:, :, None, None]
        * seen[:, :, :HEAD_DIM],
        axis=0,
    )
    after = jnp.sum(
        jnp.where(at > index, 1.0, 0.0)[:, None, None, None]
        * spans[:, :, None, None]
        * seen[:, :, HEAD_DIM : 2 * HEAD_DIM],
        axis=0,
    )
    scores = jnp.einsum("qhd,khd->hqk", query, key, preferred_element_type=jnp.float32)
    weights = jnp.exp(-jnp.abs(cumul[:, :, None] - cumul[:, None, :]))
    mix = jnp.einsum("hqk,khd->qhd", scores * weights, value_f, precision=HIGHEST)
    mix = mix + leading.T[:, :, None] * jnp.einsum(
        "qhd,hde->qhe", query_f, before, precision=HIGHEST
    )
    mix = mix + trailing.T[:, :, None] * jnp.einsum(
        "qhd,hde->qhe", query_f, after, precision=HIGHEST
    )
    middle = mix - jnp.mean(mix, axis=-1, keepdims=True)
    normed = middle * lax.rsqrt(jnp.mean(middle * middle, axis=-1, keepdims=True) + 1e-06)
    return normed.astype(jnp.bfloat16).reshape(rows, heads * HEAD_DIM)


def shards(
    tokens, gain, q_att, k_att, v_att, q_ret, k_ret, v_ret, out_att, out_ret, sink, decay_log
):
    parts = lax.axis_size("h")
    own = tokens.shape[0]
    rows = own * parts
    width = tokens.shape[1] * lax.axis_size("tp")
    kv = k_att.shape[1] // HEAD_DIM // parts
    group = q_att.shape[1] // k_att.shape[1]
    att = kv * group
    ret = q_ret.shape[1] // HEAD_DIM // parts
    offset = lax.axis_index("t") * rows
    total_rows = rows * lax.axis_size("t")

    packed = jnp.concatenate(
        [
            w.reshape(w.shape[0], parts, w.shape[1] // parts)
            for w in (q_att, k_att, v_att, q_ret, k_ret, v_ret)
        ],
        axis=2,
    )
    packed = jnp.moveaxis(packed, 1, 0)
    out_pack = jnp.concatenate(
        [w.reshape(parts, w.shape[0] // parts, w.shape[1]) for w in (out_att, out_ret)], axis=1
    )
    widened = tokens.astype(jnp.float32)
    sums = jnp.sum(widened * widened, axis=1)
    scaled = (widened * gain).astype(jnp.bfloat16)
    cores = lax.axis_size("tp")
    flat = packed.reshape(parts * packed.shape[1], packed.shape[2])
    weight = gather(exchange(flat, "h", 0, 0), "t", 0)
    whole = gather(gather(scaled, "h", 0), "tp", 1)
    proj = jnp.dot(whole, weight, preferred_element_type=jnp.float32)
    out_own = exchange(out_pack, "h", 0, 0)
    sums = lax.all_gather(sums, ("h", "tp"))
    decay = exchange(decay_log, "h", 0, 1)
    squares = jnp.sum(sums.reshape(parts, cores, own), axis=1).reshape(rows)
    inverse = lax.rsqrt(squares / width + 1e-06)[:, None]

    edges = [att, kv, kv, ret, ret, ret]
    starts = [sum(edges[:i]) * HEAD_DIM for i in range(6)]
    qa, ka, va, qr, kr, vr = (
        proj[:, s : s + n * HEAD_DIM].reshape(rows, n, HEAD_DIM) for s, n in zip(starts, edges)
    )
    scale = inverse[:, :, None]
    positions = (offset + jnp.arange(rows, dtype=jnp.int32)).astype(jnp.float32)
    freqs = 10000.0 ** (-jnp.arange(0, HEAD_DIM, 2).astype(jnp.float32) / HEAD_DIM)
    angles = positions[:, None] * freqs[None, :]
    cosine, sine = jnp.cos(angles)[:, None, :], jnp.sin(angles)[:, None, :]
    att_query = rotate(qa * scale, cosine, sine)
    att_key = rotate(ka * scale, cosine, sine)
    att_value = (va * scale).astype(jnp.bfloat16)
    ret_query = (qr * scale).astype(jnp.bfloat16)
    ret_key = (kr * (scale * HEAD_DIM ** (-0.5))).astype(jnp.bfloat16)
    ret_value = (vr * scale).astype(jnp.bfloat16)

    logits = lax.dynamic_slice_in_dim(sink, lax.axis_index("h") * att, att).reshape(kv, group)
    att_out, logs = attend(
        att_query.reshape(rows, kv, group, HEAD_DIM), att_key, att_value, logits, offset, total_rows
    )
    ret_out = retain(ret_query, ret_key, ret_value, decay)

    out_wide = gather(out_own, "t", 0)
    mixers = jnp.concatenate([att_out, ret_out], axis=1)
    depth = out_wide.shape[1]
    out_wide = jnp.moveaxis(out_wide, 0, 1).reshape(depth, -1)
    mixed = jnp.dot(mixers, out_wide, preferred_element_type=jnp.float32).astype(jnp.bfloat16)
    mixed = lax.psum_scatter(mixed, ("h", "tp"), scatter_dimension=0, tiled=True)
    return mixed, exchange(logs, "h", 1, 0)


def fits(args, sp, tp):
    tokens, _, q_att, k_att, v_att, q_ret, k_ret, v_ret, out_att, _, _, decay = args
    own, heads = tokens.shape[0] // sp, 4 * tp
    return (
        sp == 16
        and tp == 2
        and own == 2 * SPAN_RADIUS
        and q_att.shape[0] == sp * own
        and tokens.shape[1] == sp * own
        and q_att.shape[1] == 2 * heads * HEAD_DIM
        and all(v.shape[1] == heads * HEAD_DIM for v in (k_att, v_att, q_ret, k_ret, v_ret))
    )


def solution(mesh):
    sp, tp = mesh.shape["sp"], mesh.shape["tp"]

    def run(*args):
        if fits(args, sp, tp):
            seq = ("zh", "zl", "y", "x")
            fine = Mesh(mesh.devices.reshape(2, 2, 2, 2, tp), seq + ("tp",))
            step = fused
        else:
            heads = math.gcd(args[3].shape[1], args[5].shape[1]) // HEAD_DIM
            parts = math.gcd(heads // math.gcd(heads, tp), sp)
            seq = ("t", "h")
            fine = Mesh(mesh.devices.reshape(sp // parts, parts, tp), seq + ("tp",))
            step = shards
        body = jax.shard_map(
            step,
            mesh=fine,
            in_specs=(P(seq, "tp"), P("tp"))
            + (P(seq, "tp"),) * 6
            + (P("tp", seq), P("tp", seq), P("tp"), P("tp", seq)),
            out_specs=(P(seq + ("tp",), None), P("tp", seq)),
            check_vma=False,
        )
        return body(*args)

    return run
```
